256 devices in a mesh: grp: 2 (over y), ep: 32 (over z, core), tp: 4 (over x).
Axes of the slice: x: 4, y: 2, z: 16, core: 2. Of those that a mesh axis runs over, the one named last changes fastest.
The devices are a block of a 4x16x16 slice.
Arguments:
- query: bfloat16 [65536, 1024], P(('grp', 'ep'), 'tp'), parts along dimension 0, may hold values from -6 to 6
- forget_gate_logits: bfloat16 [65536, 1024], P(('grp', 'ep'), 'tp'), parts along dimension 0, may hold values from -8 to 8
- value: bfloat16 [65536, 1024], P(('grp', 'ep'), 'tp'), parts along dimension 0, may hold values from -6 to 6
- forget_lower_margin: float32 [2, 1024], P(None, 'tp'), may hold values from -30 to -2
- position_log_decay: float32 [8, 65536], P('tp', ('grp', 'ep')), parts along dimension 1, may hold values from -1.5 to 0
- head_norm_gain: float32 [128], replicated, may hold values from 0.1 to 1.9
- mixer_output_weight: bfloat16 [1024, 2048], P('tp'), may hold values from -0.1875 to 0.1875
- second_batch_tokens: bfloat16 [32768, 2048], P(('grp', 'ep', 'tp')), parts along dimension 0, may hold values from -60 to 60
- expert_norm_gain: float32 [2048], replicated, may hold values from 0.1 to 1.9
- routes: int32 [32768, 2], P(('grp', 'ep', 'tp')), parts along dimension 0, may hold values from 0 to 31, all different within a row; in each aligned block of 128 rows (0 to 127, 128 to 255, ...) at most 12 rows name the same one
- chosen_expert_weight: float32 [32768, 2], P(('grp', 'ep', 'tp')), parts along dimension 0, may hold values from 0.2 to 1
- gate_weight: bfloat16 [32, 2048, 2048], P('ep', None, 'tp'), may hold values from -0.3125 to 0.3125
- up_weight: bfloat16 [32, 2048, 2048], P('ep', None, 'tp'), may hold values from -0.3125 to 0.3125
- down_weight: bfloat16 [32, 2048, 2048], P('ep', 'tp'), may hold values from -0.02734375 to 0.02734375
Outputs:
- first_mixer_output: bfloat16 [65536, 2048], P(('grp', 'ep', 'tp')), parts along dimension 0
- moe_out: bfloat16 [32768, 2048], P(('grp', 'ep', 'tp')), parts along dimension 0
The draws below stay inside these ranges and needn't reach their ends.
There are 2 independent parts, one for each index of `grp`. The reference program is written for one: setup_inputs(seed, part) draws one part's arguments, and reference() takes and returns one part's arrays. A program takes and returns all parts, laid end to end along the dimension named above; an argument that names none is the same for every part. Nothing has to cross between parts.
Inputs may be any that keep to these rules, and one draw needn't show every extreme that they name: `routes`: each row names 2 different experts. Among the rows of one device no expert is named by more than 12 rows, and in every draw some expert is named by exactly 12 rows of some device.
All inputs are finite; a program needn't handle non-finite values.
Results may differ from the reference program's by a relative error of at most 0.015.
Values may be sent and summed in bfloat16 or wider, within the bound.
A program may use at most 128 MiB of HBM per device.

```python
import math
import jax
import jax.numpy as jnp
import numpy as np
from jax import lax

D = 2048
RECURRENT_HEADS = 8
HEAD_CHANNELS = 128
FF = 2048
TOPK = 2
BLK = 128
ROWS = 1024
TOK_DEV = 128
SEQUENCE_TOKENS = 32768
MOE_TOKENS = 16384
EXPERTS = 32
CAP = 12
HEAD_GROUP = 2
FF_GROUP = 512
N_EP = 32
N_TP = 4


def draw_forget_lower_margin(key, part):
    key = jax.random.fold_in(key, 101)
    pick_key, fast_key, slow_key = jax.random.split(key, 3)
    share = 0.5
    slow_heads = jax.random.uniform(pick_key, (2, RECURRENT_HEADS, 1)) < share
    fast_gap = jnp.log(jax.random.uniform(fast_key, (2, RECURRENT_HEADS, HEAD_CHANNELS), minval=0.02, maxval=0.06))
    slow_gap = jax.random.uniform(slow_key, (2, RECURRENT_HEADS, HEAD_CHANNELS), minval=jnp.log(0.1), maxval=jnp.log(0.4)) - jnp.log(float(SEQUENCE_TOKENS))
    chosen = jnp.where(slow_heads, slow_gap, fast_gap)
    return chosen.reshape(2, RECURRENT_HEADS * HEAD_CHANNELS).astype(jnp.float32)


def draw_position_log_decay(key, part):
    key = jax.random.fold_in(key, 202)
    rate_key, place_key, size_key = jax.random.split(key, 3)
    blocks = SEQUENCE_TOKENS // ROWS
    rates = jnp.exp(jax.random.uniform(rate_key, (RECURRENT_HEADS, blocks, 1), minval=jnp.log(0.15), maxval=jnp.log(0.6)))
    steady = jnp.broadcast_to(rates / SEQUENCE_TOKENS, (RECURRENT_HEADS, blocks, ROWS)).reshape(RECURRENT_HEADS, SEQUENCE_TOKENS)
    places = jax.random.randint(place_key, (RECURRENT_HEADS, 2), 0, SEQUENCE_TOKENS)
    sizes = jax.random.uniform(size_key, (RECURRENT_HEADS, 2), minval=0.22, maxval=0.69)
    positions = jnp.arange(SEQUENCE_TOKENS, dtype=jnp.int32)
    hits = jnp.sum(jnp.where(positions[None, None, :] == places[:, :, None], sizes[:, :, None], 0.0), axis=1)
    return (-steady - hits).astype(jnp.float32)


def draw_second_batch_tokens(key, part):
    key = jax.random.fold_in(key, 303)
    base_key, row_key, column_key = jax.random.split(key, 3)
    base = jnp.clip(jax.random.normal(base_key, (MOE_TOKENS, D)), -5.0, 5.0)
    row_scale = jnp.exp(jax.random.uniform(row_key, (MOE_TOKENS, 1), minval=jnp.log(0.3), maxval=jnp.log(3.0)))
    column_scale = jnp.exp(jax.random.uniform(column_key, (1, D), minval=jnp.log(0.4), maxval=jnp.log(4.0)))
    return (base * row_scale * column_scale).astype(jnp.bfloat16)


def level_of(own_key, dims, pieces, smallest, largest):
    factor_of, own = 1.0, jax.random.fold_in(own_key, 6)
    for axis_at, blocks in pieces:
        steps = jnp.exp(jax.random.uniform(jax.random.fold_in(own, axis_at), (blocks,), jnp.float32, smallest / len(pieces), largest / len(pieces)))
        factor_of = factor_of * jnp.repeat(steps, dims[axis_at] // blocks).reshape([-1 if axis == axis_at else 1 for axis in range(len(dims))])
    return factor_of


def routed_block(stream_key, own, number, rows, number_of, top, reach, skew):
    ranking = jax.random.permutation(stream_key, number_of)
    heavy_load, ordinary = load_shares(number_of, rows * top, reach, skew, True), load_shares(number_of, rows * top, reach, skew, False)
    places = jnp.arange(number_of)

    def named(tallies, turn):
        used = int((tallies > 0).sum())
        fixed = max(1, used // 4)
        shifted = fixed + (places - fixed + turn * (used - fixed)) % max(1, number_of - fixed)
        return jnp.zeros((number_of,), jnp.int32).at[ranking[jnp.where(places < fixed, places, shifted)]].set(jnp.asarray(tallies, jnp.int32))

    tallies = jnp.where(number % 4 == 0, named(heavy_load, number // 4), named(ordinary, number - number // 4 - 1))
    mixed = jax.random.permutation(jax.random.fold_in(own, 3), number_of)
    giver, sink = mixed[0:number_of // 2 * 2:2], mixed[1:number_of // 2 * 2:2]
    margin = jnp.minimum(tallies[giver] - 1, reach - tallies[sink]) // 2
    margin = jnp.where((giver == ranking[0]) | (sink == ranking[0]) | (tallies[sink] == 0), 0, jnp.maximum(margin, 0))
    shifted = jax.random.randint(jax.random.fold_in(own, 4), (number_of // 2,), 0, 1 << 20) % (margin + 1)
    tallies = tallies.at[giver].add(-shifted).at[sink].add(shifted)
    members = jnp.searchsorted(jnp.cumsum(tallies), jnp.arange(rows * top), side="right").astype(jnp.int32)
    grid = members.reshape(top, rows).T
    grid = grid[jax.random.permutation(jax.random.fold_in(own, 1), rows)]
    turn = jax.random.randint(jax.random.fold_in(own, 2), (rows, 1), 0, top)
    return jnp.take_along_axis(grid, (jnp.arange(top)[None, :] + turn) % top, axis=1)


def load_shares(count, total, limit, slope, full):
    loads = [(1 << 20) // math.isqrt(grade ** slope) + 1 for grade in range(1, count + 1)]
    largest = limit if full else min(limit, max(-(-total // count), total * loads[0] // sum(loads)))
    least = 1 if total - largest >= count - 1 else 0
    given, surplus = [largest] + [least] * (count - 1), total - largest - least * (count - 1)
    while surplus > 0:
        free = [i for i in range(1, count) if given[i] < largest] or [i for i in range(1, count) if given[i] < limit]
        whole, remaining = sum([loads[i] for i in free]), surplus
        for i in free:
            more = min(limit - given[i], max(1, remaining * loads[i] // whole), surplus)
            given[i] = given[i] + more
            surplus = surplus - more
    return np.array(given)


def noise(stream_key, dims, spread, most, cuts=(), kind=jnp.bfloat16):
    loudness = level_of(stream_key, dims, cuts, -0.22, 0.18) if cuts else 1.0
    values = jax.random.normal(stream_key, dims, jnp.float32) * spread * loudness
    return jnp.minimum(jnp.maximum(values, -most), most).astype(kind)


def setup_inputs(seed: int = 0, part: int = 0) -> dict:
    seeds = jax.random.split(jax.random.key(seed), 15)
    own_keys = jax.random.split(jax.random.fold_in(seeds[14], part), 15)
    query = noise(own_keys[0], (SEQUENCE_TOKENS, RECURRENT_HEADS * HEAD_CHANNELS), 1.0, 6.0, ((0, 32), (1, 4)))
    forget_gate_logits = noise(own_keys[1], (SEQUENCE_TOKENS, RECURRENT_HEADS * HEAD_CHANNELS), 1.5, 8.0, ((0, 32), (1, 4)))
    value = noise(own_keys[2], (SEQUENCE_TOKENS, RECURRENT_HEADS * HEAD_CHANNELS), 1.0, 6.0, ((0, 32), (1, 4)))
    forget_lower_margin = draw_forget_lower_margin(jax.random.fold_in(seeds[14], 71), part)
    position_log_decay = draw_position_log_decay(jax.random.fold_in(jax.random.fold_in(seeds[14], part), 71), part)
    head_norm_gain = jnp.clip(1.0 + 0.18 * jax.random.normal(seeds[5], (HEAD_CHANNELS,), jnp.float32), 0.1, 1.9)
    mixer_output_weight = noise(seeds[6], (RECURRENT_HEADS * HEAD_CHANNELS, D), (RECURRENT_HEADS * HEAD_CHANNELS) ** -0.5, 0.1875, ((0, 4),))
    second_batch_tokens = draw_second_batch_tokens(jax.random.fold_in(jax.random.fold_in(seeds[14], part), 71), part)
    expert_norm_gain = jnp.clip(1.0 + 0.18 * jax.random.normal(seeds[8], (D,), jnp.float32), 0.1, 1.9)
    routes_keys = jax.random.split(jax.random.fold_in(own_keys[9], 1), MOE_TOKENS // TOK_DEV)
    routes_turns = jax.random.permutation(jax.random.fold_in(own_keys[9], 3), MOE_TOKENS // TOK_DEV)
    routes = jax.vmap(lambda own, number: routed_block(jax.random.fold_in(own_keys[9], 2), own, number, TOK_DEV, EXPERTS, TOPK, CAP, 2))(routes_keys, routes_turns).reshape((MOE_TOKENS, TOPK))
    chosen_expert_weight = jnp.clip(0.2 + 0.8 * jax.random.uniform(own_keys[10], (MOE_TOKENS, TOPK), jnp.float32) ** level_of(own_keys[10], (MOE_TOKENS, TOPK), ((0, 128),), -0.2, 0.2), 0.2, 1.0)
    gate_weight = noise(seeds[11], (EXPERTS, D, FF), (D // 6) ** -0.5, 0.3125, ((0, 32), (2, 4)))
    up_weight = noise(seeds[12], (EXPERTS, D, FF), (D // 6) ** -0.5, 0.3125, ((0, 32), (2, 4)))
    down_weight = noise(seeds[13], (EXPERTS, FF, D), (25 * FF) ** -0.5, 0.02734375, ((0, 32), (1, 4)))
    return {"query": query, "forget_gate_logits": forget_gate_logits, "value": value, "forget_lower_margin": forget_lower_margin, "position_log_decay": position_log_decay, "head_norm_gain": head_norm_gain, "mixer_output_weight": mixer_output_weight, "second_batch_tokens": second_batch_tokens, "expert_norm_gain": expert_norm_gain, "routes": routes, "chosen_expert_weight": chosen_expert_weight, "gate_weight": gate_weight, "up_weight": up_weight, "down_weight": down_weight}


NORM_EPS = 1e-06
CLAMP_LIMIT = 7.0
SIGMOID_SCALE = 1.702
PRECISE = lax.Precision.HIGHEST

def clamped_unit(gate_pre, up_pre):
    gate_pre = jnp.minimum(gate_pre, CLAMP_LIMIT)
    up_pre = jnp.clip(up_pre, -CLAMP_LIMIT, CLAMP_LIMIT)
    return (up_pre + 1.0) * gate_pre * jax.nn.sigmoid(SIGMOID_SCALE * gate_pre)

def block_recurrence(queries, ending_state, values, forget_log_rates):
    sequence_length, number_of_heads, channels = queries.shape
    nblocks = sequence_length // BLK

    def to_blocks(array):
        return array.reshape(nblocks, BLK, number_of_heads, array.shape[-1])
    query_blocks = to_blocks(queries)
    key_blocks = to_blocks(ending_state)
    value_blocks = to_blocks(values)
    cumul = jnp.cumsum(to_blocks(forget_log_rates), axis=1)
    block_last = cumul[:, -1]
    query_in = query_blocks * jnp.exp(cumul)
    key_in = key_blocks * jnp.exp(-cumul)
    key_state = key_blocks * jnp.exp(block_last[:, None] - cumul)
    lower = jnp.tril(jnp.ones((BLK, BLK), jnp.float32))
    scores = jnp.einsum('nchd,nshd->nhcs', query_in, key_in, precision=PRECISE) * lower
    inner = jnp.einsum('nhcs,nshv->nchv', scores, value_blocks, precision=PRECISE)
    increments = jnp.einsum('nshd,nshv->nhdv', key_state, value_blocks, precision=PRECISE)

    def advance(state, inputs):
        decay, increment = inputs
        return (state * decay[..., None] + increment, state)
    initial = jnp.zeros((number_of_heads, channels, values.shape[-1]), jnp.float32)
    final_state, before = lax.scan(advance, initial, (jnp.exp(block_last), increments))
    outer = jnp.einsum('nchd,nhdv->nchv', query_in, before, precision=PRECISE)
    return (inner + outer).reshape(sequence_length, number_of_heads, values.shape[-1])

def token_mixer(query, forget_gate_logits, value, forget_lower_margin, position_log_decay, head_norm_gain, mixer_output_weight):
    queries = jax.nn.silu(query.astype(jnp.float32)).reshape(SEQUENCE_TOKENS, RECURRENT_HEADS, HEAD_CHANNELS) * HEAD_CHANNELS ** (-0.5)
    values = value.astype(jnp.float32).reshape(SEQUENCE_TOKENS, RECURRENT_HEADS, HEAD_CHANNELS)
    shutting = jax.nn.sigmoid(-forget_gate_logits.astype(jnp.float32))
    decay_spikes = jnp.transpose(position_log_decay)[:, :, None]
    mix = jnp.zeros((SEQUENCE_TOKENS, RECURRENT_HEADS, HEAD_CHANNELS), jnp.float32)
    for direction in range(2):
        ending_state = jnp.exp(forget_lower_margin[direction])[None, :] * shutting
        forget_log_rates = jnp.log1p(-ending_state).reshape(SEQUENCE_TOKENS, RECURRENT_HEADS, HEAD_CHANNELS) + decay_spikes
        ending_state = ending_state.reshape(SEQUENCE_TOKENS, RECURRENT_HEADS, HEAD_CHANNELS)
        if direction == 0:
            mix = mix + block_recurrence(queries, ending_state, values, forget_log_rates)
        else:
            turned = block_recurrence(jnp.flip(queries, 0), jnp.flip(ending_state, 0), jnp.flip(values, 0), jnp.flip(forget_log_rates, 0))
            mix = mix + jnp.flip(turned, 0)
    scaled = mix * lax.rsqrt(lax.optimization_barrier(jnp.mean(mix * mix, axis=-1, keepdims=True)) + NORM_EPS) * head_norm_gain
    head_outputs = scaled.reshape(SEQUENCE_TOKENS, RECURRENT_HEADS * HEAD_CHANNELS).astype(jnp.bfloat16)
    group_width = HEAD_GROUP * HEAD_CHANNELS
    summed = jnp.zeros((SEQUENCE_TOKENS, D), jnp.float32)
    for group in range(N_TP):
        part_sum = jnp.dot(head_outputs[:, group * group_width:(group + 1) * group_width], mixer_output_weight[group * group_width:(group + 1) * group_width], preferred_element_type=jnp.float32).astype(jnp.bfloat16)
        summed = summed + part_sum.astype(jnp.float32)
    return summed.astype(jnp.bfloat16)

def experts(second_batch_tokens, expert_norm_gain, routes, chosen_expert_weight, gate_weight, up_weight, down_weight):
    tokens_f = second_batch_tokens.astype(jnp.float32)
    normed = (tokens_f * lax.rsqrt(lax.optimization_barrier(jnp.mean(tokens_f * tokens_f, axis=-1, keepdims=True)) + NORM_EPS) * expert_norm_gain).astype(jnp.bfloat16)
    count = normed.shape[0]
    padded = jnp.concatenate([normed, jnp.zeros((1, D), jnp.bfloat16)], axis=0)
    flat_routes = routes.reshape(-1)
    scales_all = jnp.concatenate([chosen_expert_weight.reshape(-1), jnp.zeros((1,), jnp.float32)])
    most_rows = CAP * N_EP * N_TP

    def one_expert(running, expert):
        positions, = jnp.nonzero(flat_routes == expert, size=most_rows, fill_value=count * TOPK)
        positions = positions.astype(jnp.int32)
        owners = positions // TOPK
        picked_rows = padded[owners]
        scales = scales_all[positions]
        gate_pre = jnp.dot(picked_rows, gate_weight[expert], preferred_element_type=jnp.float32)
        up_pre = jnp.dot(picked_rows, up_weight[expert], preferred_element_type=jnp.float32)
        hidden = clamped_unit(gate_pre, up_pre).astype(jnp.bfloat16)
        result = jnp.zeros((most_rows, D), jnp.float32)
        for group in range(N_TP):
            part_sum = jnp.dot(hidden[:, group * FF_GROUP:(group + 1) * FF_GROUP], down_weight[expert, group * FF_GROUP:(group + 1) * FF_GROUP], preferred_element_type=jnp.float32).astype(jnp.bfloat16)
            result = result + part_sum.astype(jnp.float32)
        rounded = lax.optimization_barrier(result.astype(jnp.bfloat16)).astype(jnp.float32)
        running = running.at[owners].add(scales[:, None] * rounded)
        return (running, None)
    start_sum = jnp.zeros((count + 1, D), jnp.float32)
    total_sum, _ = lax.scan(one_expert, start_sum, jnp.arange(EXPERTS, dtype=jnp.int32))
    return total_sum[:count].astype(jnp.bfloat16)

def reference(query, forget_gate_logits, value, forget_lower_margin, position_log_decay, head_norm_gain, mixer_output_weight, second_batch_tokens, expert_norm_gain, routes, chosen_expert_weight, gate_weight, up_weight, down_weight):
    first_mixer_output = token_mixer(query, forget_gate_logits, value, forget_lower_margin, position_log_decay, head_norm_gain, mixer_output_weight)
    moe_out = experts(second_batch_tokens, expert_norm_gain, routes, chosen_expert_weight, gate_weight, up_weight, down_weight)
    return (first_mixer_output, moe_out)
```

```python
import functools

import jax
import jax.numpy as jnp
import numpy as np
from jax import lax
from jax.experimental import pallas as pl
from jax.experimental.pallas import tpu as pltpu
from jax.sharding import PartitionSpec as P

F32, BF16 = jnp.float32, jnp.bfloat16
HC = 128
BLK = 128
CAP = 12
QUARTERS = 4
EPS = 1e-06
LIMIT = 7.0
SLOPE = 1.702
VMEM = pltpu.VMEM
MESH = pl.DeviceIdType.MESH
WHOLE = pl.BlockSpec(memory_space=VMEM)
ANYWHERE = pl.BlockSpec(memory_space=pl.ANY)


def mm(a, b):
    return jnp.dot(a, b, preferred_element_type=F32)


def mm_t(a, b):
    return lax.dot_general(a, b, (((1,), (1,)), ((), ())), preferred_element_type=F32)


def t_mm(a, b):
    return lax.dot_general(a, b, (((0,), (0,)), ((), ())), preferred_element_type=F32)


def iota(shape, dim):
    return lax.broadcasted_iota(jnp.int32, shape, dim)


def silu_sigmoid(x):
    return 1.0 / (1.0 + jnp.exp(-x))


def recurrence_states(
    q_ref, g_ref, v_ref, margin_ref, pos_ref, qin, kin, before, off, fin, inc, last
):
    blocks = q_ref.shape[0] // BLK
    heads = q_ref.shape[1] // HC
    row, col = iota((BLK, BLK), 0), iota((BLK, BLK), 1)
    tri = ((row >= col).astype(BF16), (row <= col).astype(BF16))
    ends = [jnp.exp(margin_ref[d : d + 1, :]) for d in range(2)]

    def per_block(n, carry):
        rows = pl.ds(pl.multiple_of(n * BLK, BLK), BLK)
        q = q_ref[rows, :].astype(F32)
        q = q * silu_sigmoid(q) * HC**-0.5
        shut = silu_sigmoid(-g_ref[rows, :].astype(F32))
        values = v_ref[rows, :]
        pos = pos_ref[rows, :]
        pos = jnp.concatenate(
            [jnp.broadcast_to(pos[:, h : h + 1], (BLK, HC)) for h in range(heads)], axis=1
        )
        for d in range(2):
            k = ends[d] * shut
            logs = jnp.log1p(-k) + pos
            high = logs.astype(BF16)
            low = (logs - high.astype(F32)).astype(BF16)
            cum = mm(tri[d], high) + mm(tri[d], low)
            end = cum[BLK - 1 :, :] if d == 0 else cum[:1, :]
            qin[d, rows, :] = (q * jnp.exp(cum)).astype(BF16)
            kin[d, rows, :] = (k * jnp.exp(-cum)).astype(BF16)
            ks = (k * jnp.exp(end - cum)).astype(BF16)
            last[d, n] = end
            for h in range(heads):
                cols = slice(h * HC, (h + 1) * HC)
                inc[d, n, h] = t_mm(values[:, cols], ks[:, cols])
        return carry

    lax.fori_loop(0, blocks, per_block, 0)
    slab = iota((16, HC), 0)
    for d in range(2):

        def chain(i, carry):
            n = i if d == 0 else blocks - 1 - i
            offset, states = carry
            off[d, n] = offset
            end = last[d, n]
            decay = jnp.exp(end)
            new = []
            for h in range(heads):
                before[d, n, h] = states[h]
                new.append(states[h] * decay[:, h * HC : (h + 1) * HC] + inc[d, n, h])
            return offset + end, tuple(new)

        zero = tuple(jnp.zeros((HC, HC), F32) for _ in range(heads))
        total, states = lax.fori_loop(0, blocks, chain, (jnp.zeros((1, heads * HC), F32), zero))
        decay = jnp.exp(total)
        for h in range(heads):
            fin[d * heads + h, :HC, :] = states[h].astype(BF16)
            part = decay[:, h * HC : (h + 1) * HC]
            high = part.astype(BF16).astype(F32)
            fin[d * heads + h, HC:, :] = jnp.where(
                slab == 0, high, jnp.where(slab == 1, part - high, 0.0)
            ).astype(BF16)


def recurrence_outputs(qin, kin, v_ref, before, off, every, me_ref, gain, out, entering):
    blocks = v_ref.shape[0] // BLK
    heads = v_ref.shape[1] // HC
    devices = every.shape[0]
    me = me_ref[0]
    for d in range(2):
        for h in range(heads):
            at = d * heads + h

            def combine(i, state):
                j = i if d == 0 else devices - 1 - i
                decay = jnp.sum(every[j, at, HC:, :].astype(F32), axis=0, keepdims=True)
                passed = (j < me) if d == 0 else (j > me)
                return jnp.where(passed, state * decay + every[j, at, :HC, :].astype(F32), state)

            entering[at] = lax.fori_loop(0, devices, combine, jnp.zeros((HC, HC), F32))
    row, col = iota((BLK, BLK), 0), iota((BLK, BLK), 1)

    def per_block(n, carry):
        rows = pl.ds(pl.multiple_of(n * BLK, BLK), BLK)
        for h in range(heads):
            cols = slice(h * HC, (h + 1) * HC)
            scores, outer = [], None
            for d in range(2):
                q = qin[d, rows, cols]
                scores.append(mm_t(q, kin[d, rows, cols]))
                state = before[d, n, h] + entering[d * heads + h] * jnp.exp(off[d, n, :, cols])
                part = mm_t(q, state.astype(BF16))
                outer = part if outer is None else outer + part
            both = jnp.where(row >= col, scores[0], 0.0) + jnp.where(row <= col, scores[1], 0.0)
            mix = mm(both.astype(BF16), v_ref[rows, cols]) + outer
            scale = lax.rsqrt(jnp.mean(mix * mix, axis=1, keepdims=True) + EPS)
            out[rows, cols] = (mix * scale * gain[...]).astype(BF16)
        return carry

    lax.fori_loop(0, blocks, per_block, 0)


def pack_rows(tok_ref, gain_ref, routes_ref, slot_ref, quarter_ref, send, *, experts):
    x = tok_ref[...].astype(F32)
    count, features = x.shape
    width = features // QUARTERS
    scale = lax.rsqrt(jnp.mean(x * x, axis=1, keepdims=True) + EPS)
    normed = (x * scale * gain_ref[...]).astype(BF16)
    routes = routes_ref[...]
    names = iota((experts, count), 0)
    hot = [(routes[k : k + 1, :] == names).astype(F32) for k in range(2)]
    earlier = (iota((count, count), 0) < iota((count, count), 1)).astype(BF16)
    rank = mm((hot[0] + hot[1]).astype(BF16), earlier)
    base = names.astype(F32) * CAP
    dest = [jnp.sum(hot[k] * (rank + base), axis=0, keepdims=True) for k in range(2)]
    slot = slot_ref[...]
    picked = jnp.logical_or(slot == dest[0], slot == dest[1])
    quarter = quarter_ref[...]
    lhs = jnp.concatenate(
        [jnp.where(jnp.logical_and(picked, quarter == q), 1.0, 0.0) for q in range(QUARTERS)],
        axis=1,
    ).astype(BF16)
    rhs = jnp.concatenate([normed[:, q * width : (q + 1) * width] for q in range(QUARTERS)], axis=0)
    send[...] = mm(lhs, rhs).astype(BF16)


def merge_rows(ret_ref, routes_ref, weight_ref, slot_ref, quarter_ref, out, *, experts):
    routes = routes_ref[...]
    count = routes.shape[0]
    names = iota((count, experts), 1)
    hot = [(routes[:, k : k + 1] == names).astype(F32) for k in range(2)]
    earlier = (iota((count, count), 0) > iota((count, count), 1)).astype(BF16)
    rank = mm(earlier, (hot[0] + hot[1]).astype(BF16))
    base = names.astype(F32) * CAP
    slot, quarter = slot_ref[...], quarter_ref[...]
    weight = weight_ref[...]
    rows = ret_ref[...]
    width = rows.shape[1]
    totals = [None] * QUARTERS
    for k in range(2):
        dest = jnp.sum(hot[k] * (rank + base), axis=1, keepdims=True)
        picked = slot == dest
        lhs = jnp.concatenate(
            [jnp.where(jnp.logical_and(picked, quarter == q), 1.0, 0.0) for q in range(QUARTERS)],
            axis=0,
        ).astype(BF16)
        got = mm(lhs, rows)
        for q in range(QUARTERS):
            part = weight[:, k : k + 1] * got[q * count : (q + 1) * count, :]
            totals[q] = part if k == 0 else totals[q] + part
    for q in range(QUARTERS):
        out[:, q * width : (q + 1) * width] = totals[q].astype(BF16)


def expert_kernel(
    send, wg_any, wu_any, wd_any, perm, perm_t, ret,
    rows, parts, relay_l, relay_r, from_l, from_r, total, xt, wg, wu, wd,
    w_sem, zs, zr, xs, xr_l, xr_r, ys, yr, qs, qr, fs, fr, ts, tr,
    *, n_ep, n_tp,
):
    me, t = lax.axis_index("ep"), lax.axis_index("tp")
    n_z = n_ep // 2
    half = n_z // 2
    steps = n_z // 2
    z, c = me // 2, me % 2
    right, left = (t + 1) % n_tp, (t + n_tp - 1) % n_tp
    chunk = send.shape[1]
    width = send.shape[2]

    def offset(b, side):
        o = (steps + 1 - b) % steps
        return o if side == 0 else n_z - o - half * ((steps - o) // steps)

    weights = [
        pltpu.make_async_copy(src.at[0], dst, w_sem.at[i])
        for i, (src, dst) in enumerate(((wg_any, wg), (wu_any, wu), (wd_any, wd)))
    ]
    for copy in weights:
        copy.start()

    barrier = pltpu.get_barrier_semaphore()

    def greet(j, carry):
        pl.semaphore_signal(
            barrier, inc=1, device_id={"ep": (me + j) % n_ep}, device_id_type=MESH
        )
        return carry

    lax.fori_loop(1, n_ep, greet, 0)
    for other in (left, right):
        pl.semaphore_signal(barrier, inc=1, device_id={"tp": other}, device_id_type=MESH)
    pl.semaphore_wait(barrier, n_ep + 1)

    def z_copy(b, side, core):
        other = ((z + offset(b, side)) % n_z) * 2 + core
        return pltpu.make_async_remote_copy(
            src_ref=send.at[other],
            dst_ref=rows.at[0, 4 * b + 2 * side + c],
            send_sem=zs.at[4 * b + 2 * side + core],
            recv_sem=zr.at[4 * b + 2 * side + c],
            device_id={"ep": other},
            device_id_type=MESH,
        )

    def own_in(slot):
        return pltpu.make_async_copy(send.at[me], rows.at[0, slot], zr.at[slot])

    def is_self(b, side, core):
        return jnp.logical_and(jnp.logical_and(b == 1, side == 0), core == c)

    def dispatch(b, carry):
        for side in range(2):
            for core in range(2):
                own = is_self(b, side, core)

                @pl.when(own)
                def _():
                    own_in(4 * b + 2 * side + c).start()

                @pl.when(jnp.logical_not(own))
                def _():
                    z_copy(b, side, core).start()

        return carry

    lax.fori_loop(0, steps, dispatch, 0)

    def x_copy(b, way):
        group = pl.ds(4 * b, 4)
        return pltpu.make_async_remote_copy(
            src_ref=rows.at[0, group],
            dst_ref=rows.at[1 + way, group],
            send_sem=xs.at[way, b],
            recv_sem=(xr_l if way == 0 else xr_r).at[b],
            device_id={"tp": right if way == 0 else left},
            device_id_type=MESH,
        )

    def y_copy(b, way):
        group = pl.ds(4 * b + 2 * way, 2)
        return pltpu.make_async_remote_copy(
            src_ref=rows.at[1 + way, group],
            dst_ref=rows.at[3, group],
            send_sem=ys.at[way, b],
            recv_sem=yr.at[way, b],
            device_id={"tp": right if way == 0 else left},
            device_id_type=MESH,
        )

    def q_copy(b, way):
        return pltpu.make_async_remote_copy(
            src_ref=parts.at[3, pl.ds(4 * b + 2 * way, 2)],
            dst_ref=(relay_l if way == 0 else relay_r).at[pl.ds(2 * b, 2)],
            send_sem=qs.at[way, b],
            recv_sem=qr.at[way, b],
            device_id={"tp": right if way == 0 else left},
            device_id_type=MESH,
        )

    def f_copy(b, way):
        group = pl.ds(4 * b, 4)
        return pltpu.make_async_remote_copy(
            src_ref=parts.at[2 - way, group],
            dst_ref=(from_l if way == 0 else from_r).at[group],
            send_sem=fs.at[way, b],
            recv_sem=fr.at[way, b],
            device_id={"tp": right if way == 0 else left},
            device_id_type=MESH,
        )

    def t_copy(b, side, core):
        other = ((z - offset(b, side) + n_z) % n_z) * 2 + core
        slot = 4 * b + 2 * side + core
        return pltpu.make_async_remote_copy(
            src_ref=total.at[slot],
            dst_ref=ret.at[me],
            send_sem=ts.at[slot],
            recv_sem=tr.at[me],
            device_id={"ep": other},
            device_id_type=MESH,
        )

    def t_arrival(e):
        return pltpu.make_async_copy(total.at[0], ret.at[e], tr.at[e])

    def own_out(slot):
        return pltpu.make_async_copy(total.at[slot], ret.at[me], tr.at[me])

    def arrive(b):
        for k in range(4):
            own_in(4 * b + k).wait()
        x_copy(b, 0).start()
        x_copy(b, 1).start()

    def relay(b):
        for way in range(2):
            x_copy(b, way).wait_recv()
            y_copy(b, way).start()

    def compute(b):
        group = pl.ds(4 * b, 4)
        for way in range(2):
            y_copy(b, way).wait_recv()
        side = perm[...]
        for w in range(4):
            turned = mm(side, rows[w, group].reshape(4 * chunk, width)).astype(BF16)
            for q in range(QUARTERS):
                xt[w * chunk : (w + 1) * chunk, q * width : (q + 1) * width] = turned[
                    q * chunk : (q + 1) * chunk
                ]
        x = xt[...]
        gate = jnp.minimum(mm(x, wg[...]), LIMIT)
        up = jnp.clip(mm(x, wu[...]), -LIMIT, LIMIT)
        hidden = ((up + 1.0) * gate / (1.0 + jnp.exp(-SLOPE * gate))).astype(BF16)
        y = mm(hidden, wd[...]).astype(BF16)
        back = perm_t[...]
        for w in range(4):
            piece = jnp.concatenate(
                [
                    y[w * chunk : (w + 1) * chunk, q * width : (q + 1) * width]
                    for q in range(QUARTERS)
                ],
                axis=0,
            )
            parts[w, group] = mm(back, piece).astype(BF16).reshape(4, chunk, width)

    def start_sum(b):
        for way in range(2):
            q_copy(b, way).start()

    def pass_sum(b):
        for way in range(2):
            q_copy(b, way).wait_recv()
            group = pl.ds(4 * b + 2 * way, 2)
            carried = (relay_l if way == 0 else relay_r)[pl.ds(2 * b, 2)]
            parts[2 - way, group] = (
                parts[2 - way, group].astype(F32) + carried.astype(F32)
            ).astype(BF16)

    def send_sum(b):
        for way in range(2):
            f_copy(b, way).start()

    def finish(b):
        for way in range(2):
            f_copy(b, way).wait_recv()
        group = pl.ds(4 * b, 4)
        total[group] = (
            parts[0, group].astype(F32) + from_l[group].astype(F32) + from_r[group].astype(F32)
        ).astype(BF16)

    def send_back(b):
        for side in range(2):
            for core in range(2):
                own = is_self(b, side, core)

                @pl.when(own)
                def _():
                    own_out(4 * b + 2 * side + core).start()

                @pl.when(jnp.logical_not(own))
                def _():
                    t_copy(b, side, core).start()

    for copy in weights:
        copy.wait()

    def body(i, carry):
        def stage(lag, fn):
            @pl.when(jnp.logical_and(i >= lag, i < steps + lag))
            def _():
                fn(i - lag)

        stage(4, finish)
        stage(3, pass_sum)
        stage(2, compute)
        stage(4, send_back)
        stage(3, send_sum)
        stage(1, relay)
        stage(2, start_sum)
        stage(0, arrive)
        return carry

    lax.fori_loop(0, steps + 4, body, 0)

    def sent(b, carry):
        for way in range(2):
            x_copy(b, way).wait_send()
            y_copy(b, way).wait_send()
            q_copy(b, way).wait_send()
            f_copy(b, way).wait_send()
        for side in range(2):
            for core in range(2):

                @pl.when(jnp.logical_not(is_self(b, side, core)))
                def _():
                    z_copy(b, side, core).wait_send()
                    t_copy(b, side, core).wait_send()

        return carry

    lax.fori_loop(0, steps, sent, 0)

    def returned(e, carry):
        t_arrival(e).wait()
        return carry

    lax.fori_loop(0, n_ep, returned, 0)


def run_experts(send, wg, wu, wd, n_ep, n_tp):
    chunk, width = send.shape[1:]
    group = 4 * chunk
    ff, features = wd.shape[1:]
    source = np.arange(group)
    target = (source % chunk) // CAP * chunk + source // chunk * CAP + source % CAP
    perm = np.zeros((group, group), np.float32)
    perm[target, source] = 1.0
    many = send.shape
    steps = n_ep // 4
    dma = pltpu.SemaphoreType.DMA
    return pl.pallas_call(
        functools.partial(expert_kernel, n_ep=n_ep, n_tp=n_tp),
        out_shape=jax.ShapeDtypeStruct(many, BF16),
        in_specs=[WHOLE, ANYWHERE, ANYWHERE, ANYWHERE, WHOLE, WHOLE],
        out_specs=WHOLE,
        scratch_shapes=[
            VMEM((4, *many), BF16),
            VMEM((4, *many), BF16),
            VMEM((n_ep // 2, chunk, width), BF16),
            VMEM((n_ep // 2, chunk, width), BF16),
            VMEM(many, BF16),
            VMEM(many, BF16),
            VMEM(many, BF16),
            VMEM((group, features), BF16),
            VMEM(wg.shape[1:], BF16),
            VMEM(wu.shape[1:], BF16),
            VMEM(wd.shape[1:], BF16),
            dma((3,)),
            dma((n_ep,)), dma((n_ep,)),
            dma((2, steps)), dma((steps,)), dma((steps,)),
            dma((2, steps)), dma((2, steps)),
            dma((2, steps)), dma((2, steps)),
            dma((2, steps)), dma((2, steps)),
            dma((n_ep,)), dma((n_ep,)),
        ],
        compiler_params=pltpu.CompilerParams(
            collective_id=0, has_side_effects=True, vmem_limit_bytes=56 * 2**20
        ),
        cost_estimate=pl.CostEstimate(
            flops=60_000_000_000, bytes_accessed=10_000_000, transcendentals=0
        ),
        name="experts",
    )(send, wg, wu, wd, jnp.asarray(perm, BF16), jnp.asarray(perm.T, BF16))


def body(
    query, gates, value, margin, position, head_gain, mixer_weight,
    tokens, expert_gain, routes, weights, wg, wu, wd,
):
    n_ep, n_tp = lax.axis_size("ep"), lax.axis_size("tp")
    length, channels = query.shape
    heads, blocks = channels // HC, length // BLK
    count, features = tokens.shape

    states = jax.ShapeDtypeStruct((2, blocks, heads, HC, HC), F32)
    lines = jax.ShapeDtypeStruct((2, blocks, 1, channels), F32)
    streams = jax.ShapeDtypeStruct((2, length, channels), BF16)
    qin, kin, before, off, fin = pl.pallas_call(
        recurrence_states,
        out_shape=(
            streams, streams, states, lines,
            jax.ShapeDtypeStruct((2 * heads, HC + 16, HC), BF16),
        ),
        in_specs=[WHOLE] * 5,
        out_specs=[WHOLE] * 5,
        scratch_shapes=[VMEM(states.shape, F32), VMEM(lines.shape, F32)],
        compiler_params=pltpu.CompilerParams(vmem_limit_bytes=40 * 2**20),
        cost_estimate=pl.CostEstimate(
            flops=2_000_000_000, bytes_accessed=8_000_000, transcendentals=3_000_000
        ),
        name="states",
    )(query, gates, value, margin, jnp.transpose(position))
    every = lax.all_gather(fin, "ep")
    all_weight = lax.all_gather(mixer_weight, "tp")

    chunk = CAP * QUARTERS
    width = features // QUARTERS
    r = np.arange(n_ep * chunk)
    slot = (r // chunk * CAP + r % CAP).astype(np.float32)
    quarter = (r % chunk // CAP).astype(np.int32)
    send = pl.pallas_call(
        functools.partial(pack_rows, experts=n_ep),
        out_shape=jax.ShapeDtypeStruct((n_ep * chunk, width), BF16),
        in_specs=[WHOLE] * 5,
        out_specs=WHOLE,
        compiler_params=pltpu.CompilerParams(vmem_limit_bytes=40 * 2**20),
        name="pack",
    )(
        tokens, expert_gain[None, :], jnp.transpose(routes),
        jnp.asarray(slot[:, None]), jnp.asarray(quarter[:, None]),
    )
    ret = run_experts(send.reshape(n_ep, chunk, width), wg, wu, wd, n_ep, n_tp)
    ret, every, all_weight = lax.optimization_barrier((ret, every, all_weight))
    moe_out = pl.pallas_call(
        functools.partial(merge_rows, experts=n_ep),
        out_shape=jax.ShapeDtypeStruct((count, features), BF16),
        in_specs=[WHOLE] * 5,
        out_specs=WHOLE,
        compiler_params=pltpu.CompilerParams(vmem_limit_bytes=40 * 2**20),
        name="merge",
    )(
        ret.reshape(n_ep * chunk, width), routes, weights,
        jnp.asarray(slot[None, :]), jnp.asarray(quarter[None, :]),
    )

    heads_out = pl.pallas_call(
        recurrence_outputs,
        out_shape=jax.ShapeDtypeStruct((length, channels), BF16),
        in_specs=[WHOLE] * 6 + [pl.BlockSpec(memory_space=pltpu.SMEM), WHOLE],
        out_specs=WHOLE,
        scratch_shapes=[VMEM((2 * heads, HC, HC), F32)],
        compiler_params=pltpu.CompilerParams(vmem_limit_bytes=40 * 2**20),
        cost_estimate=pl.CostEstimate(
            flops=2_000_000_000, bytes_accessed=12_000_000, transcendentals=100_000
        ),
        name="outputs",
    )(qin, kin, value, before, off, every, lax.axis_index("ep")[None], head_gain[None, :])
    mine = lax.all_to_all(
        heads_out.reshape(n_tp, length // n_tp, channels), "tp", 0, 0, tiled=True
    )
    mixed = jnp.zeros((length // n_tp, features), F32)
    for g in range(n_tp):
        mixed = mixed + mm(mine[g], all_weight[g]).astype(BF16).astype(F32)
    return mixed.astype(BF16), moe_out


def solution(mesh):
    rows = P(("grp", "ep"), "tp")
    split = P(("grp", "ep", "tp"), None)
    return jax.shard_map(
        body,
        mesh=mesh,
        in_specs=(
            rows, rows, rows, P(None, "tp"), P("tp", ("grp", "ep")), P(), P("tp", None),
            split, P(), split, split,
            P("ep", None, "tp"), P("ep", None, "tp"), P("ep", "tp", None),
        ),
        out_specs=(split, split),
        check_vma=False,
    )
```

```python
import functools

import jax
import jax.numpy as jnp
from jax import lax
from jax.experimental import pallas as pl
from jax.experimental.pallas import tpu as pltpu
from jax.sharding import PartitionSpec as P

F32, BF16 = jnp.float32, jnp.bfloat16
HC = 128
BLK = 128
CAP = 12
QUARTERS = 4
EPS = 1e-06
LIMIT = 7.0
SLOPE = 1.702
VMEM = pltpu.VMEM
MESH = pl.DeviceIdType.MESH
WHOLE = pl.BlockSpec(memory_space=VMEM)
SLAB = 16
ANYWHERE = pl.BlockSpec(memory_space=pl.ANY)


def mm(a, b):
    return jnp.dot(a, b, preferred_element_type=F32)


def mm_t(a, b):
    return lax.dot_general(a, b, (((1,), (1,)), ((), ())), preferred_element_type=F32)


def t_mm(a, b):
    return lax.dot_general(a, b, (((0,), (0,)), ((), ())), preferred_element_type=F32)


def iota(shape, dim):
    return lax.broadcasted_iota(jnp.int32, shape, dim)


def logistic(x):
    return 1.0 / (1.0 + jnp.exp(-x))


def recurrence_states(q_ref, g_ref, v_ref, margin_ref, pos_ref, qin, kin, before, off, fin, inc, last):
    blocks = q_ref.shape[0] // BLK
    heads = q_ref.shape[1] // HC
    row, col = iota((BLK, BLK), 0), iota((BLK, BLK), 1)
    keep = (row >= col, row <= col)
    tri = [k.astype(BF16) for k in keep]
    ends = [jnp.exp(margin_ref[d : d + 1, :]) for d in range(2)]

    def per_block(n, carry):
        rows = pl.ds(pl.multiple_of(n * BLK, BLK), BLK)
        q = q_ref[rows, :].astype(F32)
        q = q * logistic(q) * HC**-0.5
        shut = logistic(-g_ref[rows, :].astype(F32))
        values = v_ref[rows, :]
        pos = pos_ref[:, rows]
        for d in range(2):
            k = ends[d] * shut
            logs = jnp.log1p(-k)
            high = logs.astype(BF16)
            low = (logs - high.astype(F32)).astype(BF16)
            added = jnp.concatenate(
                [
                    jnp.broadcast_to(
                        jnp.sum(
                            jnp.where(keep[d], pos[h : h + 1, :], 0.0), axis=1, keepdims=True
                        ),
                        (BLK, HC),
                    )
                    for h in range(heads)
                ],
                axis=1,
            )
            cum = mm(tri[d], high) + mm(tri[d], low) + added
            end = cum[BLK - 1 :, :] if d == 0 else cum[:1, :]
            qin[d, rows, :] = (q * jnp.exp(cum)).astype(BF16)
            kin[d, rows, :] = (k * jnp.exp(-cum)).astype(BF16)
            ks = (k * jnp.exp(end - cum)).astype(BF16)
            last[d, n] = end
            for h in range(heads):
                cols = slice(h * HC, (h + 1) * HC)
                inc[d, n, h] = t_mm(values[:, cols], ks[:, cols])
        return carry

    lax.fori_loop(0, blocks, per_block, 0)
    for d in range(2):

        def chain(i, carry):
            n = i if d == 0 else blocks - 1 - i
            offset, states = carry
            off[d, n] = offset
            end = last[d, n]
            decay = jnp.exp(end)
            new = []
            for h in range(heads):
                before[d, n, h] = states[h]
                new.append(states[h] * decay[:, h * HC : (h + 1) * HC] + inc[d, n, h])
            return offset + end, tuple(new)

        zero = tuple(jnp.zeros((HC, HC), F32) for _ in range(heads))
        total, states = lax.fori_loop(0, blocks, chain, (jnp.zeros((1, heads * HC), F32), zero))
        decay = jnp.exp(total)
        for h in range(heads):
            put_state(fin, (0, d * heads + h), states[h], decay[:, h * HC : (h + 1) * HC])


def put_state(ref, at, state, decay):
    slab = iota((SLAB, HC), 0)
    high = decay.astype(BF16).astype(F32)
    ref[(*at, slice(0, HC))] = state.astype(BF16)
    ref[(*at, slice(HC, HC + SLAB))] = jnp.where(
        slab == 0, high, jnp.where(slab == 1, decay - high, 0.0)
    ).astype(BF16)


def get_state(ref, at):
    state = ref[(*at, slice(0, HC))].astype(F32)
    decay = jnp.sum(ref[(*at, slice(HC, HC + SLAB))].astype(F32), axis=0, keepdims=True)
    return state, decay


def recurrence_outputs(qin, kin, v_ref, before, off, entering, gain, out):
    blocks = v_ref.shape[0] // BLK
    heads = v_ref.shape[1] // HC
    per = out.shape[1] // BLK
    row, col = iota((BLK, BLK), 0), iota((BLK, BLK), 1)

    def per_block(n, carry):
        rows = pl.ds(pl.multiple_of(n * BLK, BLK), BLK)
        for h in range(heads):
            cols = slice(h * HC, (h + 1) * HC)
            scores, outer = [], None
            for d in range(2):
                q = qin[d, rows, cols]
                scores.append(mm_t(q, kin[d, rows, cols]))
                state = before[d, n, h] + entering[d * heads + h] * jnp.exp(off[d, n, :, cols])
                part = mm_t(q, state.astype(BF16))
                outer = part if outer is None else outer + part
            both = jnp.where(row >= col, scores[0], 0.0) + jnp.where(row <= col, scores[1], 0.0)
            mix = mm(both.astype(BF16), v_ref[rows, cols]) + outer
            scale = lax.rsqrt(jnp.mean(mix * mix, axis=1, keepdims=True) + EPS)
            inside = pl.ds(pl.multiple_of(n % per * BLK, BLK), BLK)
            out[n // per, inside, cols] = (mix * scale * gain[...]).astype(BF16)
        return carry

    lax.fori_loop(0, blocks, per_block, 0)


def chunk_places(shape, dim):
    at = iota(shape, dim)
    piece = sum((at >= q * CAP).astype(jnp.int32) for q in range(1, QUARTERS))
    return at - piece * CAP, piece


def pack_rows(tok_ref, gain_ref, routes_ref, send):
    x = tok_ref[...].astype(F32)
    count, features = x.shape
    experts, chunk, width = send.shape
    scale = lax.rsqrt(jnp.mean(x * x, axis=1, keepdims=True) + EPS)
    normed = (x * scale * gain_ref[...]).astype(BF16)
    eye = iota((count, count), 0) == iota((count, count), 1)
    routes = routes_ref[...]
    names = iota((experts, count), 0)
    hot = []
    for k in range(2):
        line = jnp.sum(jnp.where(eye, routes[:, k : k + 1].astype(F32), 0.0), axis=0, keepdims=True)
        hot.append((line == names.astype(F32)).astype(F32))
    earlier = (iota((count, count), 0) < iota((count, count), 1)).astype(BF16)
    rank = mm((hot[0] + hot[1]).astype(BF16), earlier)
    base = names.astype(F32) * CAP
    dest = [jnp.sum(hot[k] * (rank + base), axis=0, keepdims=True) for k in range(2)]
    inner, piece = chunk_places((experts, chunk, 1), 1)
    slot = (iota((experts, chunk, 1), 0) * CAP + inner).astype(F32).reshape(experts * chunk, 1)
    piece = piece.reshape(experts * chunk, 1)
    picked = jnp.logical_or(slot == dest[0], slot == dest[1])
    lhs = jnp.concatenate(
        [jnp.where(jnp.logical_and(picked, piece == q), 1.0, 0.0) for q in range(QUARTERS)],
        axis=1,
    ).astype(BF16)
    rhs = jnp.concatenate([normed[:, q * width : (q + 1) * width] for q in range(QUARTERS)], axis=0)
    send[...] = mm(lhs, rhs).astype(BF16).reshape(experts, chunk, width)


def merge_places(routes_ref, lhs, experts, chunk):
    routes = routes_ref[...]
    count = routes.shape[0]
    names = iota((count, experts), 1)
    hot = [(routes[:, k : k + 1] == names).astype(F32) for k in range(2)]
    earlier = (iota((count, count), 0) > iota((count, count), 1)).astype(BF16)
    rank = mm(earlier, (hot[0] + hot[1]).astype(BF16))
    base = names.astype(F32) * CAP
    r = iota((1, experts * chunk), 1).astype(F32)
    expert = jnp.floor((r + 0.5) / chunk)
    rest = r - expert * chunk
    piece = jnp.floor((rest + 0.5) / CAP)
    slot = expert * CAP + rest - piece * CAP
    for k in range(2):
        dest = jnp.sum(hot[k] * (rank + base), axis=1, keepdims=True)
        picked = slot == dest
        for q in range(QUARTERS):
            at = (k * QUARTERS + q) * count
            lhs[at : at + count, :] = jnp.where(
                jnp.logical_and(picked, piece == q), 1.0, 0.0
            ).astype(BF16)


def merge_rows(lhs, ret, weight_ref, out):
    experts, chunk, width = ret.shape
    weight = weight_ref[...]
    count = weight.shape[0]
    rows = ret[...].reshape(experts * chunk, width)
    for q in range(QUARTERS):
        total = None
        for k in range(2):
            at = (k * QUARTERS + q) * count
            part = weight[:, k : k + 1] * mm(lhs[at : at + count, :], rows)
            total = part if total is None else total + part
        out[:, q * width : (q + 1) * width] = total.astype(BF16)


def kernel(
    query, gates, value, margin, position, head_gain, mixer_w, tokens, expert_gain,
    routes, token_w, wg_any, wu_any, wd_any, mixed, merged,
    q_v, g_v, v_v, margin_v, pos_v, hgain_v, tok_v, egain_v, routes_v, token_w_v, wg, wu, wd,
    w_all, qin, kin, before, off, inc, last, fin, near, far, group_state, chip_in, entering,
    heads_out, heads_in, send, rows, parts, relay_l, relay_r, from_l, from_r, total, ret,
    xt, perm, lhs,
    in_sem, zs, zr, xs, xr_l, xr_r, ys, yr, qs, qr, fs, fr, ts, tr,
    mate_s, mate_r, near_s, near_r, far_s, far_r, chip_s, chip_r,
    ws, wr, wys, wyr, wms, wmr, hs, hr,
    *, n_ep, n_tp,
):
    me, t = lax.axis_index("ep"), lax.axis_index("tp")
    n_z = n_ep // 2
    half = n_z // 2
    steps = n_z // 2
    z, c = me // 2, me % 2
    mate = 2 * z + 1 - c
    right, left = (t + 1) % n_tp, (t + n_tp - 1) % n_tp
    opposite = (t + 2) % n_tp
    chunk, width = send.shape[1:]
    heads = v_v.shape[1] // HC

    def offset(b, side):
        o = (steps + 1 - b) % steps
        return o if side == 0 else n_z - o - half * ((steps - o) // steps)

    loads = [
        pltpu.make_async_copy(src, dst, in_sem.at[i])
        for i, (src, dst) in enumerate(
            (
                (tokens, tok_v), (expert_gain, egain_v), (routes, routes_v), (token_w, token_w_v),
                (mixer_w, w_all.at[0]), (query, q_v), (gates, g_v), (value, v_v),
                (margin, margin_v), (position, pos_v), (head_gain, hgain_v),
                (wg_any.at[0], wg), (wu_any.at[0], wu), (wd_any.at[0], wd),
            )
        )
    ]
    for copy in loads:
        copy.start()

    barrier = pltpu.get_barrier_semaphore()

    def greet(j, carry):
        pl.semaphore_signal(
            barrier, inc=1, device_id={"ep": (me + j) % n_ep}, device_id_type=MESH
        )
        return carry

    lax.fori_loop(1, n_ep, greet, 0)
    for other in (left, right, opposite):
        pl.semaphore_signal(barrier, inc=1, device_id={"tp": other}, device_id_type=MESH)
    for copy in loads[:4]:
        copy.wait()
    pack_rows(tok_v, egain_v, routes_v, send)
    size = perm.shape[0]
    row, col = iota((size, size), 0), iota((size, size), 1)
    major = sum((row >= k * chunk).astype(jnp.int32) for k in range(1, 4))
    rest = row - major * chunk
    minor = sum((rest >= k * CAP).astype(jnp.int32) for k in range(1, 4))
    target = minor * chunk + major * CAP + (rest - minor * CAP)
    perm[...] = jnp.where(col == target, 1.0, 0.0).astype(BF16)
    pl.semaphore_wait(barrier, n_ep + n_tp - 2)

    def z_copy(b, side, core):
        other = ((z + offset(b, side)) % n_z) * 2 + core
        return pltpu.make_async_remote_copy(
            src_ref=send.at[other],
            dst_ref=rows.at[0, 4 * b + 2 * side + c],
            send_sem=zs.at[4 * b + 2 * side + core],
            recv_sem=zr.at[4 * b + 2 * side + c],
            device_id={"ep": other},
            device_id_type=MESH,
        )

    def own_in(slot):
        return pltpu.make_async_copy(send.at[me], rows.at[0, slot], zr.at[slot])

    def is_self(b, side, core):
        return jnp.logical_and(jnp.logical_and(b == 1, side == 0), core == c)

    def dispatch(b, carry):
        for side in range(2):
            for core in range(2):
                own = is_self(b, side, core)

                @pl.when(own)
                def _():
                    own_in(4 * b + 2 * side + c).start()

                @pl.when(jnp.logical_not(own))
                def _():
                    z_copy(b, side, core).start()

        return carry

    def x_copy(b, way):
        group = pl.ds(4 * b, 4)
        return pltpu.make_async_remote_copy(
            src_ref=rows.at[0, group],
            dst_ref=rows.at[1 + way, group],
            send_sem=xs.at[way, b],
            recv_sem=(xr_l if way == 0 else xr_r).at[b],
            device_id={"tp": right if way == 0 else left},
            device_id_type=MESH,
        )

    def y_copy(b, way):
        group = pl.ds(4 * b + 2 * way, 2)
        return pltpu.make_async_remote_copy(
            src_ref=rows.at[1 + way, group],
            dst_ref=rows.at[3, group],
            send_sem=ys.at[way, b],
            recv_sem=yr.at[way, b],
            device_id={"tp": right if way == 0 else left},
            device_id_type=MESH,
        )

    def q_copy(b, way):
        return pltpu.make_async_remote_copy(
            src_ref=parts.at[3, pl.ds(4 * b + 2 * way, 2)],
            dst_ref=(relay_l if way == 0 else relay_r).at[pl.ds(2 * b, 2)],
            send_sem=qs.at[way, b],
            recv_sem=qr.at[way, b],
            device_id={"tp": right if way == 0 else left},
            device_id_type=MESH,
        )

    def f_copy(b, way):
        group = pl.ds(4 * b, 4)
        return pltpu.make_async_remote_copy(
            src_ref=parts.at[2 - way, group],
            dst_ref=(from_l if way == 0 else from_r).at[group],
            send_sem=fs.at[way, b],
            recv_sem=fr.at[way, b],
            device_id={"tp": right if way == 0 else left},
            device_id_type=MESH,
        )

    def t_copy(b, side, core):
        other = ((z - offset(b, side) + n_z) % n_z) * 2 + core
        slot = 4 * b + 2 * side + core
        return pltpu.make_async_remote_copy(
            src_ref=total.at[slot],
            dst_ref=ret.at[me],
            send_sem=ts.at[slot],
            recv_sem=tr.at[me],
            device_id={"ep": other},
            device_id_type=MESH,
        )

    def t_arrival(e):
        return pltpu.make_async_copy(total.at[0], ret.at[e], tr.at[e])

    def own_out(slot):
        return pltpu.make_async_copy(total.at[slot], ret.at[me], tr.at[me])

    def arrive(b):
        for k in range(4):
            own_in(4 * b + k).wait()
        x_copy(b, 0).start()
        x_copy(b, 1).start()

    def relay(b):
        for way in range(2):
            x_copy(b, way).wait_recv()
            y_copy(b, way).start()

    def compute(b):
        group = pl.ds(4 * b, 4)
        for way in range(2):
            y_copy(b, way).wait_recv()
        turn = perm[...]
        for w in range(4):
            turned = mm(turn, rows[w, group].reshape(4 * chunk, width)).astype(BF16)
            for q in range(QUARTERS):
                xt[w * chunk : (w + 1) * chunk, q * width : (q + 1) * width] = turned[
                    q * chunk : (q + 1) * chunk
                ]
        x = xt[...]
        gate = jnp.minimum(mm(x, wg[...]), LIMIT)
        up = jnp.clip(mm(x, wu[...]), -LIMIT, LIMIT)
        hidden = ((up + 1.0) * gate / (1.0 + jnp.exp(-SLOPE * gate))).astype(BF16)
        y = mm(hidden, wd[...]).astype(BF16)
        for w in range(4):
            piece = jnp.concatenate(
                [
                    y[w * chunk : (w + 1) * chunk, q * width : (q + 1) * width]
                    for q in range(QUARTERS)
                ],
                axis=0,
            )
            parts[w, group] = mm(turn, piece).astype(BF16).reshape(4, chunk, width)

    def start_sum(b):
        for way in range(2):
            q_copy(b, way).start()

    def pass_sum(b):
        for way in range(2):
            q_copy(b, way).wait_recv()
            group = pl.ds(4 * b + 2 * way, 2)
            carried = (relay_l if way == 0 else relay_r)[pl.ds(2 * b, 2)]
            parts[2 - way, group] = (
                parts[2 - way, group].astype(F32) + carried.astype(F32)
            ).astype(BF16)

    def send_sum(b):
        for way in range(2):
            f_copy(b, way).start()

    def finish(b):
        for way in range(2):
            f_copy(b, way).wait_recv()
        group = pl.ds(4 * b, 4)
        total[group] = (
            parts[0, group].astype(F32) + from_l[group].astype(F32) + from_r[group].astype(F32)
        ).astype(BF16)

    def send_back(b):
        for side in range(2):
            for core in range(2):
                own = is_self(b, side, core)

                @pl.when(own)
                def _():
                    own_out(4 * b + 2 * side + core).start()

                @pl.when(jnp.logical_not(own))
                def _():
                    t_copy(b, side, core).start()


    def w_part(who, core, lo, hi):
        size = w_all.shape[1] // 2
        first = core * size + lo * (size // 2)
        return w_all.at[who, pl.ds(pl.multiple_of(first, size // 2), (hi - lo) * (size // 2))]

    def w_copy(way):
        return pltpu.make_async_remote_copy(
            src_ref=w_part(0, c, 0, 2),
            dst_ref=w_part(1 + way, c, 0, 2),
            send_sem=ws.at[way],
            recv_sem=wr.at[way],
            device_id={"tp": right if way == 0 else left},
            device_id_type=MESH,
        )

    def w_relay(way):
        return pltpu.make_async_remote_copy(
            src_ref=w_part(1 + way, c, way, way + 1),
            dst_ref=w_part(3, c, way, way + 1),
            send_sem=wys.at[way],
            recv_sem=wyr.at[way],
            device_id={"tp": right if way == 0 else left},
            device_id_type=MESH,
        )

    def w_mate(who, core):
        return pltpu.make_async_remote_copy(
            src_ref=w_part(who, core, 0, 2),
            dst_ref=w_part(who, core, 0, 2),
            send_sem=wms.at[who],
            recv_sem=wmr.at[who],
            device_id={"ep": mate},
            device_id_type=MESH,
        )

    p, g = z % 4, z // 4

    def mate_copy():
        return pltpu.make_async_remote_copy(
            src_ref=fin.at[0], dst_ref=fin.at[1], send_sem=mate_s, recv_sem=mate_r,
            device_id={"ep": mate}, device_id_type=MESH,
        )

    def near_copy(s):
        return pltpu.make_async_remote_copy(
            src_ref=near.at[0], dst_ref=near.at[s], send_sem=near_s.at[s], recv_sem=near_r.at[s],
            device_id={"ep": (g * 4 + (p + s) % 4) * 2 + c}, device_id_type=MESH,
        )

    def far_copy(d, s):
        other = (z + 4 * s) % n_z if d == 0 else (z - 4 * s + n_z) % n_z
        return pltpu.make_async_remote_copy(
            src_ref=group_state.at[d], dst_ref=far.at[d, s],
            send_sem=far_s.at[d, s], recv_sem=far_r.at[d, s],
            device_id={"ep": other * 2 + c}, device_id_type=MESH,
        )

    def sends_far(d, s):
        return g + s < n_z // 4 if d == 0 else g >= s

    def hears_far(d, s):
        return g >= s if d == 0 else g + s < n_z // 4

    def chip_copy():
        return pltpu.make_async_remote_copy(
            src_ref=chip_in.at[0], dst_ref=chip_in.at[1], send_sem=chip_s, recv_sem=chip_r,
            device_id={"ep": mate}, device_id_type=MESH,
        )

    def share_chip():
        mate_copy().wait_recv()
        for d in range(2):
            at = d * heads + c
            first, first_decay = get_state(fin, (c if d == 0 else 1 - c, at))
            second, second_decay = get_state(fin, (1 - c if d == 0 else c, at))
            put_state(near, (0, d), first * second_decay + second, first_decay * second_decay)

    def send_chip():
        for s in range(1, 4):
            near_copy(s).start()

    def share_group():
        for s in range(1, 4):
            near_copy(s).wait_recv()
        for d in range(2):
            zero, one = jnp.zeros((HC, HC), F32), jnp.ones((1, HC), F32)
            inside, inside_decay, whole, whole_decay = zero, one, zero, one
            for m in range(4) if d == 0 else range(3, -1, -1):
                state, decay = get_state(near, ((p - m + 4) % 4, d))
                passed = (m < p) if d == 0 else (m > p)
                inside = jnp.where(passed, inside * decay + state, inside)
                inside_decay = jnp.where(passed, inside_decay * decay, inside_decay)
                whole, whole_decay = whole * decay + state, whole_decay * decay
            put_state(group_state, (d,), whole, whole_decay)
            entering[2 * d] = inside
            entering[2 * d + 1, 0:8] = jnp.broadcast_to(inside_decay, (8, HC))
        for d in range(2):
            for s in range(1, n_z // 4):

                @pl.when(sends_far(d, s))
                def _():
                    far_copy(d, s).start()

    def share_all():
        for d in range(2):
            inside, inside_decay = entering[2 * d], entering[2 * d + 1, 0:1]
            entering[2 * d + 1] = jnp.zeros((HC, HC), F32)
            for s in range(n_z // 4 - 1, 0, -1):

                @pl.when(hears_far(d, s))
                def _():
                    far_copy(d, s).wait_recv()
                    state, decay = get_state(far, (d, s))
                    entering[2 * d + 1] = entering[2 * d + 1] * decay + state

            chip_in[0, d] = (entering[2 * d + 1] * inside_decay + inside).astype(BF16)
        chip_copy().start()

    def enter():
        chip_copy().wait_recv()
        for d in range(2):
            for h in range(heads):
                at = d * heads + h
                state = chip_in[(h + c) % 2, d].astype(F32)
                other, decay = get_state(fin, (1, at))
                passed = (c == 1) if d == 0 else (c == 0)
                entering[at] = jnp.where(passed, state * decay + other, state)

    def head_copy(k):
        to = (right, left, opposite)[k]
        return pltpu.make_async_remote_copy(
            src_ref=heads_out.at[to], dst_ref=heads_in.at[k],
            send_sem=hs.at[k], recv_sem=hr.at[k],
            device_id={"tp": to}, device_id_type=MESH,
        )

    ahead = 3
    lax.fori_loop(0, ahead, dispatch, 0)
    for copy in loads[4:]:
        copy.wait()
    w_copy(0).start()
    w_copy(1).start()
    recurrence_states(q_v, g_v, v_v, margin_v, pos_v, qin, kin, before, off, fin, inc, last)
    mate_copy().start()

    def body(i, carry):
        def stage(lag, fn, until=steps):
            @pl.when(jnp.logical_and(i >= lag, i < until + lag))
            def _():
                fn(i - lag)

        def once(at, fn):
            @pl.when(i == at)
            def _():
                fn()

        def relay_weights():
            for way in range(2):
                w_copy(way).wait_recv()
                w_relay(way).start()

        def pair_weights():
            for way in range(2):
                w_relay(way).wait_recv()
            for who in range(1, 4):
                w_mate(who, c).start()

        stage(4, finish)
        stage(3, pass_sum)
        stage(2, compute)
        stage(4, send_back)
        stage(3, send_sum)
        stage(1, relay)
        stage(2, start_sum)
        once(0, share_chip)
        stage(0, arrive)
        once(0, send_chip)
        once(1, relay_weights)
        once(3, share_group)
        stage(0, lambda b: dispatch(b + ahead, 0), steps - ahead)
        once(4, pair_weights)
        once(6, share_all)
        return carry

    lax.fori_loop(0, steps + 4, body, 0)

    enter()
    recurrence_outputs(qin, kin, v_v, before, off, entering, hgain_v, heads_out)
    for k in range(3):
        head_copy(k).start()
    merge_places(routes_v, lhs, n_ep, chunk)
    for who in range(1, 4):
        w_mate(who, 1 - c).wait_recv()
    for k in range(3):
        head_copy(k).wait_recv()
    span = mixed.shape[1] // 4
    for k in range(4):
        cols = slice(k * span, (k + 1) * span)
        acc = None
        for who in range(4):
            own = heads_out[t] if who == 0 else heads_in[who - 1]
            part = mm(own, w_all[who, :, cols]).astype(BF16).astype(F32)
            acc = part if acc is None else acc + part
        mixed[:, cols] = acc.astype(BF16)

    def returned(e, carry):
        t_arrival(e).wait()
        return carry

    lax.fori_loop(0, n_ep, returned, 0)
    merge_rows(lhs, ret, token_w_v, merged)

    def sent(b, carry):
        for way in range(2):
            x_copy(b, way).wait_send()
            y_copy(b, way).wait_send()
            q_copy(b, way).wait_send()
            f_copy(b, way).wait_send()
        for side in range(2):
            for core in range(2):

                @pl.when(jnp.logical_not(is_self(b, side, core)))
                def _():
                    z_copy(b, side, core).wait_send()
                    t_copy(b, side, core).wait_send()

        return carry

    lax.fori_loop(0, steps, sent, 0)
    for way in range(2):
        w_copy(way).wait_send()
        w_relay(way).wait_send()
    for s in range(1, 4):
        w_mate(s, c).wait_send()
        near_copy(s).wait_send()
    for d in range(2):
        for s in range(1, n_z // 4):

            @pl.when(sends_far(d, s))
            def _():
                far_copy(d, s).wait_send()

    mate_copy().wait_send()
    chip_copy().wait_send()
    for k in range(3):
        head_copy(k).wait_send()


def body(*args):
    (query, gates, value, margin, position, head_gain, mixer_w, tokens, expert_gain,
     routes, token_w, wg, wu, wd) = args
    n_ep, n_tp = lax.axis_size("ep"), lax.axis_size("tp")
    length, channels = query.shape
    heads, blocks = channels // HC, length // BLK
    count, features = tokens.shape
    chunk, width = CAP * QUARTERS, features // QUARTERS
    many = (n_ep, chunk, width)
    half_many = (n_ep // 2, chunk, width)
    steps = n_ep // 4
    group = 4 * chunk
    dma = pltpu.SemaphoreType.DMA
    operands = (
        query, gates, value, margin, position, head_gain[None, :], mixer_w, tokens,
        expert_gain[None, :], routes, token_w, wg, wu, wd,
    )

    def like(x):
        return VMEM(x.shape, x.dtype)

    per_block = (2, blocks, heads, HC, HC)
    lines = (2, blocks, 1, channels)
    state = (HC + SLAB, HC)
    mixed, merged = pl.pallas_call(
        functools.partial(kernel, n_ep=n_ep, n_tp=n_tp),
        out_shape=(
            jax.ShapeDtypeStruct((length // n_tp, features), BF16),
            jax.ShapeDtypeStruct((count, features), BF16),
        ),
        in_specs=[ANYWHERE] * len(operands),
        out_specs=(WHOLE, WHOLE),
        scratch_shapes=[
            like(query), like(gates), like(value), like(margin), like(position),
            like(operands[5]), like(tokens), like(operands[8]), like(routes), like(token_w),
            VMEM(wg.shape[1:], BF16), VMEM(wu.shape[1:], BF16), VMEM(wd.shape[1:], BF16),
            VMEM((n_tp, *mixer_w.shape), BF16),
            VMEM((2, length, channels), BF16), VMEM((2, length, channels), BF16),
            VMEM(per_block, F32), VMEM(lines, F32), VMEM(per_block, F32), VMEM(lines, F32),
            VMEM((2, 2 * heads, *state), BF16),
            VMEM((4, 2, *state), BF16), VMEM((2, 4, *state), BF16), VMEM((2, *state), BF16),
            VMEM((2, 2, HC, HC), BF16), VMEM((2 * heads, HC, HC), F32),
            VMEM((n_tp, length // n_tp, channels), BF16),
            VMEM((3, length // n_tp, channels), BF16),
            VMEM(many, BF16), VMEM((4, *many), BF16), VMEM((4, *many), BF16),
            VMEM(half_many, BF16), VMEM(half_many, BF16),
            VMEM(many, BF16), VMEM(many, BF16), VMEM(many, BF16), VMEM(many, BF16),
            VMEM((group, features), BF16), VMEM((group, group), BF16),
            VMEM((2 * QUARTERS * count, n_ep * chunk), BF16),
            dma((len(operands),)),
            dma((n_ep,)), dma((n_ep,)),
            dma((2, steps)), dma((steps,)), dma((steps,)),
            dma((2, steps)), dma((2, steps)),
            dma((2, steps)), dma((2, steps)),
            dma((2, steps)), dma((2, steps)),
            dma((n_ep,)), dma((n_ep,)),
            dma(()), dma(()), dma((4,)), dma((4,)), dma((2, 4)), dma((2, 4)), dma(()), dma(()),
            dma((2,)), dma((2,)), dma((2,)), dma((2,)), dma((4,)), dma((4,)),
            dma((3,)), dma((3,)),
        ],
        compiler_params=pltpu.CompilerParams(
            collective_id=0, has_side_effects=True, vmem_limit_bytes=62 * 2**20
        ),
        name="whole",
    )(*operands)
    return mixed, merged


def solution(mesh):
    rows = P(("grp", "ep"), "tp")
    split = P(("grp", "ep", "tp"), None)
    return jax.shard_map(
        body,
        mesh=mesh,
        in_specs=(
            rows, rows, rows, P(None, "tp"), P("tp", ("grp", "ep")), P(), P("tp", None),
            split, P(), split, split,
            P("ep", None, "tp"), P("ep", None, "tp"), P("ep", "tp", None),
        ),
        out_specs=(split, split),
        check_vma=False,
    )
```

```python
import functools

import jax
import jax.numpy as jnp
from jax import lax
from jax.experimental import pallas as pl
from jax.experimental.pallas import tpu as pltpu
from jax.sharding import PartitionSpec as P

F32, BF16 = jnp.float32, jnp.bfloat16
HC = 128
BLK = 128
CAP = 12
QUARTERS = 4
EPS = 1e-06
LIMIT = 7.0
SLOPE = 1.702
VMEM = pltpu.VMEM
MESH = pl.DeviceIdType.MESH
WHOLE = pl.BlockSpec(memory_space=VMEM)
SLAB = 16
ANYWHERE = pl.BlockSpec(memory_space=pl.ANY)


def mm(a, b):
    return jnp.dot(a, b, preferred_element_type=F32)


def mm_t(a, b):
    return lax.dot_general(a, b, (((1,), (1,)), ((), ())), preferred_element_type=F32)


def t_mm(a, b):
    return lax.dot_general(a, b, (((0,), (0,)), ((), ())), preferred_element_type=F32)


def iota(shape, dim):
    return lax.broadcasted_iota(jnp.int32, shape, dim)


def logistic(x):
    return 1.0 / (1.0 + jnp.exp(-x))


def recurrence_states(q_ref, g_ref, v_ref, margin_ref, pos_ref, qin, kin, before, off, fin, inc, last):
    blocks = q_ref.shape[0] // BLK
    heads = q_ref.shape[1] // HC
    row, col = iota((BLK, BLK), 0), iota((BLK, BLK), 1)
    keep = (row >= col, row <= col)
    tri = [k.astype(BF16) for k in keep]
    ends = [jnp.exp(margin_ref[d : d + 1, :]) for d in range(2)]

    def per_block(n, carry):
        rows = pl.ds(pl.multiple_of(n * BLK, BLK), BLK)
        q = q_ref[rows, :].astype(F32)
        q = q * logistic(q) * HC**-0.5
        shut = logistic(-g_ref[rows, :].astype(F32))
        values = v_ref[rows, :]
        pos = pos_ref[:, rows]
        for d in range(2):
            k = ends[d] * shut
            logs = jnp.log1p(-k)
            high = logs.astype(BF16)
            low = (logs - high.astype(F32)).astype(BF16)
            added = jnp.concatenate(
                [
                    jnp.broadcast_to(
                        jnp.sum(
                            jnp.where(keep[d], pos[h : h + 1, :], 0.0), axis=1, keepdims=True
                        ),
                        (BLK, HC),
                    )
                    for h in range(heads)
                ],
                axis=1,
            )
            cum = mm(tri[d], high) + mm(tri[d], low) + added
            end = cum[BLK - 1 :, :] if d == 0 else cum[:1, :]
            qin[d, rows, :] = (q * jnp.exp(cum)).astype(BF16)
            kin[d, rows, :] = (k * jnp.exp(-cum)).astype(BF16)
            ks = (k * jnp.exp(end - cum)).astype(BF16)
            last[d, n] = end
            for h in range(heads):
                cols = slice(h * HC, (h + 1) * HC)
                inc[d, n, h] = t_mm(values[:, cols], ks[:, cols])
        return carry

    lax.fori_loop(0, blocks, per_block, 0)
    for d in range(2):

        def chain(i, carry):
            n = i if d == 0 else blocks - 1 - i
            offset, states = carry
            off[d, n] = offset
            end = last[d, n]
            decay = jnp.exp(end)
            new = []
            for h in range(heads):
                before[d, n, h] = states[h]
                new.append(states[h] * decay[:, h * HC : (h + 1) * HC] + inc[d, n, h])
            return offset + end, tuple(new)

        zero = tuple(jnp.zeros((HC, HC), F32) for _ in range(heads))
        total, states = lax.fori_loop(0, blocks, chain, (jnp.zeros((1, heads * HC), F32), zero))
        decay = jnp.exp(total)
        for h in range(heads):
            put_state(fin, (0, d * heads + h), states[h], decay[:, h * HC : (h + 1) * HC])


def put_state(ref, at, state, decay):
    slab = iota((SLAB, HC), 0)
    high = decay.astype(BF16).astype(F32)
    ref[(*at, slice(0, HC))] = state.astype(BF16)
    ref[(*at, slice(HC, HC + SLAB))] = jnp.where(
        slab == 0, high, jnp.where(slab == 1, decay - high, 0.0)
    ).astype(BF16)


def get_state(ref, at):
    state = ref[(*at, slice(0, HC))].astype(F32)
    decay = jnp.sum(ref[(*at, slice(HC, HC + SLAB))].astype(F32), axis=0, keepdims=True)
    return state, decay


def recurrence_outputs(qin, kin, v_ref, before, off, entering, gain, out):
    blocks = v_ref.shape[0] // BLK
    heads = v_ref.shape[1] // HC
    per = out.shape[1] // BLK
    row, col = iota((BLK, BLK), 0), iota((BLK, BLK), 1)

    def per_block(n, carry):
        rows = pl.ds(pl.multiple_of(n * BLK, BLK), BLK)
        for h in range(heads):
            cols = slice(h * HC, (h + 1) * HC)
            scores, outer = [], None
            for d in range(2):
                q = qin[d, rows, cols]
                scores.append(mm_t(q, kin[d, rows, cols]))
                state = before[d, n, h] + entering[d * heads + h] * jnp.exp(off[d, n, :, cols])
                part = mm_t(q, state.astype(BF16))
                outer = part if outer is None else outer + part
            both = jnp.where(row >= col, scores[0], 0.0) + jnp.where(row <= col, scores[1], 0.0)
            mix = mm(both.astype(BF16), v_ref[rows, cols]) + outer
            scale = lax.rsqrt(jnp.mean(mix * mix, axis=1, keepdims=True) + EPS)
            inside = pl.ds(pl.multiple_of(n % per * BLK, BLK), BLK)
            out[n // per, inside, cols] = (mix * scale * gain[...]).astype(BF16)
        return carry

    lax.fori_loop(0, blocks, per_block, 0)


def chunk_places(shape, dim):
    at = iota(shape, dim)
    piece = sum((at >= q * CAP).astype(jnp.int32) for q in range(1, QUARTERS))
    return at - piece * CAP, piece


def pack_rows(tok_ref, gain_ref, routes_ref, send):
    x = tok_ref[...].astype(F32)
    count, features = x.shape
    experts, chunk, width = send.shape
    scale = lax.rsqrt(jnp.mean(x * x, axis=1, keepdims=True) + EPS)
    normed = (x * scale * gain_ref[...]).astype(BF16)
    routes = routes_ref[...]
    names = iota((experts, count), 0)
    hot = [(routes[k : k + 1, :] == names).astype(F32) for k in range(2)]
    earlier = (iota((count, count), 0) < iota((count, count), 1)).astype(BF16)
    rank = mm((hot[0] + hot[1]).astype(BF16), earlier)
    base = names.astype(F32) * CAP
    dest = [jnp.sum(hot[k] * (rank + base), axis=0, keepdims=True) for k in range(2)]
    inner, piece = chunk_places((experts, chunk, 1), 1)
    slot = (iota((experts, chunk, 1), 0) * CAP + inner).astype(F32).reshape(experts * chunk, 1)
    piece = piece.reshape(experts * chunk, 1)
    picked = jnp.logical_or(slot == dest[0], slot == dest[1])
    lhs = jnp.concatenate(
        [jnp.where(jnp.logical_and(picked, piece == q), 1.0, 0.0) for q in range(QUARTERS)],
        axis=1,
    ).astype(BF16)
    rhs = jnp.concatenate([normed[:, q * width : (q + 1) * width] for q in range(QUARTERS)], axis=0)
    send[...] = mm(lhs, rhs).astype(BF16).reshape(experts, chunk, width)


def as_column(line):
    count = line.shape[1]
    eye = iota((count, count), 0) == iota((count, count), 1)
    return jnp.sum(jnp.where(eye, line, 0.0), axis=1, keepdims=True)


def merge_places(routes_ref, lhs, chunk, expert_of):
    count = routes_ref.shape[1]
    rows = lhs.shape[1]
    experts = rows // chunk
    routes = routes_ref[...].astype(F32)
    names = iota((count, experts), 1).astype(F32)
    hot = [(as_column(routes[k : k + 1, :]) == names).astype(F32) for k in range(2)]
    earlier = (iota((count, count), 0) > iota((count, count), 1)).astype(BF16)
    rank = mm(earlier, (hot[0] + hot[1]).astype(BF16))
    base = names * CAP
    r = iota((1, rows), 1).astype(F32)
    at = jnp.floor((r + 0.5) / chunk)
    rest = r - at * chunk
    piece = jnp.floor((rest + 0.5) / CAP)
    slot = expert_of(at) * CAP + rest - piece * CAP
    for k in range(2):
        dest = jnp.sum(hot[k] * (rank + base), axis=1, keepdims=True)
        picked = slot == dest
        for q in range(QUARTERS):
            first = (k * QUARTERS + q) * count
            lhs[first : first + count, :] = jnp.where(
                jnp.logical_and(picked, piece == q), 1.0, 0.0
            ).astype(BF16)


def merge_early(lhs, ret, early, cut):
    chunk, width = ret.shape[1:]
    rows = ret[:cut].reshape(cut * chunk, width)
    early[...] = mm(lhs[:, : cut * chunk], rows)


def merge_rows(lhs, ret, early, cut, weight_ref, out):
    experts, chunk, width = ret.shape
    count = weight_ref.shape[1]
    weight = [as_column(weight_ref[k : k + 1, :]) for k in range(2)]
    rows = ret[cut:].reshape((experts - cut) * chunk, width)
    for q in range(QUARTERS):
        total = None
        for k in range(2):
            span = slice((k * QUARTERS + q) * count, (k * QUARTERS + q + 1) * count)
            part = weight[k] * (early[span, :] + mm(lhs[span, cut * chunk :], rows))
            total = part if total is None else total + part
        out[:, q * width : (q + 1) * width] = total.astype(BF16)


def kernel(
    query, gates, value, margin, position, head_gain, mixer_w, tokens, expert_gain,
    routes, token_w, wg_any, wu_any, wd_any, mixed, merged,
    q_v, g_v, v_v, margin_v, pos_v, hgain_v, tok_v, egain_v, routes_v, token_w_v, wg, wu, wd,
    w_all, qin, kin, before, off, inc, last, fin, near, far, group_state, chip_in, entering,
    heads_out, heads_in, send, rows, parts, relay_l, relay_r, from_l, from_r, total, ret,
    xt, perm, lhs, early, lead, ahead_state,
    in_sem, zs, zr, xs, xr_l, xr_r, ys, yr, qs, qr, fs, fr, ts, tr,
    mate_s, mate_r, near_s, near_r, far_s, far_r, lead_s, lead_r, chip_s, chip_r,
    ws, wr, wys, wyr, wms, wmr, hs, hr,
    *, n_ep, n_tp,
):
    me, t = lax.axis_index("ep"), lax.axis_index("tp")
    n_z = n_ep // 2
    half = n_z // 2
    steps = n_z // 2
    z, c = me // 2, me % 2
    mate = 2 * z + 1 - c
    right, left = (t + 1) % n_tp, (t + n_tp - 1) % n_tp
    opposite = (t + 2) % n_tp
    chunk, width = send.shape[1:]
    heads = v_v.shape[1] // HC

    def offset(b, side):
        o = (steps + 1 - b) % steps
        return o if side == 0 else n_z - o - half * ((steps - o) // steps)

    loads = [
        pltpu.make_async_copy(src, dst, in_sem.at[i])
        for i, (src, dst) in enumerate(
            (
                (tokens, tok_v), (expert_gain, egain_v), (routes, routes_v), (token_w, token_w_v),
                (mixer_w, w_all.at[0]), (query, q_v), (gates, g_v), (value, v_v),
                (margin, margin_v), (position, pos_v), (head_gain, hgain_v),
                (wg_any.at[0], wg), (wu_any.at[0], wu), (wd_any.at[0], wd),
            )
        )
    ]
    for copy in loads:
        copy.start()

    barrier = pltpu.get_barrier_semaphore()

    def greet(j, carry):
        pl.semaphore_signal(
            barrier, inc=1, device_id={"ep": (me + j) % n_ep}, device_id_type=MESH
        )
        return carry

    lax.fori_loop(1, n_ep, greet, 0)
    for other in (left, right, opposite):
        pl.semaphore_signal(barrier, inc=1, device_id={"tp": other}, device_id_type=MESH)
    for copy in loads[:4]:
        copy.wait()
    pack_rows(tok_v, egain_v, routes_v, send)
    pl.semaphore_wait(barrier, n_ep + n_tp - 2)

    def z_copy(b, side, core):
        other = ((z + offset(b, side)) % n_z) * 2 + core
        return pltpu.make_async_remote_copy(
            src_ref=send.at[other],
            dst_ref=rows.at[0, 4 * b + 2 * side + c],
            send_sem=zs.at[4 * b + 2 * side + core],
            recv_sem=zr.at[4 * b + 2 * side + c],
            device_id={"ep": other},
            device_id_type=MESH,
        )

    def own_in(slot):
        return pltpu.make_async_copy(send.at[me], rows.at[0, slot], zr.at[slot])

    def is_self(b, side, core):
        return jnp.logical_and(jnp.logical_and(b == 1, side == 0), core == c)

    def dispatch(b, carry):
        for side in range(2):
            for core in range(2):
                own = is_self(b, side, core)

                @pl.when(own)
                def _():
                    own_in(4 * b + 2 * side + c).start()

                @pl.when(jnp.logical_not(own))
                def _():
                    z_copy(b, side, core).start()

        return carry

    def x_copy(b, way):
        group = pl.ds(4 * b, 4)
        return pltpu.make_async_remote_copy(
            src_ref=rows.at[0, group],
            dst_ref=rows.at[1 + way, group],
            send_sem=xs.at[way, b],
            recv_sem=(xr_l if way == 0 else xr_r).at[b],
            device_id={"tp": right if way == 0 else left},
            device_id_type=MESH,
        )

    def y_copy(b, way):
        group = pl.ds(4 * b + 2 * way, 2)
        return pltpu.make_async_remote_copy(
            src_ref=rows.at[1 + way, group],
            dst_ref=rows.at[3, group],
            send_sem=ys.at[way, b],
            recv_sem=yr.at[way, b],
            device_id={"tp": right if way == 0 else left},
            device_id_type=MESH,
        )

    def q_copy(b, way):
        return pltpu.make_async_remote_copy(
            src_ref=parts.at[3, pl.ds(4 * b + 2 * way, 2)],
            dst_ref=(relay_l if way == 0 else relay_r).at[pl.ds(2 * b, 2)],
            send_sem=qs.at[way, b],
            recv_sem=qr.at[way, b],
            device_id={"tp": right if way == 0 else left},
            device_id_type=MESH,
        )

    def f_copy(b, way):
        group = pl.ds(4 * b, 4)
        return pltpu.make_async_remote_copy(
            src_ref=parts.at[2 - way, group],
            dst_ref=(from_l if way == 0 else from_r).at[group],
            send_sem=fs.at[way, b],
            recv_sem=fr.at[way, b],
            device_id={"tp": right if way == 0 else left},
            device_id_type=MESH,
        )

    def t_copy(b, side, core):
        other = ((z - offset(b, side) + n_z) % n_z) * 2 + core
        slot = 4 * b + 2 * side + core
        return pltpu.make_async_remote_copy(
            src_ref=total.at[slot],
            dst_ref=ret.at[4 * b + 2 * side + c],
            send_sem=ts.at[slot],
            recv_sem=tr.at[4 * b + 2 * side + c],
            device_id={"ep": other},
            device_id_type=MESH,
        )

    def t_arrival(e):
        return pltpu.make_async_copy(total.at[0], ret.at[e], tr.at[e])

    def own_out(slot):
        return pltpu.make_async_copy(total.at[slot], ret.at[slot], tr.at[slot])

    def arrive(b):
        for k in range(4):
            own_in(4 * b + k).wait()
        x_copy(b, 0).start()
        x_copy(b, 1).start()

    def relay(b):
        for way in range(2):
            x_copy(b, way).wait_recv()
            y_copy(b, way).start()

    def compute(b):
        group = pl.ds(4 * b, 4)
        for way in range(2):
            y_copy(b, way).wait_recv()
        turn = perm[...]
        for w in range(4):
            turned = mm(turn, rows[w, group].reshape(4 * chunk, width)).astype(BF16)
            for q in range(QUARTERS):
                xt[w * chunk : (w + 1) * chunk, q * width : (q + 1) * width] = turned[
                    q * chunk : (q + 1) * chunk
                ]
        x = xt[...]
        gate = jnp.minimum(mm(x, wg[...]), LIMIT)
        up = jnp.clip(mm(x, wu[...]), -LIMIT, LIMIT)
        hidden = ((up + 1.0) * gate / (1.0 + jnp.exp(-SLOPE * gate))).astype(BF16)
        y = mm(hidden, wd[...]).astype(BF16)
        for w in range(4):
            piece = jnp.concatenate(
                [
                    y[w * chunk : (w + 1) * chunk, q * width : (q + 1) * width]
                    for q in range(QUARTERS)
                ],
                axis=0,
            )
            parts[w, group] = mm(turn, piece).astype(BF16).reshape(4, chunk, width)

    def start_sum(b):
        for way in range(2):
            q_copy(b, way).start()

    def pass_sum(b):
        for way in range(2):
            q_copy(b, way).wait_recv()
            group = pl.ds(4 * b + 2 * way, 2)
            carried = (relay_l if way == 0 else relay_r)[pl.ds(2 * b, 2)]
            parts[2 - way, group] = (
                parts[2 - way, group].astype(F32) + carried.astype(F32)
            ).astype(BF16)

    def send_sum(b):
        for way in range(2):
            f_copy(b, way).start()

    def finish(b):
        for way in range(2):
            f_copy(b, way).wait_recv()
        group = pl.ds(4 * b, 4)
        total[group] = (
            parts[0, group].astype(F32) + from_l[group].astype(F32) + from_r[group].astype(F32)
        ).astype(BF16)

    def send_back(b):
        for side in range(2):
            for core in range(2):
                own = is_self(b, side, core)

                @pl.when(own)
                def _():
                    own_out(4 * b + 2 * side + core).start()

                @pl.when(jnp.logical_not(own))
                def _():
                    t_copy(b, side, core).start()


    def w_part(who, core, lo, hi):
        size = w_all.shape[1] // 2
        first = core * size + lo * (size // 2)
        return w_all.at[who, pl.ds(pl.multiple_of(first, size // 2), (hi - lo) * (size // 2))]

    def w_copy(way):
        return pltpu.make_async_remote_copy(
            src_ref=w_part(0, c, 0, 2),
            dst_ref=w_part(1 + way, c, 0, 2),
            send_sem=ws.at[way],
            recv_sem=wr.at[way],
            device_id={"tp": right if way == 0 else left},
            device_id_type=MESH,
        )

    def w_relay(way):
        return pltpu.make_async_remote_copy(
            src_ref=w_part(1 + way, c, way, way + 1),
            dst_ref=w_part(3, c, way, way + 1),
            send_sem=wys.at[way],
            recv_sem=wyr.at[way],
            device_id={"tp": right if way == 0 else left},
            device_id_type=MESH,
        )

    def w_mate(who, core):
        return pltpu.make_async_remote_copy(
            src_ref=w_part(who, core, 0, 2),
            dst_ref=w_part(who, core, 0, 2),
            send_sem=wms.at[who],
            recv_sem=wmr.at[who],
            device_id={"ep": mate},
            device_id_type=MESH,
        )

    p, g = z % 4, z // 4

    def mate_copy():
        return pltpu.make_async_remote_copy(
            src_ref=fin.at[0], dst_ref=fin.at[1], send_sem=mate_s, recv_sem=mate_r,
            device_id={"ep": mate}, device_id_type=MESH,
        )

    def near_copy(d, s):
        other = z + s if d == 0 else z - s
        return pltpu.make_async_remote_copy(
            src_ref=near.at[0, d], dst_ref=near.at[s, d],
            send_sem=near_s.at[d, s], recv_sem=near_r.at[d, s],
            device_id={"ep": (other + n_z) % n_z * 2 + c}, device_id_type=MESH,
        )

    def sends_near(d, s):
        return p + s < 4 if d == 0 else p >= s

    def hears_near(d, s):
        return p >= s if d == 0 else p + s < 4

    def leads(d):
        return p == 3 if d == 0 else p == 0

    def lead_copy(d, s):
        other = z - s if d == 0 else z + s
        return pltpu.make_async_remote_copy(
            src_ref=lead.at[d], dst_ref=lead.at[d],
            send_sem=lead_s.at[d, s], recv_sem=lead_r.at[d],
            device_id={"ep": (other + n_z) % n_z * 2 + c}, device_id_type=MESH,
        )

    def far_copy(d, s):
        other = (z + 4 * s) % n_z if d == 0 else (z - 4 * s + n_z) % n_z
        return pltpu.make_async_remote_copy(
            src_ref=group_state.at[d], dst_ref=far.at[d, s],
            send_sem=far_s.at[d, s], recv_sem=far_r.at[d, s],
            device_id={"ep": other * 2 + c}, device_id_type=MESH,
        )

    def sends_far(d, s):
        return jnp.logical_and(leads(d), g + s < n_z // 4 if d == 0 else g >= s)

    def hears_far(d, s):
        return jnp.logical_and(leads(d), g >= s if d == 0 else g + s < n_z // 4)

    def chip_copy():
        return pltpu.make_async_remote_copy(
            src_ref=chip_in.at[0], dst_ref=chip_in.at[1], send_sem=chip_s, recv_sem=chip_r,
            device_id={"ep": mate}, device_id_type=MESH,
        )

    def share_chip():
        mate_copy().wait_recv()
        for d in range(2):
            at = d * heads + c
            first, first_decay = get_state(fin, (c if d == 0 else 1 - c, at))
            second, second_decay = get_state(fin, (1 - c if d == 0 else c, at))
            put_state(near, (0, d), first * second_decay + second, first_decay * second_decay)

    def send_chip():
        for d in range(2):
            for s in range(1, 4):

                @pl.when(sends_near(d, s))
                def _():
                    near_copy(d, s).start()

    def share_group():
        for d in range(2):
            entering[2 * d] = jnp.zeros((HC, HC), F32)
            entering[2 * d + 1, 0:8] = jnp.ones((8, HC), F32)
            for s in range(3, 0, -1):

                @pl.when(hears_near(d, s))
                def _():
                    near_copy(d, s).wait_recv()
                    state, decay = get_state(near, (s, d))
                    entering[2 * d] = entering[2 * d] * decay + state
                    entering[2 * d + 1, 0:8] = entering[2 * d + 1, 0:8] * decay

            state, decay = get_state(near, (0, d))
            put_state(
                group_state, (d,), entering[2 * d] * decay + state, entering[2 * d + 1, 0:1] * decay
            )
        for d in range(2):
            for s in range(1, n_z // 4):

                @pl.when(sends_far(d, s))
                def _():
                    far_copy(d, s).start()

    def share_far():
        for d in range(2):
            ahead_state[d] = jnp.zeros((HC, HC), F32)
            for s in range(n_z // 4 - 1, 0, -1):

                @pl.when(hears_far(d, s))
                def _():
                    far_copy(d, s).wait_recv()
                    state, decay = get_state(far, (d, s))
                    ahead_state[d] = ahead_state[d] * decay + state

        for d in range(2):

            @pl.when(leads(d))
            def _():
                lead[d] = ahead_state[d].astype(BF16)

        for d in range(2):
            for s in range(1, 4):

                @pl.when(leads(d))
                def _():
                    lead_copy(d, s).start()

    def share_all():
        for d in range(2):

            @pl.when(jnp.logical_not(leads(d)))
            def _():
                lead_copy(d, 1).wait_recv()

            chip_in[0, d] = (
                lead[d].astype(F32) * entering[2 * d + 1, 0:1] + entering[2 * d]
            ).astype(BF16)
        chip_copy().start()

    def enter():
        chip_copy().wait_recv()
        for d in range(2):
            for h in range(heads):
                at = d * heads + h
                state = chip_in[(h + c) % 2, d].astype(F32)
                other, decay = get_state(fin, (1, at))
                passed = (c == 1) if d == 0 else (c == 0)
                entering[at] = jnp.where(passed, state * decay + other, state)

    def head_copy(k):
        to = (right, left, opposite)[k]
        return pltpu.make_async_remote_copy(
            src_ref=heads_out.at[to], dst_ref=heads_in.at[k],
            send_sem=hs.at[k], recv_sem=hr.at[k],
            device_id={"tp": to}, device_id_type=MESH,
        )

    def expert_of(at):
        b = jnp.floor((at + 0.5) / 4)
        side = jnp.floor((at - 4 * b + 0.5) / 2)
        core = at - 4 * b - 2 * side
        o = steps + 1 - b
        o = o - steps * jnp.floor((o + 0.5) / steps)
        other = jnp.where(side < 0.5, o, n_z - o - jnp.where(o < 0.5, 1.0 * half, 0.0))
        other = other + z.astype(F32)
        other = other - n_z * jnp.floor((other + 0.5) / n_z)
        return 2 * other + core

    ahead = 3
    lax.fori_loop(0, ahead, dispatch, 0)
    for copy in loads[4:]:
        copy.wait()
    w_copy(0).start()
    w_copy(1).start()
    size = perm.shape[0]
    row, col = iota((size, size), 0), iota((size, size), 1)
    major = sum((row >= k * chunk).astype(jnp.int32) for k in range(1, 4))
    rest = row - major * chunk
    minor = sum((rest >= k * CAP).astype(jnp.int32) for k in range(1, 4))
    target = minor * chunk + major * CAP + (rest - minor * CAP)
    perm[...] = jnp.where(col == target, 1.0, 0.0).astype(BF16)
    recurrence_states(q_v, g_v, v_v, margin_v, pos_v, qin, kin, before, off, fin, inc, last)
    mate_copy().start()

    def body(i, carry):
        def stage(lag, fn, until=steps):
            @pl.when(jnp.logical_and(i >= lag, i < until + lag))
            def _():
                fn(i - lag)

        def once(at, fn):
            @pl.when(i == at)
            def _():
                fn()

        def relay_weights():
            for way in range(2):
                w_copy(way).wait_recv()
                w_relay(way).start()

        def pair_weights():
            for way in range(2):
                w_relay(way).wait_recv()
            for who in range(1, 4):
                w_mate(who, c).start()

        stage(4, finish)
        stage(3, pass_sum)
        stage(2, compute)
        stage(4, send_back)
        stage(3, send_sum)
        stage(1, relay)
        stage(2, start_sum)
        once(0, share_chip)
        stage(0, arrive)
        once(0, send_chip)
        once(1, relay_weights)
        once(3, share_group)
        stage(0, lambda b: dispatch(b + ahead, 0), steps - ahead)
        once(4, pair_weights)
        once(6, share_far)
        return carry

    lax.fori_loop(0, steps + 4, body, 0)

    share_all()
    merge_places(routes_v, lhs, chunk, expert_of)
    enter()
    recurrence_outputs(qin, kin, v_v, before, off, entering, hgain_v, heads_out)
    for k in range(3):
        head_copy(k).start()
    for who in range(1, 4):
        w_mate(who, 1 - c).wait_recv()
    for k in range(3):
        head_copy(k).wait_recv()
    span = mixed.shape[1] // 4
    for k in range(4):
        cols = slice(k * span, (k + 1) * span)
        acc = None
        for who in range(4):
            own = heads_out[t] if who == 0 else heads_in[who - 1]
            part = mm(own, w_all[who, :, cols]).astype(BF16).astype(F32)
            acc = part if acc is None else acc + part
        mixed[:, cols] = acc.astype(BF16)

    def returned(e, carry):
        t_arrival(e).wait()
        return carry

    cut = n_ep - 8
    lax.fori_loop(0, cut, returned, 0)
    merge_early(lhs, ret, early, cut)
    lax.fori_loop(cut, n_ep, returned, 0)
    merge_rows(lhs, ret, early, cut, token_w_v, merged)

    def sent(b, carry):
        for way in range(2):
            x_copy(b, way).wait_send()
            y_copy(b, way).wait_send()
            q_copy(b, way).wait_send()
            f_copy(b, way).wait_send()
        for side in range(2):
            for core in range(2):

                @pl.when(jnp.logical_not(is_self(b, side, core)))
                def _():
                    z_copy(b, side, core).wait_send()
                    t_copy(b, side, core).wait_send()

        return carry

    lax.fori_loop(0, steps, sent, 0)
    for way in range(2):
        w_copy(way).wait_send()
        w_relay(way).wait_send()
    for who in range(1, 4):
        w_mate(who, c).wait_send()
    for d in range(2):
        for s in range(1, 4):

            @pl.when(sends_near(d, s))
            def _():
                near_copy(d, s).wait_send()

            @pl.when(leads(d))
            def _():
                lead_copy(d, s).wait_send()

        for s in range(1, n_z // 4):

            @pl.when(sends_far(d, s))
            def _():
                far_copy(d, s).wait_send()

    mate_copy().wait_send()
    chip_copy().wait_send()
    for k in range(3):
        head_copy(k).wait_send()


def body(*args):
    (query, gates, value, margin, position, head_gain, mixer_w, tokens, expert_gain,
     routes, token_w, wg, wu, wd) = args
    n_ep, n_tp = lax.axis_size("ep"), lax.axis_size("tp")
    length, channels = query.shape
    heads, blocks = channels // HC, length // BLK
    count, features = tokens.shape
    chunk, width = CAP * QUARTERS, features // QUARTERS
    many = (n_ep, chunk, width)
    half_many = (n_ep // 2, chunk, width)
    steps = n_ep // 4
    group = 4 * chunk
    dma = pltpu.SemaphoreType.DMA
    operands = (
        query, gates, value, margin, position, head_gain[None, :], mixer_w, tokens,
        expert_gain[None, :], jnp.transpose(routes), jnp.transpose(token_w), wg, wu, wd,
    )

    def like(x):
        return VMEM(x.shape, x.dtype)

    per_block = (2, blocks, heads, HC, HC)
    lines = (2, blocks, 1, channels)
    state = (HC + SLAB, HC)
    mixed, merged = pl.pallas_call(
        functools.partial(kernel, n_ep=n_ep, n_tp=n_tp),
        out_shape=(
            jax.ShapeDtypeStruct((length // n_tp, features), BF16),
            jax.ShapeDtypeStruct((count, features), BF16),
        ),
        in_specs=[ANYWHERE] * len(operands),
        out_specs=(WHOLE, WHOLE),
        scratch_shapes=[
            like(query), like(gates), like(value), like(margin), like(position),
            like(operands[5]), like(tokens), like(operands[8]), like(operands[9]), like(operands[10]),
            VMEM(wg.shape[1:], BF16), VMEM(wu.shape[1:], BF16), VMEM(wd.shape[1:], BF16),
            VMEM((n_tp, *mixer_w.shape), BF16),
            VMEM((2, length, channels), BF16), VMEM((2, length, channels), BF16),
            VMEM(per_block, F32), VMEM(lines, F32), VMEM(per_block, F32), VMEM(lines, F32),
            VMEM((2, 2 * heads, *state), BF16),
            VMEM((4, 2, *state), BF16), VMEM((2, 4, *state), BF16), VMEM((2, *state), BF16),
            VMEM((2, 2, HC, HC), BF16), VMEM((2 * heads, HC, HC), F32),
            VMEM((n_tp, length // n_tp, channels), BF16),
            VMEM((3, length // n_tp, channels), BF16),
            VMEM(many, BF16), VMEM((4, *many), BF16), VMEM((4, *many), BF16),
            VMEM(half_many, BF16), VMEM(half_many, BF16),
            VMEM(many, BF16), VMEM(many, BF16), VMEM(many, BF16), VMEM(many, BF16),
            VMEM((group, features), BF16), VMEM((group, group), BF16),
            VMEM((2 * QUARTERS * count, n_ep * chunk), BF16),
            VMEM((2 * QUARTERS * count, width), F32),
            VMEM((2, HC, HC), BF16), VMEM((2, HC, HC), F32),
            dma((len(operands),)),
            dma((n_ep,)), dma((n_ep,)),
            dma((2, steps)), dma((steps,)), dma((steps,)),
            dma((2, steps)), dma((2, steps)),
            dma((2, steps)), dma((2, steps)),
            dma((2, steps)), dma((2, steps)),
            dma((n_ep,)), dma((n_ep,)),
            dma(()), dma(()), dma((2, 4)), dma((2, 4)), dma((2, 4)), dma((2, 4)),
            dma((2, 4)), dma((2,)), dma(()), dma(()),
            dma((2,)), dma((2,)), dma((2,)), dma((2,)), dma((4,)), dma((4,)),
            dma((3,)), dma((3,)),
        ],
        compiler_params=pltpu.CompilerParams(
            collective_id=0, has_side_effects=True, vmem_limit_bytes=62 * 2**20
        ),
        name="whole",
    )(*operands)
    return mixed, merged


def solution(mesh):
    rows = P(("grp", "ep"), "tp")
    split = P(("grp", "ep", "tp"), None)
    return jax.shard_map(
        body,
        mesh=mesh,
        in_specs=(
            rows, rows, rows, P(None, "tp"), P("tp", ("grp", "ep")), P(), P("tp", None),
            split, P(), split, split,
            P("ep", None, "tp"), P("ep", None, "tp"), P("ep", "tp", None),
        ),
        out_specs=(split, split),
        check_vma=False,
    )
```

```python
import functools

import jax
import jax.numpy as jnp
from jax import lax
from jax.experimental import pallas as pl
from jax.experimental.pallas import tpu as pltpu
from jax.sharding import PartitionSpec as P

F32, BF16 = jnp.float32, jnp.bfloat16
HC = 128
BLK = 128
CAP = 12
QUARTERS = 4
EPS = 1e-06
LIMIT = 7.0
SLOPE = 1.702
VMEM = pltpu.VMEM
MESH = pl.DeviceIdType.MESH
WHOLE = pl.BlockSpec(memory_space=VMEM)
SLAB = 16
ANYWHERE = pl.BlockSpec(memory_space=pl.ANY)


def mm(a, b):
    return jnp.dot(a, b, preferred_element_type=F32)


def mm_t(a, b):
    return lax.dot_general(a, b, (((1,), (1,)), ((), ())), preferred_element_type=F32)


def t_mm(a, b):
    return lax.dot_general(a, b, (((0,), (0,)), ((), ())), preferred_element_type=F32)


def iota(shape, dim):
    return lax.broadcasted_iota(jnp.int32, shape, dim)


def logistic(x):
    return 1.0 / (1.0 + jnp.exp(-x))


def recurrence_states(q_ref, g_ref, v_ref, margin_ref, pos_ref, qin, kin, before, off, fin, inc, last):
    blocks = q_ref.shape[0] // BLK
    heads = q_ref.shape[1] // HC
    row, col = iota((BLK, BLK), 0), iota((BLK, BLK), 1)
    keep = (row >= col, row <= col)
    tri = [k.astype(BF16) for k in keep]
    ends = [jnp.exp(margin_ref[d : d + 1, :]) for d in range(2)]

    def per_block(n, carry):
        rows = pl.ds(pl.multiple_of(n * BLK, BLK), BLK)
        q = q_ref[rows, :].astype(F32)
        q = q * logistic(q) * HC**-0.5
        shut = logistic(-g_ref[rows, :].astype(F32))
        values = v_ref[rows, :]
        pos = pos_ref[:, rows]
        for d in range(2):
            k = ends[d] * shut
            logs = jnp.log1p(-k)
            high = logs.astype(BF16)
            low = (logs - high.astype(F32)).astype(BF16)
            added = jnp.concatenate(
                [
                    jnp.broadcast_to(
                        jnp.sum(
                            jnp.where(keep[d], pos[h : h + 1, :], 0.0), axis=1, keepdims=True
                        ),
                        (BLK, HC),
                    )
                    for h in range(heads)
                ],
                axis=1,
            )
            cum = mm(tri[d], high) + mm(tri[d], low) + added
            end = cum[BLK - 1 :, :] if d == 0 else cum[:1, :]
            qin[d, rows, :] = (q * jnp.exp(cum)).astype(BF16)
            kin[d, rows, :] = (k * jnp.exp(-cum)).astype(BF16)
            ks = (k * jnp.exp(end - cum)).astype(BF16)
            last[d, n] = end
            for h in range(heads):
                cols = slice(h * HC, (h + 1) * HC)
                inc[d, n, h] = t_mm(values[:, cols], ks[:, cols])
        return carry

    lax.fori_loop(0, blocks, per_block, 0)
    for d in range(2):

        def chain(i, carry):
            n = i if d == 0 else blocks - 1 - i
            offset, states = carry
            off[d, n] = offset
            end = last[d, n]
            decay = jnp.exp(end)
            new = []
            for h in range(heads):
                before[d, n, h] = states[h]
                new.append(states[h] * decay[:, h * HC : (h + 1) * HC] + inc[d, n, h])
            return offset + end, tuple(new)

        zero = tuple(jnp.zeros((HC, HC), F32) for _ in range(heads))
        total, states = lax.fori_loop(0, blocks, chain, (jnp.zeros((1, heads * HC), F32), zero))
        decay = jnp.exp(total)
        for h in range(heads):
            put_state(fin, (0, d * heads + h), states[h], decay[:, h * HC : (h + 1) * HC])


def put_state(ref, at, state, decay):
    slab = iota((SLAB, HC), 0)
    high = decay.astype(BF16).astype(F32)
    ref[(*at, slice(0, HC))] = state.astype(BF16)
    ref[(*at, slice(HC, HC + SLAB))] = jnp.where(
        slab == 0, high, jnp.where(slab == 1, decay - high, 0.0)
    ).astype(BF16)


def get_state(ref, at):
    state = ref[(*at, slice(0, HC))].astype(F32)
    decay = jnp.sum(ref[(*at, slice(HC, HC + SLAB))].astype(F32), axis=0, keepdims=True)
    return state, decay


def recurrence_outputs(qin, kin, v_ref, before, off, entering, gain, out):
    blocks = v_ref.shape[0] // BLK
    heads = v_ref.shape[1] // HC
    per = out.shape[1] // BLK
    row, col = iota((BLK, BLK), 0), iota((BLK, BLK), 1)

    def per_block(n, carry):
        rows = pl.ds(pl.multiple_of(n * BLK, BLK), BLK)
        for h in range(heads):
            cols = slice(h * HC, (h + 1) * HC)
            scores, outer = [], None
            for d in range(2):
                q = qin[d, rows, cols]
                scores.append(mm_t(q, kin[d, rows, cols]))
                state = before[d, n, h] + entering[d * heads + h] * jnp.exp(off[d, n, :, cols])
                part = mm_t(q, state.astype(BF16))
                outer = part if outer is None else outer + part
            both = jnp.where(row >= col, scores[0], 0.0) + jnp.where(row <= col, scores[1], 0.0)
            mix = mm(both.astype(BF16), v_ref[rows, cols]) + outer
            scale = lax.rsqrt(jnp.mean(mix * mix, axis=1, keepdims=True) + EPS)
            inside = pl.ds(pl.multiple_of(n % per * BLK, BLK), BLK)
            out[n // per, inside, cols] = (mix * scale * gain[...]).astype(BF16)
        return carry

    lax.fori_loop(0, blocks, per_block, 0)


def chunk_places(shape, dim):
    at = iota(shape, dim)
    piece = sum((at >= q * CAP).astype(jnp.int32) for q in range(1, QUARTERS))
    return at - piece * CAP, piece


def pack_rows(tok_ref, gain_ref, routes_ref, send):
    x = tok_ref[...].astype(F32)
    count, features = x.shape
    experts, chunk, width = send.shape
    scale = lax.rsqrt(jnp.mean(x * x, axis=1, keepdims=True) + EPS)
    normed = (x * scale * gain_ref[...]).astype(BF16)
    routes = routes_ref[...]
    names = iota((experts, count), 0)
    hot = [(routes[k : k + 1, :] == names).astype(F32) for k in range(2)]
    earlier = (iota((count, count), 0) < iota((count, count), 1)).astype(BF16)
    rank = mm((hot[0] + hot[1]).astype(BF16), earlier)
    base = names.astype(F32) * CAP
    dest = [jnp.sum(hot[k] * (rank + base), axis=0, keepdims=True) for k in range(2)]
    inner, piece = chunk_places((experts, chunk, 1), 1)
    slot = (iota((experts, chunk, 1), 0) * CAP + inner).astype(F32).reshape(experts * chunk, 1)
    piece = piece.reshape(experts * chunk, 1)
    picked = jnp.logical_or(slot == dest[0], slot == dest[1])
    lhs = jnp.concatenate(
        [jnp.where(jnp.logical_and(picked, piece == q), 1.0, 0.0) for q in range(QUARTERS)],
        axis=1,
    ).astype(BF16)
    rhs = jnp.concatenate([normed[:, q * width : (q + 1) * width] for q in range(QUARTERS)], axis=0)
    send[...] = mm(lhs, rhs).astype(BF16).reshape(experts, chunk, width)


def as_column(line):
    count = line.shape[1]
    eye = iota((count, count), 0) == iota((count, count), 1)
    return jnp.sum(jnp.where(eye, line, 0.0), axis=1, keepdims=True)


def merge_places(routes_ref, lhs, chunk, expert_of):
    count = routes_ref.shape[1]
    rows = lhs.shape[1]
    experts = rows // chunk
    routes = routes_ref[...].astype(F32)
    names = iota((count, experts), 1).astype(F32)
    hot = [(as_column(routes[k : k + 1, :]) == names).astype(F32) for k in range(2)]
    earlier = (iota((count, count), 0) > iota((count, count), 1)).astype(BF16)
    rank = mm(earlier, (hot[0] + hot[1]).astype(BF16))
    base = names * CAP
    r = iota((1, rows), 1).astype(F32)
    at = jnp.floor((r + 0.5) / chunk)
    rest = r - at * chunk
    piece = jnp.floor((rest + 0.5) / CAP)
    slot = expert_of(at) * CAP + rest - piece * CAP
    for k in range(2):
        dest = jnp.sum(hot[k] * (rank + base), axis=1, keepdims=True)
        picked = slot == dest
        for q in range(QUARTERS):
            first = (k * QUARTERS + q) * count
            lhs[first : first + count, :] = jnp.where(
                jnp.logical_and(picked, piece == q), 1.0, 0.0
            ).astype(BF16)


def merge_early(lhs, ret, early, cut):
    chunk, width = ret.shape[1:]
    rows = ret[:cut].reshape(cut * chunk, width)
    early[...] = mm(lhs[:, : cut * chunk], rows)


def merge_rows(lhs, ret, early, cut, weight_ref, out):
    experts, chunk, width = ret.shape
    count = weight_ref.shape[1]
    weight = [as_column(weight_ref[k : k + 1, :]) for k in range(2)]
    rows = ret[cut:].reshape((experts - cut) * chunk, width)
    for q in range(QUARTERS):
        total = None
        for k in range(2):
            span = slice((k * QUARTERS + q) * count, (k * QUARTERS + q + 1) * count)
            part = weight[k] * (early[span, :] + mm(lhs[span, cut * chunk :], rows))
            total = part if total is None else total + part
        out[:, q * width : (q + 1) * width] = total.astype(BF16)


def kernel(
    query, gates, value, margin, position, head_gain, mixer_w, tokens, expert_gain,
    routes, token_w, wg_any, wu_any, wd_any, mixed, merged,
    q_v, g_v, v_v, margin_v, pos_v, hgain_v, tok_v, egain_v, routes_v, token_w_v, wg, wu, wd,
    w_all, qin, kin, before, off, inc, last, fin, near, far, group_state, chip_in, entering,
    heads_out, heads_in, send, rows, parts, relay_l, relay_r, from_l, from_r, total, ret,
    xt, perm, lhs, early, lead, ahead_state,
    in_sem, zs, zr, xs, xr_l, xr_r, ys, yr, qs, qr, fs, fr, ts, tr,
    mate_s, mate_r, near_s, near_r, far_s, far_r, lead_s, lead_r, chip_s, chip_r,
    ws, wr, wys, wyr, wms, wmr, hs, hr,
    *, n_ep, n_tp,
):
    me, t = lax.axis_index("ep"), lax.axis_index("tp")
    n_z = n_ep // 2
    half = n_z // 2
    steps = n_z // 2
    self_step = steps // 2 - 1
    z, c = me // 2, me % 2
    mate = 2 * z + 1 - c
    right, left = (t + 1) % n_tp, (t + n_tp - 1) % n_tp
    opposite = (t + 2) % n_tp
    chunk, width = send.shape[1:]
    heads = v_v.shape[1] // HC

    def offset(b, side):
        o = (steps + self_step - b) % steps
        return o if side == 0 else n_z - o - half * ((steps - o) // steps)

    loads = [
        pltpu.make_async_copy(src, dst, in_sem.at[i])
        for i, (src, dst) in enumerate(
            (
                (tokens, tok_v), (expert_gain, egain_v), (routes, routes_v), (token_w, token_w_v),
                (mixer_w, w_all.at[0]), (query, q_v), (gates, g_v), (value, v_v),
                (margin, margin_v), (position, pos_v), (head_gain, hgain_v),
                (wg_any.at[0], wg), (wu_any.at[0], wu), (wd_any.at[0], wd),
            )
        )
    ]
    for copy in loads:
        copy.start()

    barrier = pltpu.get_barrier_semaphore()

    def greet(j, carry):
        pl.semaphore_signal(
            barrier, inc=1, device_id={"ep": (me + j) % n_ep}, device_id_type=MESH
        )
        return carry

    lax.fori_loop(1, n_ep, greet, 0)
    for other in (left, right, opposite):
        pl.semaphore_signal(barrier, inc=1, device_id={"tp": other}, device_id_type=MESH)
    for copy in loads[:4]:
        copy.wait()
    pack_rows(tok_v, egain_v, routes_v, send)
    pl.semaphore_wait(barrier, n_ep + n_tp - 2)

    def z_copy(b, side, core):
        other = ((z + offset(b, side)) % n_z) * 2 + core
        return pltpu.make_async_remote_copy(
            src_ref=send.at[other],
            dst_ref=rows.at[0, 4 * b + 2 * side + c],
            send_sem=zs.at[4 * b + 2 * side + core],
            recv_sem=zr.at[4 * b + 2 * side + c],
            device_id={"ep": other},
            device_id_type=MESH,
        )

    def own_in(slot):
        return pltpu.make_async_copy(send.at[me], rows.at[0, slot], zr.at[slot])

    def is_self(b, side, core):
        return jnp.logical_and(jnp.logical_and(b == self_step, side == 0), core == c)

    def dispatch(b, carry):
        for side in range(2):
            for core in range(2):
                own = is_self(b, side, core)

                @pl.when(own)
                def _():
                    own_in(4 * b + 2 * side + c).start()

                @pl.when(jnp.logical_not(own))
                def _():
                    z_copy(b, side, core).start()

        return carry

    def x_copy(b, way):
        group = pl.ds(4 * b, 4)
        return pltpu.make_async_remote_copy(
            src_ref=rows.at[0, group],
            dst_ref=rows.at[1 + way, group],
            send_sem=xs.at[way, b],
            recv_sem=(xr_l if way == 0 else xr_r).at[b],
            device_id={"tp": right if way == 0 else left},
            device_id_type=MESH,
        )

    def y_copy(b, way):
        group = pl.ds(4 * b + 2 * way, 2)
        return pltpu.make_async_remote_copy(
            src_ref=rows.at[1 + way, group],
            dst_ref=rows.at[3, group],
            send_sem=ys.at[way, b],
            recv_sem=yr.at[way, b],
            device_id={"tp": right if way == 0 else left},
            device_id_type=MESH,
        )

    def q_copy(b, way):
        return pltpu.make_async_remote_copy(
            src_ref=parts.at[3, pl.ds(4 * b + 2 * way, 2)],
            dst_ref=(relay_l if way == 0 else relay_r).at[pl.ds(2 * b, 2)],
            send_sem=qs.at[way, b],
            recv_sem=qr.at[way, b],
            device_id={"tp": right if way == 0 else left},
            device_id_type=MESH,
        )

    def f_copy(b, way):
        group = pl.ds(4 * b, 4)
        return pltpu.make_async_remote_copy(
            src_ref=parts.at[2 - way, group],
            dst_ref=(from_l if way == 0 else from_r).at[group],
            send_sem=fs.at[way, b],
            recv_sem=fr.at[way, b],
            device_id={"tp": right if way == 0 else left},
            device_id_type=MESH,
        )

    def t_copy(b, side, core):
        other = ((z - offset(b, side) + n_z) % n_z) * 2 + core
        slot = 4 * b + 2 * side + core
        return pltpu.make_async_remote_copy(
            src_ref=total.at[slot],
            dst_ref=ret.at[4 * b + 2 * side + c],
            send_sem=ts.at[slot],
            recv_sem=tr.at[4 * b + 2 * side + c],
            device_id={"ep": other},
            device_id_type=MESH,
        )

    def t_arrival(e):
        return pltpu.make_async_copy(total.at[0], ret.at[e], tr.at[e])

    def own_out(slot):
        return pltpu.make_async_copy(total.at[slot], ret.at[slot], tr.at[slot])

    def arrive(b):
        for k in range(4):
            own_in(4 * b + k).wait()
        x_copy(b, 0).start()
        x_copy(b, 1).start()

    def relay(b):
        for way in range(2):
            x_copy(b, way).wait_recv()
            y_copy(b, way).start()

    def compute(b):
        group = pl.ds(4 * b, 4)
        for way in range(2):
            y_copy(b, way).wait_recv()
        turn = perm[...]
        for w in range(4):
            turned = mm(turn, rows[w, group].reshape(4 * chunk, width)).astype(BF16)
            for q in range(QUARTERS):
                xt[w * chunk : (w + 1) * chunk, q * width : (q + 1) * width] = turned[
                    q * chunk : (q + 1) * chunk
                ]
        x = xt[...]
        gate = jnp.minimum(mm(x, wg[...]), LIMIT)
        up = jnp.clip(mm(x, wu[...]), -LIMIT, LIMIT)
        hidden = ((up + 1.0) * gate / (1.0 + jnp.exp(-SLOPE * gate))).astype(BF16)
        y = mm(hidden, wd[...]).astype(BF16)
        for w in (3, 2, 1, 0):
            piece = jnp.concatenate(
                [
                    y[w * chunk : (w + 1) * chunk, q * width : (q + 1) * width]
                    for q in range(QUARTERS)
                ],
                axis=0,
            )
            parts[w, group] = mm(turn, piece).astype(BF16).reshape(4, chunk, width)

    def start_sum(b):
        for way in range(2):
            q_copy(b, way).start()

    def pass_sum(b):
        for way in range(2):
            q_copy(b, way).wait_recv()
            group = pl.ds(4 * b + 2 * way, 2)
            carried = (relay_l if way == 0 else relay_r)[pl.ds(2 * b, 2)]
            parts[2 - way, group] = (
                parts[2 - way, group].astype(F32) + carried.astype(F32)
            ).astype(BF16)

    def send_sum(b):
        for way in range(2):
            f_copy(b, way).start()

    def finish(b):
        for way in range(2):
            f_copy(b, way).wait_recv()
        group = pl.ds(4 * b, 4)
        total[group] = (
            parts[0, group].astype(F32) + from_l[group].astype(F32) + from_r[group].astype(F32)
        ).astype(BF16)

    def send_back(b):
        for side in range(2):
            for core in range(2):
                own = is_self(b, side, core)

                @pl.when(own)
                def _():
                    own_out(4 * b + 2 * side + core).start()

                @pl.when(jnp.logical_not(own))
                def _():
                    t_copy(b, side, core).start()


    def w_part(who, core, lo, hi):
        size = w_all.shape[1] // 2
        first = core * size + lo * (size // 2)
        return w_all.at[who, pl.ds(pl.multiple_of(first, size // 2), (hi - lo) * (size // 2))]

    def w_copy(way):
        return pltpu.make_async_remote_copy(
            src_ref=w_part(0, c, 0, 2),
            dst_ref=w_part(1 + way, c, 0, 2),
            send_sem=ws.at[way],
            recv_sem=wr.at[way],
            device_id={"tp": right if way == 0 else left},
            device_id_type=MESH,
        )

    def w_relay(way):
        return pltpu.make_async_remote_copy(
            src_ref=w_part(1 + way, c, way, way + 1),
            dst_ref=w_part(3, c, way, way + 1),
            send_sem=wys.at[way],
            recv_sem=wyr.at[way],
            device_id={"tp": right if way == 0 else left},
            device_id_type=MESH,
        )

    def w_mate(who, core):
        return pltpu.make_async_remote_copy(
            src_ref=w_part(who, core, 0, 2),
            dst_ref=w_part(who, core, 0, 2),
            send_sem=wms.at[who],
            recv_sem=wmr.at[who],
            device_id={"ep": mate},
            device_id_type=MESH,
        )

    p, g = z % 4, z // 4

    def mate_copy():
        return pltpu.make_async_remote_copy(
            src_ref=fin.at[0], dst_ref=fin.at[1], send_sem=mate_s, recv_sem=mate_r,
            device_id={"ep": mate}, device_id_type=MESH,
        )

    def near_copy(d, s):
        other = z + s if d == 0 else z - s
        return pltpu.make_async_remote_copy(
            src_ref=near.at[0, d], dst_ref=near.at[s, d],
            send_sem=near_s.at[d, s], recv_sem=near_r.at[d, s],
            device_id={"ep": (other + n_z) % n_z * 2 + c}, device_id_type=MESH,
        )

    def sends_near(d, s):
        return p + s < 4 if d == 0 else p >= s

    def hears_near(d, s):
        return p >= s if d == 0 else p + s < 4

    def leads(d):
        return p == 3 if d == 0 else p == 0

    def lead_copy(d, s):
        other = z - s if d == 0 else z + s
        return pltpu.make_async_remote_copy(
            src_ref=lead.at[d], dst_ref=lead.at[d],
            send_sem=lead_s.at[d, s], recv_sem=lead_r.at[d],
            device_id={"ep": (other + n_z) % n_z * 2 + c}, device_id_type=MESH,
        )

    def far_copy(d, s):
        other = (z + 4 * s) % n_z if d == 0 else (z - 4 * s + n_z) % n_z
        return pltpu.make_async_remote_copy(
            src_ref=group_state.at[d], dst_ref=far.at[d, s],
            send_sem=far_s.at[d, s], recv_sem=far_r.at[d, s],
            device_id={"ep": other * 2 + c}, device_id_type=MESH,
        )

    def sends_far(d, s):
        return jnp.logical_and(leads(d), g + s < n_z // 4 if d == 0 else g >= s)

    def hears_far(d, s):
        return jnp.logical_and(leads(d), g >= s if d == 0 else g + s < n_z // 4)

    def chip_copy():
        return pltpu.make_async_remote_copy(
            src_ref=chip_in.at[0], dst_ref=chip_in.at[1], send_sem=chip_s, recv_sem=chip_r,
            device_id={"ep": mate}, device_id_type=MESH,
        )

    def share_chip():
        mate_copy().wait_recv()
        for d in range(2):
            at = d * heads + c
            first, first_decay = get_state(fin, (c if d == 0 else 1 - c, at))
            second, second_decay = get_state(fin, (1 - c if d == 0 else c, at))
            put_state(near, (0, d), first * second_decay + second, first_decay * second_decay)

    def send_chip():
        for d in range(2):
            for s in range(1, 4):

                @pl.when(sends_near(d, s))
                def _():
                    near_copy(d, s).start()

    def share_group():
        for d in range(2):
            entering[2 * d] = jnp.zeros((HC, HC), F32)
            entering[2 * d + 1, 0:8] = jnp.ones((8, HC), F32)
            for s in range(3, 0, -1):

                @pl.when(hears_near(d, s))
                def _():
                    near_copy(d, s).wait_recv()
                    state, decay = get_state(near, (s, d))
                    entering[2 * d] = entering[2 * d] * decay + state
                    entering[2 * d + 1, 0:8] = entering[2 * d + 1, 0:8] * decay

            state, decay = get_state(near, (0, d))
            put_state(
                group_state, (d,), entering[2 * d] * decay + state, entering[2 * d + 1, 0:1] * decay
            )
        for d in range(2):
            for s in range(1, n_z // 4):

                @pl.when(sends_far(d, s))
                def _():
                    far_copy(d, s).start()

    def share_far():
        for d in range(2):
            ahead_state[d] = jnp.zeros((HC, HC), F32)
            for s in range(n_z // 4 - 1, 0, -1):

                @pl.when(hears_far(d, s))
                def _():
                    far_copy(d, s).wait_recv()
                    state, decay = get_state(far, (d, s))
                    ahead_state[d] = ahead_state[d] * decay + state

        for d in range(2):

            @pl.when(leads(d))
            def _():
                lead[d] = ahead_state[d].astype(BF16)

        for d in range(2):
            for s in range(1, 4):

                @pl.when(leads(d))
                def _():
                    lead_copy(d, s).start()

    def share_all():
        for d in range(2):

            @pl.when(jnp.logical_not(leads(d)))
            def _():
                lead_copy(d, 1).wait_recv()

            chip_in[0, d] = (
                lead[d].astype(F32) * entering[2 * d + 1, 0:1] + entering[2 * d]
            ).astype(BF16)
        chip_copy().start()

    def enter():
        chip_copy().wait_recv()
        for d in range(2):
            for h in range(heads):
                at = d * heads + h
                state = chip_in[(h + c) % 2, d].astype(F32)
                other, decay = get_state(fin, (1, at))
                passed = (c == 1) if d == 0 else (c == 0)
                entering[at] = jnp.where(passed, state * decay + other, state)

    def head_copy(k):
        to = (right, left, opposite)[k]
        return pltpu.make_async_remote_copy(
            src_ref=heads_out.at[to], dst_ref=heads_in.at[k],
            send_sem=hs.at[k], recv_sem=hr.at[k],
            device_id={"tp": to}, device_id_type=MESH,
        )

    def expert_of(at):
        b = jnp.floor((at + 0.5) / 4)
        side = jnp.floor((at - 4 * b + 0.5) / 2)
        core = at - 4 * b - 2 * side
        o = steps + self_step - b
        o = o - steps * jnp.floor((o + 0.5) / steps)
        other = jnp.where(side < 0.5, o, n_z - o - jnp.where(o < 0.5, 1.0 * half, 0.0))
        other = other + z.astype(F32)
        other = other - n_z * jnp.floor((other + 0.5) / n_z)
        return 2 * other + core

    ahead = 4
    lax.fori_loop(0, ahead, dispatch, 0)
    for copy in loads[4:]:
        copy.wait()
    w_copy(0).start()
    w_copy(1).start()
    size = perm.shape[0]
    row, col = iota((size, size), 0), iota((size, size), 1)
    major = sum((row >= k * chunk).astype(jnp.int32) for k in range(1, 4))
    rest = row - major * chunk
    minor = sum((rest >= k * CAP).astype(jnp.int32) for k in range(1, 4))
    target = minor * chunk + major * CAP + (rest - minor * CAP)
    perm[...] = jnp.where(col == target, 1.0, 0.0).astype(BF16)
    recurrence_states(q_v, g_v, v_v, margin_v, pos_v, qin, kin, before, off, fin, inc, last)
    mate_copy().start()

    def body(i, carry):
        def stage(lag, fn, until=steps):
            @pl.when(jnp.logical_and(i >= lag, i < until + lag))
            def _():
                fn(i - lag)

        def once(at, fn):
            @pl.when(i == at)
            def _():
                fn()

        def relay_weights():
            for way in range(2):
                w_copy(way).wait_recv()
                w_relay(way).start()

        def pair_weights():
            for way in range(2):
                w_relay(way).wait_recv()
            for who in range(1, 4):
                w_mate(who, c).start()

        stage(3, pass_sum)
        stage(4, finish)
        stage(3, send_sum)
        stage(1, relay)
        stage(4, send_back)
        stage(2, compute)
        stage(2, start_sum)
        once(0, share_chip)
        stage(0, arrive)
        once(0, send_chip)
        once(1, relay_weights)
        once(3, share_group)
        stage(0, lambda b: dispatch(b + ahead, 0), steps - ahead)
        once(4, pair_weights)
        once(6, share_far)
        return carry

    lax.fori_loop(0, steps + 4, body, 0)

    share_all()
    merge_places(routes_v, lhs, chunk, expert_of)
    enter()
    recurrence_outputs(qin, kin, v_v, before, off, entering, hgain_v, heads_out)
    for k in range(3):
        head_copy(k).start()
    for who in range(1, 4):
        w_mate(who, 1 - c).wait_recv()
    for k in range(3):
        head_copy(k).wait_recv()
    span = mixed.shape[1] // 4
    for k in range(4):
        cols = slice(k * span, (k + 1) * span)
        acc = None
        for who in range(4):
            own = heads_out[t] if who == 0 else heads_in[who - 1]
            part = mm(own, w_all[who, :, cols]).astype(BF16).astype(F32)
            acc = part if acc is None else acc + part
        mixed[:, cols] = acc.astype(BF16)

    def returned(e, carry):
        t_arrival(e).wait()
        return carry

    cut = n_ep - 8
    lax.fori_loop(0, cut, returned, 0)
    merge_early(lhs, ret, early, cut)
    lax.fori_loop(cut, n_ep, returned, 0)
    merge_rows(lhs, ret, early, cut, token_w_v, merged)

    def sent(b, carry):
        for way in range(2):
            x_copy(b, way).wait_send()
            y_copy(b, way).wait_send()
            q_copy(b, way).wait_send()
            f_copy(b, way).wait_send()
        for side in range(2):
            for core in range(2):

                @pl.when(jnp.logical_not(is_self(b, side, core)))
                def _():
                    z_copy(b, side, core).wait_send()
                    t_copy(b, side, core).wait_send()

        return carry

    lax.fori_loop(0, steps, sent, 0)
    for way in range(2):
        w_copy(way).wait_send()
        w_relay(way).wait_send()
    for who in range(1, 4):
        w_mate(who, c).wait_send()
    for d in range(2):
        for s in range(1, 4):

            @pl.when(sends_near(d, s))
            def _():
                near_copy(d, s).wait_send()

            @pl.when(leads(d))
            def _():
                lead_copy(d, s).wait_send()

        for s in range(1, n_z // 4):

            @pl.when(sends_far(d, s))
            def _():
                far_copy(d, s).wait_send()

    mate_copy().wait_send()
    chip_copy().wait_send()
    for k in range(3):
        head_copy(k).wait_send()


def body(*args):
    (query, gates, value, margin, position, head_gain, mixer_w, tokens, expert_gain,
     routes, token_w, wg, wu, wd) = args
    n_ep, n_tp = lax.axis_size("ep"), lax.axis_size("tp")
    length, channels = query.shape
    heads, blocks = channels // HC, length // BLK
    count, features = tokens.shape
    chunk, width = CAP * QUARTERS, features // QUARTERS
    many = (n_ep, chunk, width)
    half_many = (n_ep // 2, chunk, width)
    steps = n_ep // 4
    group = 4 * chunk
    dma = pltpu.SemaphoreType.DMA
    operands = (
        query, gates, value, margin, position, head_gain[None, :], mixer_w, tokens,
        expert_gain[None, :], jnp.transpose(routes), jnp.transpose(token_w), wg, wu, wd,
    )

    def like(x):
        return VMEM(x.shape, x.dtype)

    per_block = (2, blocks, heads, HC, HC)
    lines = (2, blocks, 1, channels)
    state = (HC + SLAB, HC)
    mixed, merged = pl.pallas_call(
        functools.partial(kernel, n_ep=n_ep, n_tp=n_tp),
        out_shape=(
            VMEM((length // n_tp, features), BF16),
            VMEM((count, features), BF16),
        ),
        in_specs=[ANYWHERE] * len(operands),
        out_specs=(WHOLE, WHOLE),
        scratch_shapes=[
            like(query), like(gates), like(value), like(margin), like(position),
            like(operands[5]), like(tokens), like(operands[8]), like(operands[9]), like(operands[10]),
            VMEM(wg.shape[1:], BF16), VMEM(wu.shape[1:], BF16), VMEM(wd.shape[1:], BF16),
            VMEM((n_tp, *mixer_w.shape), BF16),
            VMEM((2, length, channels), BF16), VMEM((2, length, channels), BF16),
            VMEM(per_block, F32), VMEM(lines, F32), VMEM(per_block, F32), VMEM(lines, F32),
            VMEM((2, 2 * heads, *state), BF16),
            VMEM((4, 2, *state), BF16), VMEM((2, 4, *state), BF16), VMEM((2, *state), BF16),
            VMEM((2, 2, HC, HC), BF16), VMEM((2 * heads, HC, HC), F32),
            VMEM((n_tp, length // n_tp, channels), BF16),
            VMEM((3, length // n_tp, channels), BF16),
            VMEM(many, BF16), VMEM((4, *many), BF16), VMEM((4, *many), BF16),
            VMEM(half_many, BF16), VMEM(half_many, BF16),
            VMEM(many, BF16), VMEM(many, BF16), VMEM(many, BF16), VMEM(many, BF16),
            VMEM((group, features), BF16), VMEM((group, group), BF16),
            VMEM((2 * QUARTERS * count, n_ep * chunk), BF16),
            VMEM((2 * QUARTERS * count, width), F32),
            VMEM((2, HC, HC), BF16), VMEM((2, HC, HC), F32),
            dma((len(operands),)),
            dma((n_ep,)), dma((n_ep,)),
            dma((2, steps)), dma((steps,)), dma((steps,)),
            dma((2, steps)), dma((2, steps)),
            dma((2, steps)), dma((2, steps)),
            dma((2, steps)), dma((2, steps)),
            dma((n_ep,)), dma((n_ep,)),
            dma(()), dma(()), dma((2, 4)), dma((2, 4)), dma((2, 4)), dma((2, 4)),
            dma((2, 4)), dma((2,)), dma(()), dma(()),
            dma((2,)), dma((2,)), dma((2,)), dma((2,)), dma((4,)), dma((4,)),
            dma((3,)), dma((3,)),
        ],
        compiler_params=pltpu.CompilerParams(
            collective_id=0, has_side_effects=True, vmem_limit_bytes=62 * 2**20
        ),
        name="whole",
    )(*operands)
    return mixed, merged


def solution(mesh):
    rows = P(("grp", "ep"), "tp")
    split = P(("grp", "ep", "tp"), None)
    return jax.shard_map(
        body,
        mesh=mesh,
        in_specs=(
            rows, rows, rows, P(None, "tp"), P("tp", ("grp", "ep")), P(), P("tp", None),
            split, P(), split, split,
            P("ep", None, "tp"), P("ep", None, "tp"), P("ep", "tp", None),
        ),
        out_specs=(split, split),
        check_vma=False,
    )
```

```python
import functools

import jax
import jax.numpy as jnp
from jax import lax
from jax.experimental import pallas as pl
from jax.experimental.pallas import tpu as pltpu
from jax.sharding import PartitionSpec as P

F32, BF16 = jnp.float32, jnp.bfloat16
HC = 128
BLK = 128
CAP = 12
QUARTERS = 4
EPS = 1e-06
LIMIT = 7.0
SLOPE = 1.702
VMEM = pltpu.VMEM
MESH = pl.DeviceIdType.MESH
WHOLE = pl.BlockSpec(memory_space=VMEM)
SLAB = 16
ANYWHERE = pl.BlockSpec(memory_space=pl.ANY)


def mm(a, b):
    return jnp.dot(a, b, preferred_element_type=F32)


def mm_t(a, b):
    return lax.dot_general(a, b, (((1,), (1,)), ((), ())), preferred_element_type=F32)


def t_mm(a, b):
    return lax.dot_general(a, b, (((0,), (0,)), ((), ())), preferred_element_type=F32)


def iota(shape, dim):
    return lax.broadcasted_iota(jnp.int32, shape, dim)


def logistic(x):
    return 1.0 / (1.0 + jnp.exp(-x))


def recurrence_states(q_ref, g_ref, v_ref, margin_ref, pos_ref, qin, kin, before, off, fin, inc, last):
    blocks = q_ref.shape[0] // BLK
    heads = q_ref.shape[1] // HC
    row, col = iota((BLK, BLK), 0), iota((BLK, BLK), 1)
    keep = (row >= col, row <= col)
    tri = [k.astype(BF16) for k in keep]
    ends = [jnp.exp(margin_ref[d : d + 1, :]) for d in range(2)]

    def per_block(n, carry):
        rows = pl.ds(pl.multiple_of(n * BLK, BLK), BLK)
        q = q_ref[rows, :].astype(F32)
        q = q * logistic(q) * HC**-0.5
        shut = logistic(-g_ref[rows, :].astype(F32))
        values = v_ref[rows, :]
        pos = pos_ref[:, rows]
        for d in range(2):
            k = ends[d] * shut
            logs = jnp.log1p(-k)
            high = logs.astype(BF16)
            low = (logs - high.astype(F32)).astype(BF16)
            added = jnp.concatenate(
                [
                    jnp.broadcast_to(
                        jnp.sum(
                            jnp.where(keep[d], pos[h : h + 1, :], 0.0), axis=1, keepdims=True
                        ),
                        (BLK, HC),
                    )
                    for h in range(heads)
                ],
                axis=1,
            )
            cum = mm(tri[d], high) + mm(tri[d], low) + added
            end = cum[BLK - 1 :, :] if d == 0 else cum[:1, :]
            qin[d, rows, :] = (q * jnp.exp(cum)).astype(BF16)
            kin[d, rows, :] = (k * jnp.exp(-cum)).astype(BF16)
            ks = (k * jnp.exp(end - cum)).astype(BF16)
            last[d, n] = end
            for h in range(heads):
                cols = slice(h * HC, (h + 1) * HC)
                inc[d, n, h] = t_mm(values[:, cols], ks[:, cols])
        return carry

    lax.fori_loop(0, blocks, per_block, 0)
    for d in range(2):

        def chain(i, carry):
            n = i if d == 0 else blocks - 1 - i
            offset, states = carry
            off[d, n] = offset
            end = last[d, n]
            decay = jnp.exp(end)
            new = []
            for h in range(heads):
                before[d, n, h] = states[h]
                new.append(states[h] * decay[:, h * HC : (h + 1) * HC] + inc[d, n, h])
            return offset + end, tuple(new)

        zero = tuple(jnp.zeros((HC, HC), F32) for _ in range(heads))
        total, states = lax.fori_loop(0, blocks, chain, (jnp.zeros((1, heads * HC), F32), zero))
        decay = jnp.exp(total)
        for h in range(heads):
            put_state(fin, (0, d * heads + h), states[h], decay[:, h * HC : (h + 1) * HC])


def put_state(ref, at, state, decay):
    slab = iota((SLAB, HC), 0)
    high = decay.astype(BF16).astype(F32)
    ref[(*at, slice(0, HC))] = state.astype(BF16)
    ref[(*at, slice(HC, HC + SLAB))] = jnp.where(
        slab == 0, high, jnp.where(slab == 1, decay - high, 0.0)
    ).astype(BF16)


def get_state(ref, at):
    state = ref[(*at, slice(0, HC))].astype(F32)
    decay = jnp.sum(ref[(*at, slice(HC, HC + SLAB))].astype(F32), axis=0, keepdims=True)
    return state, decay


def recurrence_outputs(qin, kin, v_ref, before, off, entering, gain, out):
    blocks = v_ref.shape[0] // BLK
    heads = v_ref.shape[1] // HC
    per = out.shape[1] // BLK
    row, col = iota((BLK, BLK), 0), iota((BLK, BLK), 1)

    def per_block(n, carry):
        rows = pl.ds(pl.multiple_of(n * BLK, BLK), BLK)
        for h in range(heads):
            cols = slice(h * HC, (h + 1) * HC)
            scores, outer = [], None
            for d in range(2):
                q = qin[d, rows, cols]
                scores.append(mm_t(q, kin[d, rows, cols]))
                state = before[d, n, h] + entering[d * heads + h] * jnp.exp(off[d, n, :, cols])
                part = mm_t(q, state.astype(BF16))
                outer = part if outer is None else outer + part
            both = jnp.where(row >= col, scores[0], 0.0) + jnp.where(row <= col, scores[1], 0.0)
            mix = mm(both.astype(BF16), v_ref[rows, cols]) + outer
            scale = lax.rsqrt(jnp.mean(mix * mix, axis=1, keepdims=True) + EPS)
            inside = pl.ds(pl.multiple_of(n % per * BLK, BLK), BLK)
            out[n // per, inside, cols] = (mix * scale * gain[...]).astype(BF16)
        return carry

    lax.fori_loop(0, blocks, per_block, 0)


def chunk_places(shape, dim):
    at = iota(shape, dim)
    piece = sum((at >= q * CAP).astype(jnp.int32) for q in range(1, QUARTERS))
    return at - piece * CAP, piece


def pack_rows(tok_ref, gain_ref, routes_ref, send):
    x = tok_ref[...].astype(F32)
    count, features = x.shape
    experts, chunk, width = send.shape
    scale = lax.rsqrt(jnp.mean(x * x, axis=1, keepdims=True) + EPS)
    normed = (x * scale * gain_ref[...]).astype(BF16)
    routes = routes_ref[...]
    names = iota((experts, count), 0)
    hot = [(routes[k : k + 1, :] == names).astype(F32) for k in range(2)]
    earlier = (iota((count, count), 0) < iota((count, count), 1)).astype(BF16)
    rank = mm((hot[0] + hot[1]).astype(BF16), earlier)
    base = names.astype(F32) * CAP
    dest = [jnp.sum(hot[k] * (rank + base), axis=0, keepdims=True) for k in range(2)]
    inner, piece = chunk_places((experts, chunk, 1), 1)
    slot = (iota((experts, chunk, 1), 0) * CAP + inner).astype(F32).reshape(experts * chunk, 1)
    piece = piece.reshape(experts * chunk, 1)
    picked = jnp.logical_or(slot == dest[0], slot == dest[1])
    lhs = jnp.concatenate(
        [jnp.where(jnp.logical_and(picked, piece == q), 1.0, 0.0) for q in range(QUARTERS)],
        axis=1,
    ).astype(BF16)
    rhs = jnp.concatenate([normed[:, q * width : (q + 1) * width] for q in range(QUARTERS)], axis=0)
    send[...] = mm(lhs, rhs).astype(BF16).reshape(experts, chunk, width)


def as_column(line):
    count = line.shape[1]
    eye = iota((count, count), 0) == iota((count, count), 1)
    return jnp.sum(jnp.where(eye, line, 0.0), axis=1, keepdims=True)


def merge_places(routes_ref, lhs, chunk, expert_of):
    count = routes_ref.shape[1]
    rows = lhs.shape[1]
    experts = rows // chunk
    routes = routes_ref[...].astype(F32)
    names = iota((count, experts), 1).astype(F32)
    hot = [(as_column(routes[k : k + 1, :]) == names).astype(F32) for k in range(2)]
    earlier = (iota((count, count), 0) > iota((count, count), 1)).astype(BF16)
    rank = mm(earlier, (hot[0] + hot[1]).astype(BF16))
    base = names * CAP
    r = iota((1, rows), 1).astype(F32)
    at = jnp.floor((r + 0.5) / chunk)
    rest = r - at * chunk
    piece = jnp.floor((rest + 0.5) / CAP)
    slot = expert_of(at) * CAP + rest - piece * CAP
    for k in range(2):
        dest = jnp.sum(hot[k] * (rank + base), axis=1, keepdims=True)
        picked = slot == dest
        for q in range(QUARTERS):
            first = (k * QUARTERS + q) * count
            lhs[first : first + count, :] = jnp.where(
                jnp.logical_and(picked, piece == q), 1.0, 0.0
            ).astype(BF16)


def merge_early(lhs, ret, early, cut):
    chunk, width = ret.shape[1:]
    rows = ret[:cut].reshape(cut * chunk, width)
    early[...] = mm(lhs[:, : cut * chunk], rows)


def merge_rows(lhs, ret, early, cut, weight_ref, out):
    experts, chunk, width = ret.shape
    count = weight_ref.shape[1]
    weight = [as_column(weight_ref[k : k + 1, :]) for k in range(2)]
    rows = ret[cut:].reshape((experts - cut) * chunk, width)
    for q in range(QUARTERS):
        total = None
        for k in range(2):
            span = slice((k * QUARTERS + q) * count, (k * QUARTERS + q + 1) * count)
            part = weight[k] * (early[span, :] + mm(lhs[span, cut * chunk :], rows))
            total = part if total is None else total + part
        out[:, q * width : (q + 1) * width] = total.astype(BF16)


def kernel(
    query, gates, value, margin, position, head_gain, mixer_w, tokens, expert_gain,
    routes, token_w, wg_any, wu_any, wd_any, mixed, merged,
    q_v, g_v, v_v, margin_v, pos_v, hgain_v, tok_v, egain_v, routes_v, token_w_v, wg, wu, wd,
    w_all, qin, kin, before, off, inc, last, fin, near, far, group_state, chip_in, entering,
    heads_out, heads_in, send, rows, parts, relay_l, relay_r, from_l, from_r, total, ret,
    xt, perm, lhs, early, lead, ahead_state,
    ready, in_sem, zs, zr, xs, xr_l, xr_r, ys, yr, qs, qr, fs, fr, ts, tr,
    mate_s, mate_r, near_s, near_r, far_s, far_r, lead_s, lead_r, chip_s, chip_r,
    ws, wr, wys, wyr, wms, wmr, hs, hr,
    *, n_ep, n_tp,
):
    me, t = lax.axis_index("ep"), lax.axis_index("tp")
    n_z = n_ep // 2
    half = n_z // 2
    steps = n_z // 2
    self_step = steps // 2 - 1
    z, c = me // 2, me % 2
    mate = 2 * z + 1 - c
    right, left = (t + 1) % n_tp, (t + n_tp - 1) % n_tp
    opposite = (t + 2) % n_tp
    chunk, width = send.shape[1:]
    heads = v_v.shape[1] // HC

    def offset(b, side):
        o = (steps + self_step - b) % steps
        return o if side == 0 else n_z - o - half * ((steps - o) // steps)

    loads = [
        pltpu.make_async_copy(src, dst, in_sem.at[i])
        for i, (src, dst) in enumerate(
            (
                (tokens, tok_v), (expert_gain, egain_v), (routes, routes_v), (token_w, token_w_v),
                (mixer_w, w_all.at[0]), (query, q_v), (gates, g_v), (value, v_v),
                (margin, margin_v), (position, pos_v), (head_gain, hgain_v),
                (wg_any.at[0], wg), (wu_any.at[0], wu), (wd_any.at[0], wd),
            )
        )
    ]
    for copy in loads:
        copy.start()

    barrier = pltpu.get_barrier_semaphore()

    def greet(e, carry):
        @pl.when(e // 2 > z)
        def _():
            pl.semaphore_signal(barrier, inc=1, device_id={"ep": e}, device_id_type=MESH)

        return carry

    lax.fori_loop(0, n_ep, greet, 0)
    pl.semaphore_signal(barrier, inc=1, device_id={"ep": mate}, device_id_type=MESH)
    for other in (left, right, opposite):
        pl.semaphore_signal(barrier, inc=1, device_id={"tp": other}, device_id_type=MESH)
    for copy in loads[:4]:
        copy.wait()
    pack_rows(tok_v, egain_v, routes_v, send)
    pl.semaphore_wait(barrier, 2 * z + n_tp)

    def announce(e, carry):
        @pl.when(e // 2 < z)
        def _():
            pl.semaphore_signal(ready.at[me], inc=1, device_id={"ep": e}, device_id_type=MESH)

        return carry

    lax.fori_loop(0, n_ep, announce, 0)

    def z_copy(b, side, core):
        other = ((z + offset(b, side)) % n_z) * 2 + core
        return pltpu.make_async_remote_copy(
            src_ref=send.at[other],
            dst_ref=rows.at[0, 4 * b + 2 * side + c],
            send_sem=zs.at[4 * b + 2 * side + core],
            recv_sem=zr.at[4 * b + 2 * side + c],
            device_id={"ep": other},
            device_id_type=MESH,
        )

    def own_in(slot):
        return pltpu.make_async_copy(send.at[me], rows.at[0, slot], zr.at[slot])

    def is_self(b, side, core):
        return jnp.logical_and(jnp.logical_and(b == self_step, side == 0), core == c)

    def dispatch_before(b, carry):
        for side in range(2):
            for core in range(2):
                own = is_self(b, side, core)
                chip = (z + offset(b, side)) % n_z

                @pl.when(own)
                def _():
                    own_in(4 * b + 2 * side + c).start()

                @pl.when(jnp.logical_and(chip <= z, jnp.logical_not(own)))
                def _():
                    z_copy(b, side, core).start()

        return carry

    def dispatch_after(b, lowest, highest):
        for side in range(2):
            for core in range(2):
                chip = (z + offset(b, side)) % n_z

                @pl.when(jnp.logical_and(chip >= z + lowest, chip <= z + highest))
                def _():
                    pl.semaphore_wait(ready.at[2 * chip + core], 1)
                    z_copy(b, side, core).start()

    def dispatch(b):
        dispatch_before(b, 0)
        dispatch_after(b, 1, n_z)

    def soon(b, carry):
        dispatch_after(b, 1, 3)
        return carry

    def later(b, carry):
        dispatch_after(b, 4, n_z)
        return carry

    def x_copy(b, way):
        group = pl.ds(4 * b, 4)
        return pltpu.make_async_remote_copy(
            src_ref=rows.at[0, group],
            dst_ref=rows.at[1 + way, group],
            send_sem=xs.at[way, b],
            recv_sem=(xr_l if way == 0 else xr_r).at[b],
            device_id={"tp": right if way == 0 else left},
            device_id_type=MESH,
        )

    def y_copy(b, way):
        group = pl.ds(4 * b + 2 * way, 2)
        return pltpu.make_async_remote_copy(
            src_ref=rows.at[1 + way, group],
            dst_ref=rows.at[3, group],
            send_sem=ys.at[way, b],
            recv_sem=yr.at[way, b],
            device_id={"tp": right if way == 0 else left},
            device_id_type=MESH,
        )

    def q_copy(b, way):
        return pltpu.make_async_remote_copy(
            src_ref=parts.at[3, pl.ds(4 * b + 2 * way, 2)],
            dst_ref=(relay_l if way == 0 else relay_r).at[pl.ds(2 * b, 2)],
            send_sem=qs.at[way, b],
            recv_sem=qr.at[way, b],
            device_id={"tp": right if way == 0 else left},
            device_id_type=MESH,
        )

    def f_copy(b, way):
        group = pl.ds(4 * b, 4)
        return pltpu.make_async_remote_copy(
            src_ref=parts.at[2 - way, group],
            dst_ref=(from_l if way == 0 else from_r).at[group],
            send_sem=fs.at[way, b],
            recv_sem=fr.at[way, b],
            device_id={"tp": right if way == 0 else left},
            device_id_type=MESH,
        )

    def t_copy(b, side, core):
        other = ((z - offset(b, side) + n_z) % n_z) * 2 + core
        slot = 4 * b + 2 * side + core
        return pltpu.make_async_remote_copy(
            src_ref=total.at[slot],
            dst_ref=ret.at[4 * b + 2 * side + c],
            send_sem=ts.at[slot],
            recv_sem=tr.at[4 * b + 2 * side + c],
            device_id={"ep": other},
            device_id_type=MESH,
        )

    def t_arrival(e):
        return pltpu.make_async_copy(total.at[0], ret.at[e], tr.at[e])

    def own_out(slot):
        return pltpu.make_async_copy(total.at[slot], ret.at[slot], tr.at[slot])

    def arrive(b):
        for k in range(4):
            own_in(4 * b + k).wait()
        x_copy(b, 0).start()
        x_copy(b, 1).start()

    def relay(b):
        for way in range(2):
            x_copy(b, way).wait_recv()
            y_copy(b, way).start()

    def compute(b):
        group = pl.ds(4 * b, 4)
        for way in range(2):
            y_copy(b, way).wait_recv()
        turn = perm[...]
        for w in range(4):
            turned = mm(turn, rows[w, group].reshape(4 * chunk, width)).astype(BF16)
            for q in range(QUARTERS):
                xt[w * chunk : (w + 1) * chunk, q * width : (q + 1) * width] = turned[
                    q * chunk : (q + 1) * chunk
                ]
        x = xt[...]
        gate = jnp.minimum(mm(x, wg[...]), LIMIT)
        up = jnp.clip(mm(x, wu[...]), -LIMIT, LIMIT)
        hidden = ((up + 1.0) * gate / (1.0 + jnp.exp(-SLOPE * gate))).astype(BF16)
        y = mm(hidden, wd[...]).astype(BF16)
        for w in (3, 2, 1, 0):
            piece = jnp.concatenate(
                [
                    y[w * chunk : (w + 1) * chunk, q * width : (q + 1) * width]
                    for q in range(QUARTERS)
                ],
                axis=0,
            )
            parts[w, group] = mm(turn, piece).astype(BF16).reshape(4, chunk, width)

    def start_sum(b):
        for way in range(2):
            q_copy(b, way).start()

    def pass_sum(b):
        for way in range(2):
            q_copy(b, way).wait_recv()
            group = pl.ds(4 * b + 2 * way, 2)
            carried = (relay_l if way == 0 else relay_r)[pl.ds(2 * b, 2)]
            parts[2 - way, group] = (
                parts[2 - way, group].astype(F32) + carried.astype(F32)
            ).astype(BF16)

    def send_sum(b):
        for way in range(2):
            f_copy(b, way).start()

    def finish(b):
        for way in range(2):
            f_copy(b, way).wait_recv()
        group = pl.ds(4 * b, 4)
        total[group] = (
            parts[0, group].astype(F32) + from_l[group].astype(F32) + from_r[group].astype(F32)
        ).astype(BF16)

    def send_back(b):
        for side in range(2):
            for core in range(2):
                own = is_self(b, side, core)

                @pl.when(own)
                def _():
                    own_out(4 * b + 2 * side + core).start()

                @pl.when(jnp.logical_not(own))
                def _():
                    t_copy(b, side, core).start()


    def w_part(who, core, lo, hi):
        size = w_all.shape[1] // 2
        first = core * size + lo * (size // 2)
        return w_all.at[who, pl.ds(pl.multiple_of(first, size // 2), (hi - lo) * (size // 2))]

    def w_copy(way):
        return pltpu.make_async_remote_copy(
            src_ref=w_part(0, c, 0, 2),
            dst_ref=w_part(1 + way, c, 0, 2),
            send_sem=ws.at[way],
            recv_sem=wr.at[way],
            device_id={"tp": right if way == 0 else left},
            device_id_type=MESH,
        )

    def w_relay(way):
        return pltpu.make_async_remote_copy(
            src_ref=w_part(1 + way, c, way, way + 1),
            dst_ref=w_part(3, c, way, way + 1),
            send_sem=wys.at[way],
            recv_sem=wyr.at[way],
            device_id={"tp": right if way == 0 else left},
            device_id_type=MESH,
        )

    def w_mate(who, core):
        return pltpu.make_async_remote_copy(
            src_ref=w_part(who, core, 0, 2),
            dst_ref=w_part(who, core, 0, 2),
            send_sem=wms.at[who],
            recv_sem=wmr.at[who],
            device_id={"ep": mate},
            device_id_type=MESH,
        )

    p, g = z % 4, z // 4

    def mate_copy():
        return pltpu.make_async_remote_copy(
            src_ref=fin.at[0], dst_ref=fin.at[1], send_sem=mate_s, recv_sem=mate_r,
            device_id={"ep": mate}, device_id_type=MESH,
        )

    def near_copy(d, s):
        other = z + s if d == 0 else z - s
        return pltpu.make_async_remote_copy(
            src_ref=near.at[0, d], dst_ref=near.at[s, d],
            send_sem=near_s.at[d, s], recv_sem=near_r.at[d, s],
            device_id={"ep": (other + n_z) % n_z * 2 + c}, device_id_type=MESH,
        )

    def sends_near(d, s):
        return p + s < 4 if d == 0 else p >= s

    def hears_near(d, s):
        return p >= s if d == 0 else p + s < 4

    def leads(d):
        return p == 3 if d == 0 else p == 0

    def lead_copy(d, s):
        other = z - s if d == 0 else z + s
        return pltpu.make_async_remote_copy(
            src_ref=lead.at[d], dst_ref=lead.at[d],
            send_sem=lead_s.at[d, s], recv_sem=lead_r.at[d],
            device_id={"ep": (other + n_z) % n_z * 2 + c}, device_id_type=MESH,
        )

    def far_copy(d, s):
        other = (z + 4 * s) % n_z if d == 0 else (z - 4 * s + n_z) % n_z
        return pltpu.make_async_remote_copy(
            src_ref=group_state.at[d], dst_ref=far.at[d, s],
            send_sem=far_s.at[d, s], recv_sem=far_r.at[d, s],
            device_id={"ep": other * 2 + c}, device_id_type=MESH,
        )

    def sends_far(d, s):
        return jnp.logical_and(leads(d), g + s < n_z // 4 if d == 0 else g >= s)

    def hears_far(d, s):
        return jnp.logical_and(leads(d), g >= s if d == 0 else g + s < n_z // 4)

    def chip_copy():
        return pltpu.make_async_remote_copy(
            src_ref=chip_in.at[0], dst_ref=chip_in.at[1], send_sem=chip_s, recv_sem=chip_r,
            device_id={"ep": mate}, device_id_type=MESH,
        )

    def share_chip():
        mate_copy().wait_recv()
        for d in range(2):
            at = d * heads + c
            first, first_decay = get_state(fin, (c if d == 0 else 1 - c, at))
            second, second_decay = get_state(fin, (1 - c if d == 0 else c, at))
            put_state(near, (0, d), first * second_decay + second, first_decay * second_decay)

    def send_chip():
        for d in range(2):
            for s in range(1, 4):

                @pl.when(sends_near(d, s))
                def _():
                    near_copy(d, s).start()

    def share_group():
        for d in range(2):
            entering[2 * d] = jnp.zeros((HC, HC), F32)
            entering[2 * d + 1, 0:8] = jnp.ones((8, HC), F32)
            for s in range(3, 0, -1):

                @pl.when(hears_near(d, s))
                def _():
                    near_copy(d, s).wait_recv()
                    state, decay = get_state(near, (s, d))
                    entering[2 * d] = entering[2 * d] * decay + state
                    entering[2 * d + 1, 0:8] = entering[2 * d + 1, 0:8] * decay

            state, decay = get_state(near, (0, d))
            put_state(
                group_state, (d,), entering[2 * d] * decay + state, entering[2 * d + 1, 0:1] * decay
            )
        for d in range(2):
            for s in range(1, n_z // 4):

                @pl.when(sends_far(d, s))
                def _():
                    far_copy(d, s).start()

    def share_far():
        for d in range(2):
            ahead_state[d] = jnp.zeros((HC, HC), F32)
            for s in range(n_z // 4 - 1, 0, -1):

                @pl.when(hears_far(d, s))
                def _():
                    far_copy(d, s).wait_recv()
                    state, decay = get_state(far, (d, s))
                    ahead_state[d] = ahead_state[d] * decay + state

        for d in range(2):

            @pl.when(leads(d))
            def _():
                lead[d] = ahead_state[d].astype(BF16)

        for d in range(2):
            for s in range(1, 4):

                @pl.when(leads(d))
                def _():
                    lead_copy(d, s).start()

    def share_all():
        for d in range(2):

            @pl.when(jnp.logical_not(leads(d)))
            def _():
                lead_copy(d, 1).wait_recv()

            chip_in[0, d] = (
                lead[d].astype(F32) * entering[2 * d + 1, 0:1] + entering[2 * d]
            ).astype(BF16)
        chip_copy().start()

    def enter():
        chip_copy().wait_recv()
        for d in range(2):
            for h in range(heads):
                at = d * heads + h
                state = chip_in[(h + c) % 2, d].astype(F32)
                other, decay = get_state(fin, (1, at))
                passed = (c == 1) if d == 0 else (c == 0)
                entering[at] = jnp.where(passed, state * decay + other, state)

    def head_copy(k):
        to = (right, left, opposite)[k]
        return pltpu.make_async_remote_copy(
            src_ref=heads_out.at[to], dst_ref=heads_in.at[k],
            send_sem=hs.at[k], recv_sem=hr.at[k],
            device_id={"tp": to}, device_id_type=MESH,
        )

    def expert_of(at):
        b = jnp.floor((at + 0.5) / 4)
        side = jnp.floor((at - 4 * b + 0.5) / 2)
        core = at - 4 * b - 2 * side
        o = steps + self_step - b
        o = o - steps * jnp.floor((o + 0.5) / steps)
        other = jnp.where(side < 0.5, o, n_z - o - jnp.where(o < 0.5, 1.0 * half, 0.0))
        other = other + z.astype(F32)
        other = other - n_z * jnp.floor((other + 0.5) / n_z)
        return 2 * other + core

    ahead = 4
    lax.fori_loop(0, ahead, dispatch_before, 0)
    lax.fori_loop(0, ahead, soon, 0)
    for copy in loads[4:]:
        copy.wait()
    w_copy(0).start()
    w_copy(1).start()
    size = perm.shape[0]
    row, col = iota((size, size), 0), iota((size, size), 1)
    major = sum((row >= k * chunk).astype(jnp.int32) for k in range(1, 4))
    rest = row - major * chunk
    minor = sum((rest >= k * CAP).astype(jnp.int32) for k in range(1, 4))
    target = minor * chunk + major * CAP + (rest - minor * CAP)
    perm[...] = jnp.where(col == target, 1.0, 0.0).astype(BF16)
    recurrence_states(q_v, g_v, v_v, margin_v, pos_v, qin, kin, before, off, fin, inc, last)
    mate_copy().start()
    lax.fori_loop(0, ahead, later, 0)

    def body(i, carry):
        def stage(lag, fn, until=steps):
            @pl.when(jnp.logical_and(i >= lag, i < until + lag))
            def _():
                fn(i - lag)

        def once(at, fn):
            @pl.when(i == at)
            def _():
                fn()

        def relay_weights():
            for way in range(2):
                w_copy(way).wait_recv()
                w_relay(way).start()

        def pair_weights():
            for way in range(2):
                w_relay(way).wait_recv()
            for who in range(1, 4):
                w_mate(who, c).start()

        stage(3, pass_sum)
        stage(4, finish)
        stage(3, send_sum)
        stage(1, relay)
        stage(4, send_back)
        stage(2, compute)
        stage(2, start_sum)
        once(0, share_chip)
        stage(0, arrive)
        once(0, send_chip)
        once(1, relay_weights)
        stage(0, lambda b: dispatch(b + ahead), steps - ahead)
        once(3, share_group)
        once(4, pair_weights)
        once(7, share_far)
        return carry

    lax.fori_loop(0, steps + 4, body, 0)

    share_all()
    merge_places(routes_v, lhs, chunk, expert_of)
    enter()
    recurrence_outputs(qin, kin, v_v, before, off, entering, hgain_v, heads_out)
    for k in range(3):
        head_copy(k).start()
    for who in range(1, 4):
        w_mate(who, 1 - c).wait_recv()
    for k in range(3):
        head_copy(k).wait_recv()
    span = mixed.shape[1] // 4
    for k in range(4):
        cols = slice(k * span, (k + 1) * span)
        acc = None
        for who in range(4):
            own = heads_out[t] if who == 0 else heads_in[who - 1]
            part = mm(own, w_all[who, :, cols]).astype(BF16).astype(F32)
            acc = part if acc is None else acc + part
        mixed[:, cols] = acc.astype(BF16)

    def returned(e, carry):
        t_arrival(e).wait()
        return carry

    cut = n_ep - 8
    lax.fori_loop(0, cut, returned, 0)
    merge_early(lhs, ret, early, cut)
    lax.fori_loop(cut, n_ep, returned, 0)
    merge_rows(lhs, ret, early, cut, token_w_v, merged)

    def sent(b, carry):
        for way in range(2):
            x_copy(b, way).wait_send()
            y_copy(b, way).wait_send()
            q_copy(b, way).wait_send()
            f_copy(b, way).wait_send()
        for side in range(2):
            for core in range(2):

                @pl.when(jnp.logical_not(is_self(b, side, core)))
                def _():
                    z_copy(b, side, core).wait_send()
                    t_copy(b, side, core).wait_send()

        return carry

    lax.fori_loop(0, steps, sent, 0)
    for way in range(2):
        w_copy(way).wait_send()
        w_relay(way).wait_send()
    for who in range(1, 4):
        w_mate(who, c).wait_send()
    for d in range(2):
        for s in range(1, 4):

            @pl.when(sends_near(d, s))
            def _():
                near_copy(d, s).wait_send()

            @pl.when(leads(d))
            def _():
                lead_copy(d, s).wait_send()

        for s in range(1, n_z // 4):

            @pl.when(sends_far(d, s))
            def _():
                far_copy(d, s).wait_send()

    mate_copy().wait_send()
    chip_copy().wait_send()
    for k in range(3):
        head_copy(k).wait_send()


def body(*args):
    (query, gates, value, margin, position, head_gain, mixer_w, tokens, expert_gain,
     routes, token_w, wg, wu, wd) = args
    n_ep, n_tp = lax.axis_size("ep"), lax.axis_size("tp")
    length, channels = query.shape
    heads, blocks = channels // HC, length // BLK
    count, features = tokens.shape
    chunk, width = CAP * QUARTERS, features // QUARTERS
    many = (n_ep, chunk, width)
    half_many = (n_ep // 2, chunk, width)
    steps = n_ep // 4
    group = 4 * chunk
    dma = pltpu.SemaphoreType.DMA
    operands = (
        query, gates, value, margin, position, head_gain[None, :], mixer_w, tokens,
        expert_gain[None, :], jnp.transpose(routes), jnp.transpose(token_w), wg, wu, wd,
    )

    def like(x):
        return VMEM(x.shape, x.dtype)

    per_block = (2, blocks, heads, HC, HC)
    lines = (2, blocks, 1, channels)
    state = (HC + SLAB, HC)
    mixed, merged = pl.pallas_call(
        functools.partial(kernel, n_ep=n_ep, n_tp=n_tp),
        out_shape=(
            VMEM((length // n_tp, features), BF16),
            VMEM((count, features), BF16),
        ),
        in_specs=[ANYWHERE] * len(operands),
        out_specs=(WHOLE, WHOLE),
        scratch_shapes=[
            like(query), like(gates), like(value), like(margin), like(position),
            like(operands[5]), like(tokens), like(operands[8]), like(operands[9]), like(operands[10]),
            VMEM(wg.shape[1:], BF16), VMEM(wu.shape[1:], BF16), VMEM(wd.shape[1:], BF16),
            VMEM((n_tp, *mixer_w.shape), BF16),
            VMEM((2, length, channels), BF16), VMEM((2, length, channels), BF16),
            VMEM(per_block, F32), VMEM(lines, F32), VMEM(per_block, F32), VMEM(lines, F32),
            VMEM((2, 2 * heads, *state), BF16),
            VMEM((4, 2, *state), BF16), VMEM((2, 4, *state), BF16), VMEM((2, *state), BF16),
            VMEM((2, 2, HC, HC), BF16), VMEM((2 * heads, HC, HC), F32),
            VMEM((n_tp, length // n_tp, channels), BF16),
            VMEM((3, length // n_tp, channels), BF16),
            VMEM(many, BF16), VMEM((4, *many), BF16), VMEM((4, *many), BF16),
            VMEM(half_many, BF16), VMEM(half_many, BF16),
            VMEM(many, BF16), VMEM(many, BF16), VMEM(many, BF16), VMEM(many, BF16),
            VMEM((group, features), BF16), VMEM((group, group), BF16),
            VMEM((2 * QUARTERS * count, n_ep * chunk), BF16),
            VMEM((2 * QUARTERS * count, width), F32),
            VMEM((2, HC, HC), BF16), VMEM((2, HC, HC), F32),
            pltpu.SemaphoreType.REGULAR((n_ep,)),
            dma((len(operands),)),
            dma((n_ep,)), dma((n_ep,)),
            dma((2, steps)), dma((steps,)), dma((steps,)),
            dma((2, steps)), dma((2, steps)),
            dma((2, steps)), dma((2, steps)),
            dma((2, steps)), dma((2, steps)),
            dma((n_ep,)), dma((n_ep,)),
            dma(()), dma(()), dma((2, 4)), dma((2, 4)), dma((2, 4)), dma((2, 4)),
            dma((2, 4)), dma((2,)), dma(()), dma(()),
            dma((2,)), dma((2,)), dma((2,)), dma((2,)), dma((4,)), dma((4,)),
            dma((3,)), dma((3,)),
        ],
        compiler_params=pltpu.CompilerParams(
            collective_id=0, has_side_effects=True, vmem_limit_bytes=62 * 2**20
        ),
        name="whole",
    )(*operands)
    return mixed, merged


def solution(mesh):
    rows = P(("grp", "ep"), "tp")
    split = P(("grp", "ep", "tp"), None)
    return jax.shard_map(
        body,
        mesh=mesh,
        in_specs=(
            rows, rows, rows, P(None, "tp"), P("tp", ("grp", "ep")), P(), P("tp", None),
            split, P(), split, split,
            P("ep", None, "tp"), P("ep", None, "tp"), P("ep", "tp", None),
        ),
        out_specs=(split, split),
        check_vma=False,
    )
```

```python
import functools

import jax
import jax.numpy as jnp
from jax import lax
from jax.experimental import pallas as pl
from jax.experimental.pallas import tpu as pltpu
from jax.sharding import PartitionSpec as P

F32, BF16 = jnp.float32, jnp.bfloat16
HC = 128
BLK = 128
CAP = 12
QUARTERS = 4
EPS = 1e-06
LIMIT = 7.0
SLOPE = 1.702
VMEM = pltpu.VMEM
MESH = pl.DeviceIdType.MESH
WHOLE = pl.BlockSpec(memory_space=VMEM)
SLAB = 16
ANYWHERE = pl.BlockSpec(memory_space=pl.ANY)


def mm(a, b):
    return jnp.dot(a, b, preferred_element_type=F32)


def mm_t(a, b):
    return lax.dot_general(a, b, (((1,), (1,)), ((), ())), preferred_element_type=F32)


def t_mm(a, b):
    return lax.dot_general(a, b, (((0,), (0,)), ((), ())), preferred_element_type=F32)


def iota(shape, dim):
    return lax.broadcasted_iota(jnp.int32, shape, dim)


def logistic(x):
    return 1.0 / (1.0 + jnp.exp(-x))


def recurrence_states(q_ref, g_ref, v_ref, margin_ref, pos_ref, qin, kin, before, off, fin, inc, last):
    blocks = q_ref.shape[0] // BLK
    heads = q_ref.shape[1] // HC
    row, col = iota((BLK, BLK), 0), iota((BLK, BLK), 1)
    keep = (row >= col, row <= col)
    tri = [k.astype(BF16) for k in keep]
    ends = [jnp.exp(margin_ref[d : d + 1, :]) for d in range(2)]

    def per_block(n, carry):
        rows = pl.ds(pl.multiple_of(n * BLK, BLK), BLK)
        q = q_ref[rows, :].astype(F32)
        q = q * logistic(q) * HC**-0.5
        shut = logistic(-g_ref[rows, :].astype(F32))
        values = v_ref[rows, :]
        pos = pos_ref[:, rows]
        for d in range(2):
            k = ends[d] * shut
            logs = jnp.log1p(-k)
            high = logs.astype(BF16)
            low = (logs - high.astype(F32)).astype(BF16)
            added = jnp.concatenate(
                [
                    jnp.broadcast_to(
                        jnp.sum(
                            jnp.where(keep[d], pos[h : h + 1, :], 0.0), axis=1, keepdims=True
                        ),
                        (BLK, HC),
                    )
                    for h in range(heads)
                ],
                axis=1,
            )
            cum = mm(tri[d], high) + mm(tri[d], low) + added
            end = cum[BLK - 1 :, :] if d == 0 else cum[:1, :]
            qin[d, rows, :] = (q * jnp.exp(cum)).astype(BF16)
            kin[d, rows, :] = (k * jnp.exp(-cum)).astype(BF16)
            ks = (k * jnp.exp(end - cum)).astype(BF16)
            last[d, n] = end
            for h in range(heads):
                cols = slice(h * HC, (h + 1) * HC)
                inc[d, n, h] = t_mm(values[:, cols], ks[:, cols])
        return carry

    lax.fori_loop(0, blocks, per_block, 0)
    for d in range(2):

        def chain(i, carry):
            n = i if d == 0 else blocks - 1 - i
            offset, states = carry
            off[d, n] = offset
            end = last[d, n]
            decay = jnp.exp(end)
            new = []
            for h in range(heads):
                before[d, n, h] = states[h]
                new.append(states[h] * decay[:, h * HC : (h + 1) * HC] + inc[d, n, h])
            return offset + end, tuple(new)

        zero = tuple(jnp.zeros((HC, HC), F32) for _ in range(heads))
        total, states = lax.fori_loop(0, blocks, chain, (jnp.zeros((1, heads * HC), F32), zero))
        decay = jnp.exp(total)
        for h in range(heads):
            put_state(fin, (0, d * heads + h), states[h], decay[:, h * HC : (h + 1) * HC])


def put_state(ref, at, state, decay):
    slab = iota((SLAB, HC), 0)
    high = decay.astype(BF16).astype(F32)
    ref[(*at, slice(0, HC))] = state.astype(BF16)
    ref[(*at, slice(HC, HC + SLAB))] = jnp.where(
        slab == 0, high, jnp.where(slab == 1, decay - high, 0.0)
    ).astype(BF16)


def get_state(ref, at):
    state = ref[(*at, slice(0, HC))].astype(F32)
    decay = jnp.sum(ref[(*at, slice(HC, HC + SLAB))].astype(F32), axis=0, keepdims=True)
    return state, decay


def recurrence_outputs(qin, kin, v_ref, before, off, entering, gain, out):
    blocks = v_ref.shape[0] // BLK
    heads = v_ref.shape[1] // HC
    per = out.shape[1] // BLK
    row, col = iota((BLK, BLK), 0), iota((BLK, BLK), 1)

    def per_block(n, carry):
        rows = pl.ds(pl.multiple_of(n * BLK, BLK), BLK)
        for h in range(heads):
            cols = slice(h * HC, (h + 1) * HC)
            scores, outer = [], None
            for d in range(2):
                q = qin[d, rows, cols]
                scores.append(mm_t(q, kin[d, rows, cols]))
                state = before[d, n, h] + entering[d * heads + h] * jnp.exp(off[d, n, :, cols])
                part = mm_t(q, state.astype(BF16))
                outer = part if outer is None else outer + part
            both = jnp.where(row >= col, scores[0], 0.0) + jnp.where(row <= col, scores[1], 0.0)
            mix = mm(both.astype(BF16), v_ref[rows, cols]) + outer
            scale = lax.rsqrt(jnp.mean(mix * mix, axis=1, keepdims=True) + EPS)
            inside = pl.ds(pl.multiple_of(n % per * BLK, BLK), BLK)
            out[n // per, inside, cols] = (mix * scale * gain[...]).astype(BF16)
        return carry

    lax.fori_loop(0, blocks, per_block, 0)


def chunk_places(shape, dim):
    at = iota(shape, dim)
    piece = sum((at >= q * CAP).astype(jnp.int32) for q in range(1, QUARTERS))
    return at - piece * CAP, piece


def pack_rows(tok_ref, gain_ref, routes_ref, send):
    x = tok_ref[...].astype(F32)
    count, features = x.shape
    experts, chunk, width = send.shape
    scale = lax.rsqrt(jnp.mean(x * x, axis=1, keepdims=True) + EPS)
    normed = (x * scale * gain_ref[...]).astype(BF16)
    routes = routes_ref[...]
    names = iota((experts, count), 0)
    hot = [(routes[k : k + 1, :] == names).astype(F32) for k in range(2)]
    earlier = (iota((count, count), 0) < iota((count, count), 1)).astype(BF16)
    rank = mm((hot[0] + hot[1]).astype(BF16), earlier)
    base = names.astype(F32) * CAP
    dest = [jnp.sum(hot[k] * (rank + base), axis=0, keepdims=True) for k in range(2)]
    inner, piece = chunk_places((experts, chunk, 1), 1)
    slot = (iota((experts, chunk, 1), 0) * CAP + inner).astype(F32).reshape(experts * chunk, 1)
    piece = piece.reshape(experts * chunk, 1)
    picked = jnp.logical_or(slot == dest[0], slot == dest[1])
    lhs = jnp.concatenate(
        [jnp.where(jnp.logical_and(picked, piece == q), 1.0, 0.0) for q in range(QUARTERS)],
        axis=1,
    ).astype(BF16)
    rhs = jnp.concatenate([normed[:, q * width : (q + 1) * width] for q in range(QUARTERS)], axis=0)
    send[...] = mm(lhs, rhs).astype(BF16).reshape(experts, chunk, width)


def as_column(line):
    count = line.shape[1]
    eye = iota((count, count), 0) == iota((count, count), 1)
    return jnp.sum(jnp.where(eye, line, 0.0), axis=1, keepdims=True)


def merge_places(routes_ref, lhs, chunk, expert_of):
    count = routes_ref.shape[1]
    rows = lhs.shape[1]
    experts = rows // chunk
    routes = routes_ref[...].astype(F32)
    names = iota((count, experts), 1).astype(F32)
    hot = [(as_column(routes[k : k + 1, :]) == names).astype(F32) for k in range(2)]
    earlier = (iota((count, count), 0) > iota((count, count), 1)).astype(BF16)
    rank = mm(earlier, (hot[0] + hot[1]).astype(BF16))
    base = names * CAP
    r = iota((1, rows), 1).astype(F32)
    at = jnp.floor((r + 0.5) / chunk)
    rest = r - at * chunk
    piece = jnp.floor((rest + 0.5) / CAP)
    slot = expert_of(at) * CAP + rest - piece * CAP
    for k in range(2):
        dest = jnp.sum(hot[k] * (rank + base), axis=1, keepdims=True)
        picked = slot == dest
        for q in range(QUARTERS):
            first = (k * QUARTERS + q) * count
            lhs[first : first + count, :] = jnp.where(
                jnp.logical_and(picked, piece == q), 1.0, 0.0
            ).astype(BF16)


def merge_early(lhs, ret, early, cut):
    chunk, width = ret.shape[1:]
    rows = ret[:cut].reshape(cut * chunk, width)
    early[...] = mm(lhs[:, : cut * chunk], rows)


def merge_rows(lhs, ret, early, cut, weight_ref, out):
    experts, chunk, width = ret.shape
    count = weight_ref.shape[1]
    weight = [as_column(weight_ref[k : k + 1, :]) for k in range(2)]
    rows = ret[cut:].reshape((experts - cut) * chunk, width)
    for q in range(QUARTERS):
        total = None
        for k in range(2):
            span = slice((k * QUARTERS + q) * count, (k * QUARTERS + q + 1) * count)
            part = weight[k] * (early[span, :] + mm(lhs[span, cut * chunk :], rows))
            total = part if total is None else total + part
        out[:, q * width : (q + 1) * width] = total.astype(BF16)


def kernel(
    query, gates, value, margin, position, head_gain, mixer_w, tokens, expert_gain,
    routes, token_w, wg_any, wu_any, wd_any, mixed, merged,
    q_v, g_v, v_v, margin_v, pos_v, hgain_v, tok_v, egain_v, routes_v, token_w_v, wg, wu, wd,
    w_all, qin, kin, before, off, inc, last, fin, near, far, group_state, chip_in, entering,
    heads_out, heads_in, send, rows, parts, relay_l, relay_r, from_l, from_r, total, ret,
    xt, perm, lhs, early, lead, ahead_state,
    in_sem, zs, zr, xs, xr_l, xr_r, ys, yr, qs, qr, fs, fr, ts, tr,
    mate_s, mate_r, near_s, near_r, far_s, far_r, lead_s, lead_r, chip_s, chip_r,
    ws, wr, wys, wyr, wms, wmr, hs, hr,
    *, n_ep, n_tp,
):
    me, t = lax.axis_index("ep"), lax.axis_index("tp")
    n_z = n_ep // 2
    half = n_z // 2
    steps = n_z // 2
    self_step = steps // 2 - 1
    z, c = me // 2, me % 2
    mate = 2 * z + 1 - c
    right, left = (t + 1) % n_tp, (t + n_tp - 1) % n_tp
    opposite = (t + 2) % n_tp
    chunk, width = send.shape[1:]
    heads = v_v.shape[1] // HC

    def offset(b, side):
        o = (steps + self_step - b) % steps
        return o if side == 0 else n_z - o - half * ((steps - o) // steps)

    loads = [
        pltpu.make_async_copy(src, dst, in_sem.at[i])
        for i, (src, dst) in enumerate(
            (
                (tokens, tok_v), (expert_gain, egain_v), (routes, routes_v), (token_w, token_w_v),
                (mixer_w, w_all.at[0]), (query, q_v), (gates, g_v), (value, v_v),
                (margin, margin_v), (position, pos_v), (head_gain, hgain_v),
                (wg_any.at[0], wg), (wu_any.at[0], wu), (wd_any.at[0], wd),
            )
        )
    ]
    for copy in loads[:3]:
        copy.start()

    barrier = pltpu.get_barrier_semaphore()

    def greet(j, carry):
        pl.semaphore_signal(
            barrier, inc=1, device_id={"ep": (me + j) % n_ep}, device_id_type=MESH
        )
        return carry

    lax.fori_loop(1, n_ep, greet, 0)
    for other in (left, right, opposite):
        pl.semaphore_signal(barrier, inc=1, device_id={"tp": other}, device_id_type=MESH)
    for copy in loads[:3]:
        copy.wait()
    for copy in loads[3:]:
        copy.start()
    pack_rows(tok_v, egain_v, routes_v, send)
    pl.semaphore_wait(barrier, n_ep + n_tp - 2)

    def z_copy(b, side, core):
        other = ((z + offset(b, side)) % n_z) * 2 + core
        return pltpu.make_async_remote_copy(
            src_ref=send.at[other],
            dst_ref=rows.at[0, 4 * b + 2 * side + c],
            send_sem=zs.at[4 * b + 2 * side + core],
            recv_sem=zr.at[4 * b + 2 * side + c],
            device_id={"ep": other},
            device_id_type=MESH,
        )

    def own_in(slot):
        return pltpu.make_async_copy(send.at[me], rows.at[0, slot], zr.at[slot])

    def is_self(b, side, core):
        return jnp.logical_and(jnp.logical_and(b == self_step, side == 0), core == c)

    def dispatch(b, carry):
        for side in range(2):
            for core in range(2):
                own = is_self(b, side, core)

                @pl.when(own)
                def _():
                    own_in(4 * b + 2 * side + c).start()

                @pl.when(jnp.logical_not(own))
                def _():
                    z_copy(b, side, core).start()

        return carry

    def x_copy(b, way):
        group = pl.ds(4 * b, 4)
        return pltpu.make_async_remote_copy(
            src_ref=rows.at[0, group],
            dst_ref=rows.at[1 + way, group],
            send_sem=xs.at[way, b],
            recv_sem=(xr_l if way == 0 else xr_r).at[b],
            device_id={"tp": right if way == 0 else left},
            device_id_type=MESH,
        )

    def y_copy(b, way):
        group = pl.ds(4 * b + 2 * way, 2)
        return pltpu.make_async_remote_copy(
            src_ref=rows.at[1 + way, group],
            dst_ref=rows.at[3, group],
            send_sem=ys.at[way, b],
            recv_sem=yr.at[way, b],
            device_id={"tp": right if way == 0 else left},
            device_id_type=MESH,
        )

    def q_copy(b, way):
        return pltpu.make_async_remote_copy(
            src_ref=parts.at[3, pl.ds(4 * b + 2 * way, 2)],
            dst_ref=(relay_l if way == 0 else relay_r).at[pl.ds(2 * b, 2)],
            send_sem=qs.at[way, b],
            recv_sem=qr.at[way, b],
            device_id={"tp": right if way == 0 else left},
            device_id_type=MESH,
        )

    def f_copy(b, way):
        group = pl.ds(4 * b, 4)
        return pltpu.make_async_remote_copy(
            src_ref=parts.at[2 - way, group],
            dst_ref=(from_l if way == 0 else from_r).at[group],
            send_sem=fs.at[way, b],
            recv_sem=fr.at[way, b],
            device_id={"tp": right if way == 0 else left},
            device_id_type=MESH,
        )

    def t_copy(b, side, core):
        other = ((z - offset(b, side) + n_z) % n_z) * 2 + core
        slot = 4 * b + 2 * side + core
        return pltpu.make_async_remote_copy(
            src_ref=total.at[slot],
            dst_ref=ret.at[4 * b + 2 * side + c],
            send_sem=ts.at[slot],
            recv_sem=tr.at[4 * b + 2 * side + c],
            device_id={"ep": other},
            device_id_type=MESH,
        )

    def t_arrival(e):
        return pltpu.make_async_copy(total.at[0], ret.at[e], tr.at[e])

    def own_out(slot):
        return pltpu.make_async_copy(total.at[slot], ret.at[slot], tr.at[slot])

    def arrive(b):
        for k in range(4):
            own_in(4 * b + k).wait()
        x_copy(b, 0).start()
        x_copy(b, 1).start()

    def relay(b):
        for way in range(2):
            x_copy(b, way).wait_recv()
            y_copy(b, way).start()

    def compute(b):
        group = pl.ds(4 * b, 4)
        for way in range(2):
            y_copy(b, way).wait_recv()
        turn = perm[...]
        for w in range(4):
            turned = mm(turn, rows[w, group].reshape(4 * chunk, width)).astype(BF16)
            for q in range(QUARTERS):
                xt[w * chunk : (w + 1) * chunk, q * width : (q + 1) * width] = turned[
                    q * chunk : (q + 1) * chunk
                ]
        x = xt[...]
        gate = jnp.minimum(mm(x, wg[...]), LIMIT)
        up = jnp.clip(mm(x, wu[...]), -LIMIT, LIMIT)
        hidden = ((up + 1.0) * gate / (1.0 + jnp.exp(-SLOPE * gate))).astype(BF16)
        y = mm(hidden, wd[...]).astype(BF16)
        for w in (3, 2, 1, 0):
            piece = jnp.concatenate(
                [
                    y[w * chunk : (w + 1) * chunk, q * width : (q + 1) * width]
                    for q in range(QUARTERS)
                ],
                axis=0,
            )
            parts[w, group] = mm(turn, piece).astype(BF16).reshape(4, chunk, width)

    def start_sum(b):
        for way in range(2):
            q_copy(b, way).start()

    def pass_sum(b):
        for way in range(2):
            q_copy(b, way).wait_recv()
            group = pl.ds(4 * b + 2 * way, 2)
            carried = (relay_l if way == 0 else relay_r)[pl.ds(2 * b, 2)]
            parts[2 - way, group] = (
                parts[2 - way, group].astype(F32) + carried.astype(F32)
            ).astype(BF16)

    def send_sum(b):
        for way in range(2):
            f_copy(b, way).start()

    def finish(b):
        for way in range(2):
            f_copy(b, way).wait_recv()
        group = pl.ds(4 * b, 4)
        total[group] = (
            parts[0, group].astype(F32) + from_l[group].astype(F32) + from_r[group].astype(F32)
        ).astype(BF16)

    def send_back(b):
        for side in range(2):
            for core in range(2):
                own = is_self(b, side, core)

                @pl.when(own)
                def _():
                    own_out(4 * b + 2 * side + core).start()

                @pl.when(jnp.logical_not(own))
                def _():
                    t_copy(b, side, core).start()


    def w_part(who, core, lo, hi):
        size = w_all.shape[1] // 2
        first = core * size + lo * (size // 2)
        return w_all.at[who, pl.ds(pl.multiple_of(first, size // 2), (hi - lo) * (size // 2))]

    def w_copy(way):
        return pltpu.make_async_remote_copy(
            src_ref=w_part(0, c, 0, 2),
            dst_ref=w_part(1 + way, c, 0, 2),
            send_sem=ws.at[way],
            recv_sem=wr.at[way],
            device_id={"tp": right if way == 0 else left},
            device_id_type=MESH,
        )

    def w_relay(way):
        return pltpu.make_async_remote_copy(
            src_ref=w_part(1 + way, c, way, way + 1),
            dst_ref=w_part(3, c, way, way + 1),
            send_sem=wys.at[way],
            recv_sem=wyr.at[way],
            device_id={"tp": right if way == 0 else left},
            device_id_type=MESH,
        )

    def w_mate(who, core):
        return pltpu.make_async_remote_copy(
            src_ref=w_part(who, core, 0, 2),
            dst_ref=w_part(who, core, 0, 2),
            send_sem=wms.at[who],
            recv_sem=wmr.at[who],
            device_id={"ep": mate},
            device_id_type=MESH,
        )

    p, g = z % 4, z // 4

    def mate_copy():
        return pltpu.make_async_remote_copy(
            src_ref=fin.at[0], dst_ref=fin.at[1], send_sem=mate_s, recv_sem=mate_r,
            device_id={"ep": mate}, device_id_type=MESH,
        )

    def near_copy(d, s):
        other = z + s if d == 0 else z - s
        return pltpu.make_async_remote_copy(
            src_ref=near.at[0, d], dst_ref=near.at[s, d],
            send_sem=near_s.at[d, s], recv_sem=near_r.at[d, s],
            device_id={"ep": (other + n_z) % n_z * 2 + c}, device_id_type=MESH,
        )

    def sends_near(d, s):
        return p + s < 4 if d == 0 else p >= s

    def hears_near(d, s):
        return p >= s if d == 0 else p + s < 4

    def leads(d):
        return p == 3 if d == 0 else p == 0

    def lead_copy(d, s):
        other = z - s if d == 0 else z + s
        return pltpu.make_async_remote_copy(
            src_ref=lead.at[d], dst_ref=lead.at[d],
            send_sem=lead_s.at[d, s], recv_sem=lead_r.at[d],
            device_id={"ep": (other + n_z) % n_z * 2 + c}, device_id_type=MESH,
        )

    def far_copy(d, s):
        other = (z + 4 * s) % n_z if d == 0 else (z - 4 * s + n_z) % n_z
        return pltpu.make_async_remote_copy(
            src_ref=group_state.at[d], dst_ref=far.at[d, s],
            send_sem=far_s.at[d, s], recv_sem=far_r.at[d, s],
            device_id={"ep": other * 2 + c}, device_id_type=MESH,
        )

    def sends_far(d, s):
        return jnp.logical_and(leads(d), g + s < n_z // 4 if d == 0 else g >= s)

    def hears_far(d, s):
        return jnp.logical_and(leads(d), g >= s if d == 0 else g + s < n_z // 4)

    def chip_copy():
        return pltpu.make_async_remote_copy(
            src_ref=chip_in.at[0], dst_ref=chip_in.at[1], send_sem=chip_s, recv_sem=chip_r,
            device_id={"ep": mate}, device_id_type=MESH,
        )

    def share_chip():
        mate_copy().wait_recv()
        for d in range(2):
            at = d * heads + c
            first, first_decay = get_state(fin, (c if d == 0 else 1 - c, at))
            second, second_decay = get_state(fin, (1 - c if d == 0 else c, at))
            put_state(near, (0, d), first * second_decay + second, first_decay * second_decay)

    def send_chip():
        for d in range(2):
            for s in range(1, 4):

                @pl.when(sends_near(d, s))
                def _():
                    near_copy(d, s).start()

    def share_group():
        for d in range(2):
            entering[2 * d] = jnp.zeros((HC, HC), F32)
            entering[2 * d + 1, 0:8] = jnp.ones((8, HC), F32)
            for s in range(3, 0, -1):

                @pl.when(hears_near(d, s))
                def _():
                    near_copy(d, s).wait_recv()
                    state, decay = get_state(near, (s, d))
                    entering[2 * d] = entering[2 * d] * decay + state
                    entering[2 * d + 1, 0:8] = entering[2 * d + 1, 0:8] * decay

            state, decay = get_state(near, (0, d))
            put_state(
                group_state, (d,), entering[2 * d] * decay + state, entering[2 * d + 1, 0:1] * decay
            )
        for d in range(2):
            for s in range(1, n_z // 4):

                @pl.when(sends_far(d, s))
                def _():
                    far_copy(d, s).start()

    def share_far():
        for d in range(2):
            ahead_state[d] = jnp.zeros((HC, HC), F32)
            for s in range(n_z // 4 - 1, 0, -1):

                @pl.when(hears_far(d, s))
                def _():
                    far_copy(d, s).wait_recv()
                    state, decay = get_state(far, (d, s))
                    ahead_state[d] = ahead_state[d] * decay + state

        for d in range(2):

            @pl.when(leads(d))
            def _():
                lead[d] = ahead_state[d].astype(BF16)

        for d in range(2):
            for s in range(1, 4):

                @pl.when(leads(d))
                def _():
                    lead_copy(d, s).start()

    def share_all():
        for d in range(2):

            @pl.when(jnp.logical_not(leads(d)))
            def _():
                lead_copy(d, 1).wait_recv()

            chip_in[0, d] = (
                lead[d].astype(F32) * entering[2 * d + 1, 0:1] + entering[2 * d]
            ).astype(BF16)
        chip_copy().start()

    def enter():
        chip_copy().wait_recv()
        for d in range(2):
            for h in range(heads):
                at = d * heads + h
                state = chip_in[(h + c) % 2, d].astype(F32)
                other, decay = get_state(fin, (1, at))
                passed = (c == 1) if d == 0 else (c == 0)
                entering[at] = jnp.where(passed, state * decay + other, state)

    def head_copy(k):
        to = (right, left, opposite)[k]
        return pltpu.make_async_remote_copy(
            src_ref=heads_out.at[to], dst_ref=heads_in.at[k],
            send_sem=hs.at[k], recv_sem=hr.at[k],
            device_id={"tp": to}, device_id_type=MESH,
        )

    def expert_of(at):
        b = jnp.floor((at + 0.5) / 4)
        side = jnp.floor((at - 4 * b + 0.5) / 2)
        core = at - 4 * b - 2 * side
        o = steps + self_step - b
        o = o - steps * jnp.floor((o + 0.5) / steps)
        other = jnp.where(side < 0.5, o, n_z - o - jnp.where(o < 0.5, 1.0 * half, 0.0))
        other = other + z.astype(F32)
        other = other - n_z * jnp.floor((other + 0.5) / n_z)
        return 2 * other + core

    ahead = 4
    lax.fori_loop(0, ahead, dispatch, 0)
    for copy in loads[3:]:
        copy.wait()
    w_copy(0).start()
    w_copy(1).start()
    size = perm.shape[0]
    row, col = iota((size, size), 0), iota((size, size), 1)
    major = sum((row >= k * chunk).astype(jnp.int32) for k in range(1, 4))
    rest = row - major * chunk
    minor = sum((rest >= k * CAP).astype(jnp.int32) for k in range(1, 4))
    target = minor * chunk + major * CAP + (rest - minor * CAP)
    perm[...] = jnp.where(col == target, 1.0, 0.0).astype(BF16)
    recurrence_states(q_v, g_v, v_v, margin_v, pos_v, qin, kin, before, off, fin, inc, last)
    mate_copy().start()

    def body(i, carry):
        def stage(lag, fn, until=steps):
            @pl.when(jnp.logical_and(i >= lag, i < until + lag))
            def _():
                fn(i - lag)

        def once(at, fn):
            @pl.when(i == at)
            def _():
                fn()

        def relay_weights():
            for way in range(2):
                w_copy(way).wait_recv()
                w_relay(way).start()

        def pair_weights():
            for way in range(2):
                w_relay(way).wait_recv()
            for who in range(1, 4):
                w_mate(who, c).start()

        stage(3, pass_sum)
        stage(4, finish)
        stage(3, send_sum)
        stage(1, relay)
        stage(4, send_back)
        stage(2, compute)
        stage(2, start_sum)
        once(0, share_chip)
        stage(0, arrive)
        once(0, send_chip)
        once(1, relay_weights)
        once(3, share_group)
        stage(0, lambda b: dispatch(b + ahead, 0), steps - ahead)
        once(4, pair_weights)
        once(6, share_far)
        return carry

    lax.fori_loop(0, steps + 4, body, 0)

    share_all()
    merge_places(routes_v, lhs, chunk, expert_of)
    enter()
    recurrence_outputs(qin, kin, v_v, before, off, entering, hgain_v, heads_out)
    for k in range(3):
        head_copy(k).start()
    for who in range(1, 4):
        w_mate(who, 1 - c).wait_recv()
    for k in range(3):
        head_copy(k).wait_recv()
    span = mixed.shape[1] // 4
    for k in range(4):
        cols = slice(k * span, (k + 1) * span)
        acc = None
        for who in range(4):
            own = heads_out[t] if who == 0 else heads_in[who - 1]
            part = mm(own, w_all[who, :, cols]).astype(BF16).astype(F32)
            acc = part if acc is None else acc + part
        mixed[:, cols] = acc.astype(BF16)

    def returned(e, carry):
        t_arrival(e).wait()
        return carry

    cut = n_ep - 8
    lax.fori_loop(0, cut, returned, 0)
    merge_early(lhs, ret, early, cut)
    lax.fori_loop(cut, n_ep, returned, 0)
    merge_rows(lhs, ret, early, cut, token_w_v, merged)

    def sent(b, carry):
        for way in range(2):
            x_copy(b, way).wait_send()
            y_copy(b, way).wait_send()
            q_copy(b, way).wait_send()
            f_copy(b, way).wait_send()
        for side in range(2):
            for core in range(2):

                @pl.when(jnp.logical_not(is_self(b, side, core)))
                def _():
                    z_copy(b, side, core).wait_send()
                    t_copy(b, side, core).wait_send()

        return carry

    lax.fori_loop(0, steps, sent, 0)
    for way in range(2):
        w_copy(way).wait_send()
        w_relay(way).wait_send()
    for who in range(1, 4):
        w_mate(who, c).wait_send()
    for d in range(2):
        for s in range(1, 4):

            @pl.when(sends_near(d, s))
            def _():
                near_copy(d, s).wait_send()

            @pl.when(leads(d))
            def _():
                lead_copy(d, s).wait_send()

        for s in range(1, n_z // 4):

            @pl.when(sends_far(d, s))
            def _():
                far_copy(d, s).wait_send()

    mate_copy().wait_send()
    chip_copy().wait_send()
    for k in range(3):
        head_copy(k).wait_send()


def body(*args):
    (query, gates, value, margin, position, head_gain, mixer_w, tokens, expert_gain,
     routes, token_w, wg, wu, wd) = args
    n_ep, n_tp = lax.axis_size("ep"), lax.axis_size("tp")
    length, channels = query.shape
    heads, blocks = channels // HC, length // BLK
    count, features = tokens.shape
    chunk, width = CAP * QUARTERS, features // QUARTERS
    many = (n_ep, chunk, width)
    half_many = (n_ep // 2, chunk, width)
    steps = n_ep // 4
    group = 4 * chunk
    dma = pltpu.SemaphoreType.DMA
    operands = (
        query, gates, value, margin, position, head_gain[None, :], mixer_w, tokens,
        expert_gain[None, :], jnp.transpose(routes), jnp.transpose(token_w), wg, wu, wd,
    )

    def like(x):
        return VMEM(x.shape, x.dtype)

    per_block = (2, blocks, heads, HC, HC)
    lines = (2, blocks, 1, channels)
    state = (HC + SLAB, HC)
    mixed, merged = pl.pallas_call(
        functools.partial(kernel, n_ep=n_ep, n_tp=n_tp),
        out_shape=(
            VMEM((length // n_tp, features), BF16),
            VMEM((count, features), BF16),
        ),
        in_specs=[ANYWHERE] * len(operands),
        out_specs=(WHOLE, WHOLE),
        scratch_shapes=[
            like(query), like(gates), like(value), like(margin), like(position),
            like(operands[5]), like(tokens), like(operands[8]), like(operands[9]), like(operands[10]),
            VMEM(wg.shape[1:], BF16), VMEM(wu.shape[1:], BF16), VMEM(wd.shape[1:], BF16),
            VMEM((n_tp, *mixer_w.shape), BF16),
            VMEM((2, length, channels), BF16), VMEM((2, length, channels), BF16),
            VMEM(per_block, F32), VMEM(lines, F32), VMEM(per_block, F32), VMEM(lines, F32),
            VMEM((2, 2 * heads, *state), BF16),
            VMEM((4, 2, *state), BF16), VMEM((2, 4, *state), BF16), VMEM((2, *state), BF16),
            VMEM((2, 2, HC, HC), BF16), VMEM((2 * heads, HC, HC), F32),
            VMEM((n_tp, length // n_tp, channels), BF16),
            VMEM((3, length // n_tp, channels), BF16),
            VMEM(many, BF16), VMEM((4, *many), BF16), VMEM((4, *many), BF16),
            VMEM(half_many, BF16), VMEM(half_many, BF16),
            VMEM(many, BF16), VMEM(many, BF16), VMEM(many, BF16), VMEM(many, BF16),
            VMEM((group, features), BF16), VMEM((group, group), BF16),
            VMEM((2 * QUARTERS * count, n_ep * chunk), BF16),
            VMEM((2 * QUARTERS * count, width), F32),
            VMEM((2, HC, HC), BF16), VMEM((2, HC, HC), F32),
            dma((len(operands),)),
            dma((n_ep,)), dma((n_ep,)),
            dma((2, steps)), dma((steps,)), dma((steps,)),
            dma((2, steps)), dma((2, steps)),
            dma((2, steps)), dma((2, steps)),
            dma((2, steps)), dma((2, steps)),
            dma((n_ep,)), dma((n_ep,)),
            dma(()), dma(()), dma((2, 4)), dma((2, 4)), dma((2, 4)), dma((2, 4)),
            dma((2, 4)), dma((2,)), dma(()), dma(()),
            dma((2,)), dma((2,)), dma((2,)), dma((2,)), dma((4,)), dma((4,)),
            dma((3,)), dma((3,)),
        ],
        compiler_params=pltpu.CompilerParams(
            collective_id=0, has_side_effects=True, vmem_limit_bytes=62 * 2**20
        ),
        name="whole",
    )(*operands)
    return mixed, merged


def solution(mesh):
    rows = P(("grp", "ep"), "tp")
    split = P(("grp", "ep", "tp"), None)
    return jax.shard_map(
        body,
        mesh=mesh,
        in_specs=(
            rows, rows, rows, P(None, "tp"), P("tp", ("grp", "ep")), P(), P("tp", None),
            split, P(), split, split,
            P("ep", None, "tp"), P("ep", None, "tp"), P("ep", "tp", None),
        ),
        out_specs=(split, split),
        check_vma=False,
    )
```
